128 devices in a mesh: sp: 16 (over z, x), dp: 8 (over y, core).
Axes of the slice: x: 4, y: 4, z: 4, core: 2. Of those that a mesh axis runs over, the one named last changes fastest.
Arguments:
- residual: bfloat16 [8, 2048, 2048], P('dp', 'sp'), may hold values from -6 to 6
- query: bfloat16 [8, 2048, 2048], P('dp', 'sp'), may hold values from -6 to 6
- key: bfloat16 [8, 2048, 2048], P('dp', 'sp'), may hold values from -6 to 6
- value: bfloat16 [8, 2048, 2048], P('dp', 'sp'), may hold values from -6 to 6
- output_gate_input: bfloat16 [8, 2048, 2048], P('dp', 'sp'), may hold values from -6 to 6
- write_strength_logit: bfloat16 [8, 2048, 16], P('dp', 'sp'), may hold values from -6 to 6
- decay_head_input: bfloat16 [8, 2048, 16], P('dp', 'sp'), may hold values from -5 to 5
- added_log_decay: float32 [8, 16, 2048], P('dp', 'sp'), may hold values from -2 to 0
- head_decay_rate: float32 [16], P('sp'), may hold values from 0 to 1
- head_norm_gain: float32 [128], replicated, may hold values from 0.1 to 1.9
- output_projection: bfloat16 [2048, 2048], P(None, 'dp'), may hold values from -0.125 to 0.125
- mixer_norm_gain: float32 [2048], replicated, may hold values from 0.1 to 1.9
- token_expert_index: int32 [8, 2048, 4], P('dp', 'sp'), may hold values from 0 to 127, all different within a row; in each aligned block of 128 rows (0 to 127, 128 to 255, ..., all dimensions but the last counted through in order) at most 6 rows name the same one
- token_expert_weight: float32 [8, 2048, 4], P('dp', 'sp'), may hold values from 0.1 to 0.6
- expert_gate_weight: bfloat16 [128, 2048, 1024], P(('sp', 'dp')), may hold values from -1 to 1
- expert_up_weight: bfloat16 [128, 2048, 1024], P(('sp', 'dp')), may hold values from -1 to 1
- expert_down_weight: bfloat16 [128, 1024, 2048], P(('sp', 'dp')), may hold values from -0.1875 to 0.1875
- feedforward_norm_gain: float32 [2048], replicated, may hold values from 0.1 to 1.9
Outputs:
- blended: float32 [8, 2048, 2048], P('dp', 'sp')
The draws below stay inside these ranges and needn't reach their ends.
Inputs may be any that keep to these rules, and one draw needn't show every extreme that they name: `token_expert_index`: each row names 4 different experts; within the 128 rows of one device no expert is named by more than 6 rows, and in every draw some expert is named by exactly 6 rows of some device.
All inputs are finite; a program needn't handle non-finite values.
Results may differ from the reference program's by a relative error of at most 0.0062.
Values may be sent and summed in bfloat16 or wider, within the bound.
No kernel may reach another device: no remote copies, remote signals or barrier semaphores. Data moves between devices by JAX's collectives and lax.ppermute only.
A program may use at most 128 MiB of HBM per device.

```python
import math
import jax
import jax.numpy as jnp
import numpy as np
from jax import lax

D = 2048
RECURRENT_HEADS = 16
HD = 128
WIDTH = 2048
FF = 1024
TOP = 4
SPAN = 64
TOK_DEV = 128
SEQUENCE_COUNT = 8
SEQUENCE_LENGTH = 2048
EXPERTS = 128
CAP = 6


def draw_decay_head_input(key, part):
    base_key = jax.random.fold_in(key, 21)
    noise_key, level_key = jax.random.split(base_key)
    noise = jax.random.normal(noise_key, (SEQUENCE_COUNT, SEQUENCE_LENGTH, RECURRENT_HEADS), jnp.float32)
    levels = jax.random.uniform(level_key, (SEQUENCE_COUNT, SEQUENCE_LENGTH // TOK_DEV, 1, RECURRENT_HEADS), jnp.float32, -1.0, 1.5)
    levels = jnp.broadcast_to(levels, (SEQUENCE_COUNT, SEQUENCE_LENGTH // TOK_DEV, TOK_DEV, RECURRENT_HEADS)).reshape(SEQUENCE_COUNT, SEQUENCE_LENGTH, RECURRENT_HEADS)
    return jnp.clip(noise + levels, -5.0, 5.0).astype(jnp.bfloat16)


def draw_added_log_decay(key, part):
    base_key = jax.random.fold_in(key, 22)
    where_key, kept_key = jax.random.split(base_key)
    spots = jax.random.randint(where_key, (SEQUENCE_COUNT, RECURRENT_HEADS, 2, 1), 0, SEQUENCE_LENGTH)
    kept = jax.random.uniform(kept_key, (SEQUENCE_COUNT, RECURRENT_HEADS, 2, 1), jnp.float32, 0.5, 0.8)
    places = jnp.arange(SEQUENCE_LENGTH)[None, None, None, :]
    return jnp.sum(jnp.where(places == spots, jnp.log(kept), 0.0), axis=2).astype(jnp.float32)


def draw_head_decay_rate(key, part):
    base_key = jax.random.fold_in(key, 23)
    order_key, fast_key, slow_key = jax.random.split(base_key, 3)
    ranks = jax.random.permutation(order_key, RECURRENT_HEADS)
    fast = jax.random.uniform(fast_key, (RECURRENT_HEADS,), jnp.float32, 0.02, 0.05)
    slow = jax.random.uniform(slow_key, (RECURRENT_HEADS,), jnp.float32, 0.1, 0.3) / SEQUENCE_LENGTH
    return jnp.where(ranks < RECURRENT_HEADS // 2, fast, slow)


def expert_input_weight(key):
    entry_key = jax.random.fold_in(key, 0)
    entries = jax.random.normal(entry_key, (EXPERTS, D, FF), jnp.float32) / math.sqrt(D)
    return jnp.clip(entries, -1.0, 1.0).astype(jnp.bfloat16)


def draw_expert_gate_weight(key, part):
    return expert_input_weight(jax.random.fold_in(key, 11))


def draw_expert_up_weight(key, part):
    return expert_input_weight(jax.random.fold_in(key, 12))


def shard_levels(own_key, dims, cuts, smallest, top_value):
    loudness, own = 1.0, jax.random.fold_in(own_key, 6)
    for axis_at, blocks in cuts:
        draws = jnp.exp(jax.random.uniform(jax.random.fold_in(own, axis_at), (blocks,), jnp.float32, smallest / len(cuts), top_value / len(cuts)))
        loudness = loudness * jnp.repeat(draws, dims[axis_at] // blocks).reshape([-1 if axis == axis_at else 1 for axis in range(len(dims))])
    return loudness


def shared_out(stream_key, own, number, rows, amount, top, reach, lean):
    sequence = jax.random.permutation(stream_key, amount)
    packed, usual = shares(amount, rows * top, reach, lean, True), shares(amount, rows * top, reach, lean, False)
    places = jnp.arange(amount)

    def named(tallies, offset_by):
        used = int((tallies > 0).sum())
        fixed = max(1, used // 4)
        moved = fixed + (places - fixed + offset_by * (used - fixed)) % max(1, amount - fixed)
        return jnp.zeros((amount,), jnp.int32).at[sequence[jnp.where(places < fixed, places, moved)]].set(jnp.asarray(tallies, jnp.int32))

    tallies = jnp.where(number % 4 == 0, named(packed, number // 4), named(usual, number - number // 4 - 1))
    mixed = jax.random.permutation(jax.random.fold_in(own, 3), amount)
    giver, sink = mixed[0:amount // 2 * 2:2], mixed[1:amount // 2 * 2:2]
    room = jnp.minimum(tallies[giver] - 1, reach - tallies[sink]) // 2
    room = jnp.where((giver == sequence[0]) | (sink == sequence[0]) | (tallies[sink] == 0), 0, jnp.maximum(room, 0))
    moved = jax.random.randint(jax.random.fold_in(own, 4), (amount // 2,), 0, 1 << 20) % (room + 1)
    tallies = tallies.at[giver].add(-moved).at[sink].add(moved)
    items = jnp.searchsorted(jnp.cumsum(tallies), jnp.arange(rows * top), side="right").astype(jnp.int32)
    listing = items.reshape(top, rows).T
    listing = listing[jax.random.permutation(jax.random.fold_in(own, 1), rows)]
    offset_by = jax.random.randint(jax.random.fold_in(own, 2), (rows, 1), 0, top)
    return jnp.take_along_axis(listing, (jnp.arange(top)[None, :] + offset_by) % top, axis=1)


def shares(count, total, bound, slope, full):
    loads = [(1 << 20) // math.isqrt(grade ** slope) + 1 for grade in range(1, count + 1)]
    largest = bound if full else min(bound, max(-(-total // count), total * loads[0] // sum(loads)))
    least = 1 if total - largest >= count - 1 else 0
    holding, rest = [largest] + [least] * (count - 1), total - largest - least * (count - 1)
    while rest > 0:
        free = [i for i in range(1, count) if holding[i] < largest] or [i for i in range(1, count) if holding[i] < bound]
        pool, left = sum([loads[i] for i in free]), rest
        for i in free:
            extra = min(bound - holding[i], max(1, left * loads[i] // pool), rest)
            holding[i] = holding[i] + extra
            rest = rest - extra
    return np.array(holding)


def bell_draw(own_key, dims, spread, reach, shards=(), held_as=jnp.bfloat16):
    drawn = spread * jax.random.normal(own_key, dims, jnp.float32)
    if shards:
        drawn = drawn * shard_levels(own_key, dims, shards, -0.22, 0.18)
    return jnp.clip(drawn, -reach, reach).astype(held_as)


def setup_inputs(seed: int = 0) -> dict:
    keys = jax.random.split(jax.random.key(seed), 19)
    residual = bell_draw(keys[0], (SEQUENCE_COUNT, SEQUENCE_LENGTH, D), 1.0, 6.0, ((0, 8), (1, 16)))
    query = bell_draw(keys[1], (SEQUENCE_COUNT, SEQUENCE_LENGTH, WIDTH), 1.0, 6.0, ((0, 8), (1, 16)))
    key = bell_draw(keys[2], (SEQUENCE_COUNT, SEQUENCE_LENGTH, WIDTH), 1.0, 6.0, ((0, 8), (1, 16)))
    value = bell_draw(keys[3], (SEQUENCE_COUNT, SEQUENCE_LENGTH, WIDTH), 1.0, 6.0, ((0, 8), (1, 16)))
    output_gate_input = bell_draw(keys[4], (SEQUENCE_COUNT, SEQUENCE_LENGTH, WIDTH), 1.0, 6.0, ((0, 8), (1, 16)))
    write_strength_logit = bell_draw(keys[5], (SEQUENCE_COUNT, SEQUENCE_LENGTH, RECURRENT_HEADS), 1.5, 6.0, ((0, 8), (1, 16)))
    decay_head_input = draw_decay_head_input(jax.random.fold_in(keys[18], 71), 0)
    added_log_decay = draw_added_log_decay(jax.random.fold_in(keys[18], 71), 0)
    head_decay_rate = draw_head_decay_rate(jax.random.fold_in(keys[18], 71), 0)
    head_norm_gain = jnp.clip(1.0 + 0.18 * jax.random.normal(keys[9], (HD,), jnp.float32), 0.1, 1.9)
    output_projection = bell_draw(keys[10], (WIDTH, D), WIDTH ** -0.5, 0.125, ((1, 8),))
    mixer_norm_gain = jnp.clip(1.0 + 0.18 * jax.random.normal(keys[11], (D,), jnp.float32), 0.1, 1.9)
    token_expert_index_keys = jax.random.split(jax.random.fold_in(keys[12], 1), SEQUENCE_COUNT * SEQUENCE_LENGTH // TOK_DEV)
    token_expert_index_turns = jax.random.permutation(jax.random.fold_in(keys[12], 3), SEQUENCE_COUNT * SEQUENCE_LENGTH // TOK_DEV)
    token_expert_index = jax.vmap(lambda own, number: shared_out(jax.random.fold_in(keys[12], 2), own, number, TOK_DEV, EXPERTS, TOP, CAP, 2))(token_expert_index_keys, token_expert_index_turns).reshape((SEQUENCE_COUNT, SEQUENCE_LENGTH, TOP))
    token_expert_weight = jnp.clip(0.1 + 0.5 * jax.random.uniform(keys[13], (SEQUENCE_COUNT, SEQUENCE_LENGTH, TOP), jnp.float32) ** shard_levels(keys[13], (SEQUENCE_COUNT, SEQUENCE_LENGTH, TOP), ((0, 8), (1, 16)), -0.2, 0.2), 0.1, 0.6)
    expert_gate_weight = draw_expert_gate_weight(jax.random.fold_in(keys[18], 71), 0)
    expert_up_weight = draw_expert_up_weight(jax.random.fold_in(keys[18], 71), 0)
    expert_down_weight = bell_draw(keys[16], (EXPERTS, FF, D), FF ** -0.5, 0.1875, ((0, 128),))
    feedforward_norm_gain = jnp.clip(1.0 + 0.18 * jax.random.normal(keys[17], (D,), jnp.float32), 0.1, 1.9)
    return {"residual": residual, "query": query, "key": key, "value": value, "output_gate_input": output_gate_input, "write_strength_logit": write_strength_logit, "decay_head_input": decay_head_input, "added_log_decay": added_log_decay, "head_decay_rate": head_decay_rate, "head_norm_gain": head_norm_gain, "output_projection": output_projection, "mixer_norm_gain": mixer_norm_gain, "token_expert_index": token_expert_index, "token_expert_weight": token_expert_weight, "expert_gate_weight": expert_gate_weight, "expert_up_weight": expert_up_weight, "expert_down_weight": expert_down_weight, "feedforward_norm_gain": feedforward_norm_gain}


HIGHEST = lax.Precision.HIGHEST
CLAMP_LIMIT = 7.0
SWISH_SLOPE = 1.702

def unit_lower_inverse(strict_part):
    order_len = strict_part.shape[-1]
    identity = jnp.eye(order_len, dtype=jnp.float32)
    result = identity - strict_part
    squared = strict_part
    for _unused in range(int(math.log2(order_len)) - 1):
        squared = jnp.einsum('nij,njk->nik', squared, squared, precision=HIGHEST)
        result = jnp.einsum('nij,njk->nik', result, identity + squared, precision=HIGHEST)
    return result

def delta_rule(q_unit, k_unit, values, write_rate, log_decay):
    length, head_dim = q_unit.shape
    blocks = length // SPAN
    q_block = q_unit.reshape(blocks, SPAN, head_dim)
    k_block = k_unit.reshape(blocks, SPAN, head_dim)
    v_block = values.reshape(blocks, SPAN, head_dim)
    rate_block = write_rate.reshape(blocks, SPAN)
    cumulative = jnp.cumsum(log_decay.reshape(blocks, SPAN), axis=1)
    position = jnp.arange(SPAN)
    strict = position[:, None] > position[None, :]
    inclusive = position[:, None] >= position[None, :]
    within = jnp.exp(jnp.where(inclusive, cumulative[:, :, None] - cumulative[:, None, :], -jnp.inf))
    keys_dot = jnp.einsum('nid,njd->nij', k_block, k_block, precision=HIGHEST)
    lower_part = jnp.where(strict, rate_block[:, :, None] * within * keys_dot, 0.0)
    inverse = unit_lower_inverse(lower_part)
    right_side = jnp.concatenate([rate_block[..., None] * v_block, (rate_block * jnp.exp(cumulative))[..., None] * k_block], axis=-1)
    solved = jnp.einsum('nij,njd->nid', inverse, right_side, precision=HIGHEST)
    base_part = solved[..., :head_dim]
    weight_part = solved[..., head_dim:]
    scores = jnp.einsum('nid,njd->nij', q_block, k_block, precision=HIGHEST) * within
    q_decayed = q_block * jnp.exp(cumulative)[..., None]
    k_decayed = k_block * jnp.exp(cumulative[:, -1:] - cumulative)[..., None]
    carried = jnp.exp(cumulative[:, -1])

    def advance(state, inputs):
        base_rows, weight_rows, score_rows, q_rows, k_rows, carry_rate = inputs
        fresh = base_rows - jnp.dot(weight_rows, state, precision=HIGHEST)
        output = jnp.dot(q_rows, state, precision=HIGHEST) + jnp.dot(score_rows, fresh, precision=HIGHEST)
        state = state * carry_rate + jnp.dot(k_rows.T, fresh, precision=HIGHEST)
        return (state, output)
    initial = jnp.zeros((head_dim, head_dim), jnp.float32)
    _, outputs = lax.scan(advance, initial, (base_part, weight_part, scores, q_decayed, k_decayed, carried))
    return outputs.reshape(length, head_dim)

def unit_rows(values):
    values = values.astype(jnp.float32)
    return values * lax.rsqrt(lax.optimization_barrier(jnp.sum(values * values, -1, keepdims=True)) + 1e-06)

def head_output(recurrent, gate_input, head_norm_gain):
    norm_scale = lax.rsqrt(lax.optimization_barrier(jnp.mean(recurrent * recurrent, -1, keepdims=True)) + 1e-05)
    return (recurrent * norm_scale * head_norm_gain * jax.nn.silu(gate_input.astype(jnp.float32))).astype(jnp.bfloat16)

def layer_norm(values, gain):
    average = lax.optimization_barrier(jnp.mean(values, -1, keepdims=True))
    centred = values - average
    variance = lax.optimization_barrier(jnp.mean(centred * centred, -1, keepdims=True))
    return centred * lax.rsqrt(variance + 1e-05) * gain

def expert_rows(rows, gate_weight, up_weight, down_weight):
    gate = jnp.minimum(jnp.dot(rows, gate_weight, preferred_element_type=jnp.float32), CLAMP_LIMIT)
    upper = jnp.clip(jnp.dot(rows, up_weight, preferred_element_type=jnp.float32), -CLAMP_LIMIT, CLAMP_LIMIT)
    hidden = (gate * jax.nn.sigmoid(SWISH_SLOPE * gate) * (upper + 1.0)).astype(jnp.bfloat16)
    return jnp.dot(hidden, down_weight, preferred_element_type=jnp.float32).astype(jnp.bfloat16)

def reference(residual, query, key, value, output_gate_input, write_strength_logit, decay_head_input, added_log_decay, head_decay_rate, head_norm_gain, output_projection, mixer_norm_gain, token_expert_index, token_expert_weight, expert_gate_weight, expert_up_weight, expert_down_weight, feedforward_norm_gain):

    def by_head(values):
        return values.reshape(SEQUENCE_COUNT, SEQUENCE_LENGTH, RECURRENT_HEADS, HD).transpose(0, 2, 1, 3).reshape(SEQUENCE_COUNT * RECURRENT_HEADS, SEQUENCE_LENGTH, HD)
    q_heads = by_head(query)
    k_heads = by_head(key)
    v_heads = by_head(value)
    rate_heads = jax.nn.sigmoid(write_strength_logit.astype(jnp.float32)).transpose(0, 2, 1).reshape(SEQUENCE_COUNT * RECURRENT_HEADS, SEQUENCE_LENGTH)
    head_decays = (-head_decay_rate[None, :, None] * jax.nn.softplus(decay_head_input.astype(jnp.float32).transpose(0, 2, 1)) + added_log_decay).reshape(SEQUENCE_COUNT * RECURRENT_HEADS, SEQUENCE_LENGTH)

    def one_head(index):
        return delta_rule(unit_rows(q_heads[index]) * HD ** (-0.5), unit_rows(k_heads[index]), v_heads[index].astype(jnp.float32), rate_heads[index], head_decays[index])
    recurrent = lax.map(one_head, jnp.arange(SEQUENCE_COUNT * RECURRENT_HEADS))
    recurrent = recurrent.reshape(SEQUENCE_COUNT, RECURRENT_HEADS, SEQUENCE_LENGTH, HD).transpose(0, 2, 1, 3)
    gated = head_output(recurrent, output_gate_input.reshape(SEQUENCE_COUNT, SEQUENCE_LENGTH, RECURRENT_HEADS, HD), head_norm_gain)
    gated = gated.reshape(SEQUENCE_COUNT * SEQUENCE_LENGTH, WIDTH)
    mixed = jnp.dot(gated, output_projection, preferred_element_type=jnp.float32)
    normed = layer_norm(residual.reshape(SEQUENCE_COUNT * SEQUENCE_LENGTH, D).astype(jnp.float32) + mixed, mixer_norm_gain).astype(jnp.bfloat16)
    tokens = SEQUENCE_COUNT * SEQUENCE_LENGTH
    flat_ids = token_expert_index.reshape(-1)
    flat_weight = jnp.concatenate([token_expert_weight.reshape(-1), jnp.zeros((1,), jnp.float32)])
    padded = jnp.concatenate([normed, jnp.zeros((1, D), jnp.bfloat16)], 0)

    def one_expert(total, expert):
        chosen = jnp.nonzero(flat_ids == expert, size=EXPERTS * CAP, fill_value=tokens * TOP)[0]
        token_index = (chosen // TOP).astype(jnp.int32)
        weight = flat_weight[chosen]
        produced = expert_rows(padded[token_index], expert_gate_weight[expert], expert_up_weight[expert], expert_down_weight[expert])
        return (total.at[token_index].add(weight[:, None] * produced.astype(jnp.float32)), None)
    moe, _ = lax.scan(one_expert, jnp.zeros((tokens + 1, D), jnp.float32), jnp.arange(EXPERTS))
    blended = layer_norm(normed.astype(jnp.float32) + moe[:tokens], feedforward_norm_gain)
    return blended.reshape(SEQUENCE_COUNT, SEQUENCE_LENGTH, D)
```

```python
import jax
import jax.numpy as jnp
from jax import lax
from jax.experimental import pallas as pl
from jax.experimental.pallas import tpu as pltpu
from jax.sharding import Mesh
from jax.sharding import PartitionSpec as P

DP = ("dp_0", "dp_1")
SP_DP = ("sp", "dp_0", "dp_1")
CLAMP_LIMIT = 7.0
SWISH_SLOPE = 1.702
F32 = jnp.float32
BF16 = jnp.bfloat16
HIGHEST = lax.Precision.HIGHEST
C = 128
EXTRA = 16
VMEM = pl.BlockSpec(memory_space=pltpu.VMEM)
SMEM = pl.BlockSpec(memory_space=pltpu.SMEM)
HBM = pl.BlockSpec(memory_space=pl.ANY)


def dot(a, b):
    return jnp.dot(a, b, preferred_element_type=F32)


def dot_nt(a, b, precision=None):
    return lax.dot_general(
        a, b, (((1,), (1,)), ((), ())), precision=precision, preferred_element_type=F32
    )


def dot_tn(a, b):
    return lax.dot_general(a, b, (((0,), (0,)), ((), ())), preferred_element_type=F32)


def halves(x):
    high = x.astype(BF16)
    return high, (x - high.astype(F32)).astype(BF16)


def iotas(rows, columns):
    shape = (rows, columns)
    return lax.broadcasted_iota(jnp.int32, shape, 0), lax.broadcasted_iota(jnp.int32, shape, 1)


def swap_matrix():
    row, column = iotas(256, 256)
    return jnp.where((row % 16) * 16 + row // 16 == column, 1.0, 0.0).astype(BF16)


def pack_kernel(q_ref, k_ref, v_ref, logit_ref, decay_ref, out_ref):
    heads = out_ref.shape[0]
    row, column = iotas(heads, heads)
    eye = jnp.where(row == column, 1.0, 0.0).astype(BF16)
    logits = dot_nt(eye, logit_ref[0])
    decays = dot_nt(eye, decay_ref[0])
    extra_row, _unused = iotas(EXTRA, C)
    for h in range(heads):
        columns = slice(h * C, (h + 1) * C)
        out_ref[h, 0:C] = k_ref[0, :, columns]
        out_ref[h, C : 2 * C] = q_ref[0, :, columns]
        out_ref[h, 2 * C : 3 * C] = v_ref[0, :, columns]
        extra = jnp.where(extra_row == 0, logits[h : h + 1], decays[h : h + 1])
        out_ref[h, 3 * C : 3 * C + EXTRA] = extra.astype(BF16)


def pack(query, key, value, logit, decay_input):
    heads = logit.shape[2]
    return pl.pallas_call(
        pack_kernel,
        out_shape=jax.ShapeDtypeStruct((heads, 3 * C + EXTRA, C), BF16),
        in_specs=[VMEM] * 5,
        out_specs=VMEM,
        name="pack",
    )(query, key, value, logit, decay_input)


GROUP = 4


def delta_kernel(
    x_ref, added_ref, rate_ref, out_ref,
    a_ref, b_ref, qe_ref, su_ref, cum_col_ref, cum_row_ref, write_col_ref, write_row_ref,
):
    chunks = x_ref.shape[0]
    row, column = iotas(C, C)
    inclusive = row >= column
    strict = row > column
    diagonal = row == column

    chunk_row, _unused = iotas(chunks, C)
    logits = jnp.zeros((chunks, C), F32)
    decays = jnp.zeros((chunks, C), F32)
    for n in range(chunks):
        extra = x_ref[n, 3 * C : 3 * C + EXTRA].astype(F32)
        logits = jnp.where(chunk_row == n, extra[0:1], logits)
        decays = jnp.where(chunk_row == n, extra[1:2], decays)
    softplus = jnp.maximum(decays, 0.0) + jnp.log(1.0 + jnp.exp(-jnp.abs(decays)))
    log_decay = added_ref[...] - rate_ref[0] * softplus
    upper = jnp.where(row <= column, 1.0, 0.0)
    lower = jnp.where(row >= column, 1.0, 0.0)
    eye = jnp.where(diagonal, 1.0, 0.0)
    cum_row_ref[...] = jnp.dot(log_decay, upper, precision=HIGHEST, preferred_element_type=F32)
    cum_col_ref[...] = dot_nt(lower, log_decay, precision=HIGHEST)
    write = 1.0 / (1.0 + jnp.exp(-logits))
    write_row_ref[...] = write
    write_col_ref[...] = dot_nt(eye, write, precision=HIGHEST)

    def column_of(ref, n):
        lane = lax.broadcasted_iota(jnp.int32, (C, ref.shape[1]), 1)
        return jnp.sum(jnp.where(lane == n, ref[...], 0.0), axis=1, keepdims=True)

    def prepare(n):
        keys = x_ref[n, 0:C]
        queries = x_ref[n, C : 2 * C]
        values = x_ref[n, 2 * C : 3 * C]
        cum_c = column_of(cum_col_ref, n)
        write_c = column_of(write_col_ref, n)
        cum_r = cum_row_ref[pl.ds(n, 1), :]
        write_r = write_row_ref[pl.ds(n, 1), :]
        products = dot_nt(jnp.concatenate([keys, queries], axis=0), keys)
        keys_dot, scores = products[:C], products[C:]
        squares = jnp.where(diagonal, keys_dot, 0.0)
        key_c = lax.rsqrt(jnp.sum(squares, axis=1, keepdims=True) + 1e-06)
        key_r = lax.rsqrt(jnp.sum(squares, axis=0, keepdims=True) + 1e-06)
        q32 = queries.astype(F32)
        query_c = lax.rsqrt(jnp.sum(q32 * q32, axis=1, keepdims=True) + 1e-06) * C ** (-0.5)
        within = jnp.exp(jnp.where(inclusive, cum_c - cum_r, -jnp.inf)) * key_r
        lower_part = jnp.where(strict, keys_dot * within * (write_c * key_c), 0.0)
        scores = scores * within * query_c

        high, low = halves(lower_part)
        left = jnp.concatenate([high, low], axis=1)
        pair = (row // 2 == column // 2) & strict
        inverse = jnp.where(pair, -lower_part, eye)
        size = 2
        while size < C:
            high, low = halves(inverse)
            first = dot(left, jnp.concatenate([high, high], axis=0))
            first_high, first_low = halves(first)
            second = dot(
                jnp.concatenate([high, high], axis=1),
                jnp.concatenate([first_high, first_low], axis=0),
            )
            joined = (row // (2 * size) == column // (2 * size)) & (row // size > column // size)
            inverse = jnp.where(joined, -second, inverse)
            size *= 2

        decay_r = jnp.exp(cum_r)
        base_high, base_low = halves(inverse * write_r)
        base = dot(
            jnp.concatenate([base_high, base_low], axis=1),
            jnp.concatenate([values, values], axis=0),
        )
        weight_high, weight_low = halves(inverse * (write_r * decay_r * key_r))
        weight = dot(
            jnp.concatenate([weight_high, weight_low], axis=1),
            jnp.concatenate([keys, keys], axis=0),
        )
        last = cum_c[C - 1 : C]
        both = jnp.concatenate([base, weight], axis=1)
        carried_high, carried_low = halves(both * (key_c * jnp.exp(last - cum_c)))
        keys_t = keys.T
        update = dot(
            jnp.concatenate([keys_t, keys_t], axis=1),
            jnp.concatenate([carried_high, carried_low], axis=0),
        )
        b_ref[n] = update[:, :C]
        a_ref[n] = jnp.where(diagonal, jnp.exp(last), 0.0) - update[:, C:]
        score_high, score_low = halves(scores)
        both = both.astype(BF16)
        seen = dot(
            jnp.concatenate([score_high, score_low], axis=1),
            jnp.concatenate([both, both], axis=0),
        )
        su_ref[n] = seen[:, :C]
        qe_ref[n] = q32 * (query_c * jnp.exp(cum_c)) - seen[:, C:]

    def group(g, carry):
        for k in range(GROUP):
            prepare(g * GROUP + k)
        return carry

    lax.fori_loop(0, chunks // GROUP, group, 0)

    def advance(n, state):
        high, low = halves(state)
        both = jnp.concatenate([high, low], axis=0)
        q_high, q_low = halves(qe_ref[n])
        out = dot(jnp.concatenate([q_high, q_high], axis=1), both) + su_ref[n]
        scale = lax.rsqrt(jnp.mean(out * out, axis=1, keepdims=True) + 1e-05)
        out_ref[n] = (out * scale).astype(BF16)
        a_high, a_low = halves(a_ref[n])
        return (
            dot(jnp.concatenate([a_high, a_high], axis=1), both) + dot(a_low, high) + b_ref[n]
        )

    def steps(g, state):
        for k in range(2):
            state = advance(g * 2 + k, state)
        return state

    lax.fori_loop(0, chunks // 2, steps, jnp.zeros((C, C), F32))


def delta(blocks, added, decay_rate):
    chunks = blocks.shape[0]
    return pl.pallas_call(
        delta_kernel,
        out_shape=jax.ShapeDtypeStruct((chunks, C, C), BF16),
        in_specs=[VMEM, VMEM, SMEM],
        out_specs=VMEM,
        scratch_shapes=[pltpu.VMEM((chunks, C, C), F32)] * 4
        + [
            pltpu.VMEM((C, chunks), F32),
            pltpu.VMEM((chunks, C), F32),
            pltpu.VMEM((C, chunks), F32),
            pltpu.VMEM((chunks, C), F32),
        ],
        cost_estimate=pl.CostEstimate(flops=4 * 10**9, bytes_accessed=2**21, transcendentals=0),
        name="delta",
    )(blocks, added, decay_rate)


def slots_kernel(index_ref, dest_ref, source_ref, count_ref):
    experts = count_ref.shape[0]
    capacity = source_ref.shape[0] // experts

    def clear(e, carry):
        count_ref[e] = 0
        for k in range(capacity):
            source_ref[e * capacity + k] = 0
        return carry

    lax.fori_loop(0, experts, clear, 0)

    def place(t, carry):
        for k in range(4):
            e = index_ref[t * 4 + k]
            used = count_ref[e]
            count_ref[e] = used + 1
            slot = e * capacity + used
            dest_ref[t * 4 + k] = slot
            source_ref[slot] = t
        return carry

    lax.fori_loop(0, index_ref.shape[0] // 4, place, 0)


def slots(index, experts, capacity):
    return pl.pallas_call(
        slots_kernel,
        out_shape=(
            jax.ShapeDtypeStruct(index.shape, jnp.int32),
            jax.ShapeDtypeStruct((experts * capacity,), jnp.int32),
        ),
        in_specs=[SMEM],
        out_specs=(SMEM, SMEM),
        scratch_shapes=[pltpu.SMEM((experts,), jnp.int32)],
        name="slots",
    )(index)


def project_kernel(
    rec_ref, gate_ref, head_gain_ref, residual_ref, gain_ref, source_ref, place_ref,
    *rest,
):
    weight_refs = rest[:8]
    normed_ref, out_ref, gated_ref, mixed_ref, w_ref, sems = rest[8:]
    copies = [
        pltpu.make_async_copy(weight_refs[k], w_ref.at[k], sems.at[k]) for k in range(8)
    ]
    for copy in copies:
        copy.start()
    heads = rec_ref.shape[0]
    head_gain = head_gain_ref[...]
    for h in range(heads):
        columns = slice(h * C, (h + 1) * C)
        gate = gate_ref[0, :, columns].astype(F32)
        gate = gate / (1.0 + jnp.exp(-gate))
        gated_ref[:, columns] = (rec_ref[h].astype(F32) * head_gain * gate).astype(BF16)
    for k in range(8):
        copies[k].wait()
        mixed_ref[place_ref[k]] = dot(gated_ref[...], w_ref[k])
    total = jnp.concatenate([mixed_ref[k] for k in range(8)], axis=1)
    total = total + residual_ref[0].astype(F32)
    centred = total - jnp.mean(total, axis=1, keepdims=True)
    variance = jnp.mean(centred * centred, axis=1, keepdims=True)
    normed = (centred * lax.rsqrt(variance + 1e-05) * gain_ref[...]).astype(BF16)
    swap = swap_matrix()
    tiles = normed.shape[1] // C
    for g in range(normed.shape[0] // 16):
        rows = normed[g * 16 : (g + 1) * 16]
        stacked = jnp.concatenate([rows[:, j * C : (j + 1) * C] for j in range(tiles)], axis=0)
        turned = dot(swap, stacked).astype(BF16)
        normed_ref[g * 16 : (g + 1) * 16] = turned.reshape(16, tiles, C)

    def send(i, carry):
        for k in range(16):
            slot = i * 16 + k
            out_ref[slot] = normed_ref[source_ref[slot]]
        return carry

    lax.fori_loop(0, out_ref.shape[0] // 16, send, 0)


def project(recurrent, gate, head_gain, residual, gain, source, place, weights):
    tokens = residual.shape[1]
    features = residual.shape[2]
    tiles = features // C
    return pl.pallas_call(
        project_kernel,
        out_shape=(
            jax.ShapeDtypeStruct((tokens, tiles, C), BF16),
            jax.ShapeDtypeStruct((source.shape[0], tiles, C), BF16),
        ),
        in_specs=[VMEM] * 5 + [SMEM] * 2 + [HBM] * 8,
        out_specs=(VMEM, VMEM),
        scratch_shapes=[
            pltpu.VMEM((tokens, features), BF16),
            pltpu.VMEM((8, tokens, features // 8), F32),
            pltpu.VMEM((8, features, features // 8), BF16),
            pltpu.SemaphoreType.DMA((8,)),
        ],
        cost_estimate=pl.CostEstimate(flops=10**9, bytes_accessed=2**24, transcendentals=0),
        name="project",
    )(recurrent, gate, head_gain, residual, gain, source, place, *weights)


FF_BLOCK = 256


def expert_kernel(x_ref, gate_ref, up_ref, down_ref, out_ref, rows_ref, hidden_ref, made_ref):
    step = pl.program_id(0)
    slots_ = x_ref.shape[0]
    tiles = x_ref.shape[1]
    groups = slots_ // 16
    ff_steps = hidden_ref.shape[0]

    @pl.when(step == 0)
    def _():
        swap = swap_matrix()

        def turn(i, carry):
            for k in range(4):
                start = pl.multiple_of((i * 4 + k) * 16, 16)
                turned = dot(swap, x_ref[pl.ds(start, 16)].reshape(16 * tiles, C)).astype(BF16)
                for j in range(tiles):
                    rows_ref[pl.ds(start, 16), j * C : (j + 1) * C] = turned[j * 16 : (j + 1) * 16]
            return carry

        lax.fori_loop(0, groups // 4, turn, 0)

    @pl.when(step < ff_steps)
    def _():
        rows = rows_ref[...]
        gate = jnp.minimum(dot(rows, gate_ref[...]), CLAMP_LIMIT)
        up = jnp.clip(dot(rows, up_ref[...]), -CLAMP_LIMIT, CLAMP_LIMIT)
        hidden = gate / (1.0 + jnp.exp(-SWISH_SLOPE * gate)) * (up + 1.0)
        hidden_ref[step] = hidden.astype(BF16)

    @pl.when(step >= ff_steps)
    def _():
        total = dot(hidden_ref[0], down_ref[0:FF_BLOCK])
        for k in range(1, ff_steps):
            total = total + dot(hidden_ref[k], down_ref[k * FF_BLOCK : (k + 1) * FF_BLOCK])
        made_ref[step - ff_steps] = total.astype(BF16)

    @pl.when(step == pl.num_programs(0) - 1)
    def _():
        swap = swap_matrix()
        down_steps, _rows, width = made_ref.shape

        def turn(i, carry):
            for k in range(2):
                start = pl.multiple_of((i * 2 + k) * 16, 16)
                pieces = []
                for d in range(down_steps):
                    piece = made_ref[d, pl.ds(start, 16), :]
                    pieces += [piece[:, j * C : (j + 1) * C] for j in range(width // C)]
                turned = dot(swap, jnp.concatenate(pieces, axis=0)).astype(BF16)
                out_ref[pl.ds(start, 16)] = turned.reshape(16, tiles, C)
            return carry

        lax.fori_loop(0, groups // 2, turn, 0)


def expert(rows, gate_weight, up_weight, down_weight):
    slots_, tiles, _lanes = rows.shape
    features, hidden = gate_weight.shape
    ff_steps = hidden // FF_BLOCK
    width = 512
    down_steps = features // width
    return pl.pallas_call(
        expert_kernel,
        grid=(ff_steps + down_steps,),
        out_shape=jax.ShapeDtypeStruct(rows.shape, BF16),
        in_specs=[
            pl.BlockSpec(rows.shape, lambda i: (0, 0, 0), pipeline_mode=pl.Buffered(1)),
            pl.BlockSpec((features, FF_BLOCK), lambda i: (0, jnp.minimum(i, ff_steps - 1))),
            pl.BlockSpec((features, FF_BLOCK), lambda i: (0, jnp.minimum(i, ff_steps - 1))),
            pl.BlockSpec((hidden, width), lambda i: (0, jnp.maximum(i - ff_steps, 0))),
        ],
        out_specs=pl.BlockSpec(rows.shape, lambda i: (0, 0, 0), pipeline_mode=pl.Buffered(1)),
        scratch_shapes=[
            pltpu.VMEM((slots_, features), BF16),
            pltpu.VMEM((ff_steps, slots_, FF_BLOCK), BF16),
            pltpu.VMEM((down_steps, slots_, width), BF16),
        ],
        compiler_params=pltpu.CompilerParams(dimension_semantics=("arbitrary",)),
        cost_estimate=pl.CostEstimate(flops=10**10, bytes_accessed=2**24, transcendentals=0),
        name="expert",
    )(rows, gate_weight, up_weight, down_weight)


def combine_kernel(back_ref, normed_ref, gain_ref, dest_ref, weight_ref, out_ref, z_ref):
    tokens, tiles, _lanes = normed_ref.shape
    features = tiles * C
    gain = gain_ref[...]

    def token(t):
        total = normed_ref[t].astype(F32)
        for k in range(4):
            slot = dest_ref[t * 4 + k]
            total = total + weight_ref[t * 4 + k] * back_ref[slot].astype(F32)
        centred = total - jnp.sum(total, keepdims=True) * (1.0 / features)
        variance = jnp.sum(centred * centred, keepdims=True) * (1.0 / features)
        z_ref[t] = centred * lax.rsqrt(variance + 1e-05) * gain

    def some(i, carry):
        for k in range(8):
            token(i * 8 + k)
        return carry

    lax.fori_loop(0, tokens // 8, some, 0)
    swap = swap_matrix()
    for g in range(tokens // 16):
        z = z_ref[g * 16 : (g + 1) * 16].reshape(16 * tiles, C)
        high = z.astype(BF16)
        rest = z - high.astype(F32)
        middle = rest.astype(BF16)
        low = (rest - middle.astype(F32)).astype(BF16)
        turned = dot(swap, high) + dot(swap, middle) + dot(swap, low)
        for j in range(tiles):
            out_ref[0, g * 16 : (g + 1) * 16, j * C : (j + 1) * C] = turned[j * 16 : (j + 1) * 16]


def combine(back, normed, gain, dest, weight):
    tokens, tiles, _lanes = normed.shape
    return pl.pallas_call(
        combine_kernel,
        out_shape=jax.ShapeDtypeStruct((1, tokens, tiles * C), F32),
        in_specs=[VMEM] * 3 + [SMEM] * 2,
        out_specs=VMEM,
        scratch_shapes=[pltpu.VMEM((tokens, tiles, C), F32)],
        name="combine",
    )(back, normed, gain, dest, weight)


def gathered(block):
    y_size, core_size = lax.axis_size("dp_0"), lax.axis_size("dp_1")
    y, core = lax.axis_index("dp_0"), lax.axis_index("dp_1")
    found = [block]
    for shift in range(1, y_size):
        pairs = [(i, (i + shift) % y_size) for i in range(y_size)]
        found.append(lax.ppermute(block, "dp_0", pairs))
    places = [((y - shift) % y_size) * core_size + core for shift in range(y_size)]
    swapped = [lax.ppermute(b, "dp_1", [(0, 1), (1, 0)]) for b in found]
    others = [((y - shift) % y_size) * core_size + 1 - core for shift in range(y_size)]
    return found + swapped, jnp.stack(places + others).astype(jnp.int32)


def per_device(
    residual,
    query,
    key,
    value,
    output_gate_input,
    write_strength_logit,
    decay_head_input,
    added_log_decay,
    head_decay_rate,
    head_norm_gain,
    output_projection,
    mixer_norm_gain,
    token_expert_index,
    token_expert_weight,
    expert_gate_weight,
    expert_up_weight,
    expert_down_weight,
    feedforward_norm_gain,
):
    experts = lax.axis_size(SP_DP)
    tokens, features = residual.shape[1:]
    picks = token_expert_index.shape[2]
    capacity = tokens * picks * 3 // (2 * experts)
    tiles = features // C
    weights, places = gathered(output_projection)
    dest, source = slots(token_expert_index.reshape(-1), experts, capacity)
    blocks = pack(query, key, value, write_strength_logit, decay_head_input)
    blocks = lax.all_to_all(blocks, "sp", split_axis=0, concat_axis=0, tiled=True)
    recurrent = delta(blocks, added_log_decay.reshape(-1, C), head_decay_rate)
    returned = lax.all_to_all(recurrent, "sp", split_axis=0, concat_axis=0, tiled=True)
    normed, rows = project(
        returned,
        output_gate_input,
        head_norm_gain.reshape(1, C),
        residual,
        mixer_norm_gain.reshape(1, features),
        source,
        places,
        weights,
    )
    rows = rows.reshape(experts, capacity * tiles, C)
    rows = lax.all_to_all(rows, SP_DP, split_axis=0, concat_axis=0, tiled=True)
    made = expert(
        rows.reshape(experts * capacity, tiles, C),
        expert_gate_weight[0],
        expert_up_weight[0],
        expert_down_weight[0],
    )
    made = made.reshape(experts, capacity * tiles, C)
    back = lax.all_to_all(made, SP_DP, split_axis=0, concat_axis=0, tiled=True)
    return combine(
        back.reshape(experts * capacity, tiles, C),
        normed,
        feedforward_norm_gain.reshape(tiles, C),
        dest,
        token_expert_weight.reshape(-1),
    )


def solution(mesh):
    torus = Mesh(mesh.devices.reshape(mesh.shape["sp"], 4, 2), ("sp", "dp_0", "dp_1"))
    return jax.shard_map(
        per_device,
        mesh=torus,
        in_specs=(
            P(DP, "sp", None),
            P(DP, "sp", None),
            P(DP, "sp", None),
            P(DP, "sp", None),
            P(DP, "sp", None),
            P(DP, "sp", None),
            P(DP, "sp", None),
            P(DP, "sp", None),
            P("sp"),
            P(),
            P(None, DP),
            P(),
            P(DP, "sp", None),
            P(DP, "sp", None),
            P(SP_DP, None, None),
            P(SP_DP, None, None),
            P(SP_DP, None, None),
            P(),
        ),
        out_specs=P(DP, "sp", None),
        check_vma=False,
    )
```

```python
import jax
import jax.numpy as jnp
from jax import lax
from jax.experimental import pallas as pl
from jax.experimental.pallas import tpu as pltpu
from jax.sharding import Mesh
from jax.sharding import PartitionSpec as P

DP = ("dp_0", "dp_1")
SP_DP = ("sp", "dp_0", "dp_1")
CLAMP_LIMIT = 7.0
SWISH_SLOPE = 1.702
F32 = jnp.float32
BF16 = jnp.bfloat16
HIGHEST = lax.Precision.HIGHEST
C = 128
EXTRA = 16
VMEM = pl.BlockSpec(memory_space=pltpu.VMEM)
SMEM = pl.BlockSpec(memory_space=pltpu.SMEM)
HBM = pl.BlockSpec(memory_space=pl.ANY)


def dot(a, b):
    return jnp.dot(a, b, preferred_element_type=F32)


def dot_nt(a, b, precision=None):
    return lax.dot_general(
        a, b, (((1,), (1,)), ((), ())), precision=precision, preferred_element_type=F32
    )


def dot_tn(a, b):
    return lax.dot_general(a, b, (((0,), (0,)), ((), ())), preferred_element_type=F32)


def halves(x):
    high = x.astype(BF16)
    return high, (x - high.astype(F32)).astype(BF16)


def iotas(rows, columns):
    shape = (rows, columns)
    return lax.broadcasted_iota(jnp.int32, shape, 0), lax.broadcasted_iota(jnp.int32, shape, 1)


def swap_matrix():
    row, column = iotas(256, 256)
    return jnp.where((row % 16) * 16 + row // 16 == column, 1.0, 0.0).astype(BF16)


def pack_kernel(q_ref, k_ref, v_ref, logit_ref, decay_ref, key_out_ref, out_ref):
    heads = out_ref.shape[0]
    logits = logit_ref[0].astype(F32)
    decays = decay_ref[0].astype(F32)
    extra_row, _unused = iotas(EXTRA, C)
    for h in range(heads):
        columns = slice(h * C, (h + 1) * C)
        key_out_ref[h, 0:C] = k_ref[0, :, columns]
        extra = jnp.where(extra_row == 0, logits[h : h + 1], decays[h : h + 1])
        key_out_ref[h, C : C + EXTRA] = extra.astype(BF16)
        out_ref[h, 0:C] = q_ref[0, :, columns]
        out_ref[h, C : 2 * C] = v_ref[0, :, columns]


def pack(query, key, value, logit, decay_input):
    heads = logit.shape[1]
    return pl.pallas_call(
        pack_kernel,
        out_shape=(
            jax.ShapeDtypeStruct((heads, C + EXTRA, C), BF16),
            jax.ShapeDtypeStruct((heads, 2 * C, C), BF16),
        ),
        in_specs=[VMEM] * 5,
        out_specs=(VMEM, VMEM),
        name="pack",
    )(query, key, value, logit, decay_input)


GROUP = 4


def column_of(ref, n):
    lane = lax.broadcasted_iota(jnp.int32, ref.shape, 1)
    return jnp.sum(jnp.where(lane == n, ref[...], 0.0), axis=1, keepdims=True)


def beside(a, b):
    return jnp.concatenate([a, b], axis=1)


def above(a, b):
    return jnp.concatenate([a, b], axis=0)


def inverse_kernel(
    x_ref, added_ref, rate_ref,
    base_ref, weight_ref, a_ref, cum_col_ref, cum_row_ref, key_col_ref, key_row_ref,
    write_col_ref, write_row_ref,
):
    chunks = x_ref.shape[0]
    row, column = iotas(C, C)
    inclusive = row >= column
    strict = row > column
    diagonal = row == column

    chunk_row, _unused = iotas(chunks, C)
    logits = jnp.zeros((chunks, C), F32)
    decays = jnp.zeros((chunks, C), F32)
    for n in range(chunks):
        extra = x_ref[n, C : C + EXTRA].astype(F32)
        logits = jnp.where(chunk_row == n, extra[0:1], logits)
        decays = jnp.where(chunk_row == n, extra[1:2], decays)
    softplus = jnp.maximum(decays, 0.0) + jnp.log(1.0 + jnp.exp(-jnp.abs(decays)))
    log_decay = added_ref[...] - rate_ref[0] * softplus
    upper = jnp.where(row <= column, 1.0, 0.0)
    lower = jnp.where(inclusive, 1.0, 0.0)
    eye = jnp.where(diagonal, 1.0, 0.0)
    cum_row_ref[...] = jnp.dot(log_decay, upper, precision=HIGHEST, preferred_element_type=F32)
    cum_col_ref[...] = dot_nt(lower, log_decay, precision=HIGHEST)
    write = 1.0 / (1.0 + jnp.exp(-logits))
    write_row_ref[...] = write
    write_col_ref[...] = dot_nt(eye, write, precision=HIGHEST)
    lane = lax.broadcasted_iota(jnp.int32, (C, chunks), 1)

    def group(g, key_columns):
        ns = [g * GROUP + k for k in range(GROUP)]
        keys = [x_ref[n, 0:C] for n in ns]
        products = [dot_nt(k, k) for k in keys]
        cum_c = [column_of(cum_col_ref, n) for n in ns]
        write_c = [column_of(write_col_ref, n) for n in ns]
        cum_r = [cum_row_ref[pl.ds(n, 1), :] for n in ns]
        write_r = [write_row_ref[pl.ds(n, 1), :] for n in ns]
        squares = [jnp.where(diagonal, p, 0.0) for p in products]
        key_c = [lax.rsqrt(jnp.sum(s, axis=1, keepdims=True) + 1e-06) for s in squares]
        key_r = [lax.rsqrt(jnp.sum(s, axis=0, keepdims=True) + 1e-06) for s in squares]
        for n, c, r in zip(ns, key_c, key_r):
            key_columns = jnp.where(lane == n, c, key_columns)
            key_row_ref[pl.ds(n, 1), :] = r
        lower_part = [
            jnp.where(
                strict,
                p * jnp.exp(jnp.where(inclusive, cc - cr, -jnp.inf)) * (wc * kc) * kr,
                0.0,
            )
            for p, cc, cr, wc, kc, kr in zip(products, cum_c, cum_r, write_c, key_c, key_r)
        ]

        left = [beside(*halves(part)) for part in lower_part]
        pair = (row // 2 == column // 2) & strict
        inverse = [jnp.where(pair, -part, eye) for part in lower_part]
        size = 2
        while size < C:
            highs = [i.astype(BF16) for i in inverse]
            first = [dot(f, above(h, h)) for f, h in zip(left, highs)]
            first = [above(*halves(f)) for f in first]
            second = [dot(beside(h, h), f) for h, f in zip(highs, first)]
            joined = (row // (2 * size) == column // (2 * size)) & (row // size > column // size)
            inverse = [jnp.where(joined, -s, i) for s, i in zip(second, inverse)]
            size *= 2

        for n, i, w in zip(ns, inverse, write_r):
            base_ref[n] = beside(*halves(i * w))
        weight = [
            beside(*halves(i * (w * jnp.exp(c) * k)))
            for i, w, c, k in zip(inverse, write_r, cum_r, key_r)
        ]
        weight = [dot(w, above(k, k)) for w, k in zip(weight, keys)]
        for n, w in zip(ns, weight):
            weight_ref[n] = w.astype(BF16)
        last = [c[C - 1 : C] for c in cum_c]
        carried = [
            above(*halves(w * (k * jnp.exp(end - c))))
            for w, k, end, c in zip(weight, key_c, last, cum_c)
        ]
        turned = [k.T for k in keys]
        update = [dot(beside(t, t), c) for t, c in zip(turned, carried)]
        for n, u, end in zip(ns, update, last):
            a_ref[n] = beside(*halves(jnp.where(diagonal, jnp.exp(end), 0.0) - u))
        return key_columns

    key_col_ref[...] = lax.fori_loop(
        0, chunks // GROUP, group, jnp.zeros((C, chunks), F32)
    )


def chunk_inverse(blocks, added, decay_rate):
    chunks = blocks.shape[0]
    wide = jax.ShapeDtypeStruct((chunks, C, 2 * C), BF16)
    columns = jax.ShapeDtypeStruct((C, chunks), F32)
    rows = jax.ShapeDtypeStruct((chunks, C), F32)
    return pl.pallas_call(
        inverse_kernel,
        out_shape=(
            wide, jax.ShapeDtypeStruct((chunks, C, C), BF16), wide, columns, rows, columns, rows,
        ),
        in_specs=[VMEM, VMEM, SMEM],
        out_specs=(VMEM,) * 7,
        scratch_shapes=[pltpu.VMEM((C, chunks), F32), pltpu.VMEM((chunks, C), F32)],
        cost_estimate=pl.CostEstimate(flops=4 * 10**9, bytes_accessed=2**21, transcendentals=0),
        name="inverse",
    )(blocks, added, decay_rate)


def delta_kernel(
    key_ref, x_ref, base_ref, weight_ref, a_ref, cum_col_ref, cum_row_ref, key_col_ref,
    key_row_ref, out_ref, b_ref, qe_ref, su_ref,
):
    chunks = x_ref.shape[0]
    row, column = iotas(C, C)
    inclusive = row >= column

    def prepare(g):
        ns = [g * GROUP + k for k in range(GROUP)]
        keys = [key_ref[n, 0:C] for n in ns]
        queries = [x_ref[n, 0:C] for n in ns]
        values = [x_ref[n, C : 2 * C] for n in ns]
        scores = [dot_nt(q, k) for q, k in zip(queries, keys)]
        base = [dot(base_ref[n], above(v, v)) for n, v in zip(ns, values)]
        cum_c = [column_of(cum_col_ref, n) for n in ns]
        key_c = [column_of(key_col_ref, n) for n in ns]
        cum_r = [cum_row_ref[pl.ds(n, 1), :] for n in ns]
        key_r = [key_row_ref[pl.ds(n, 1), :] for n in ns]
        q32 = [q.astype(F32) for q in queries]
        query_c = [
            lax.rsqrt(jnp.sum(q * q, axis=1, keepdims=True) + 1e-06) * C ** (-0.5) for q in q32
        ]
        scores = [
            s * jnp.exp(jnp.where(inclusive, cc - cr, -jnp.inf)) * kr * qc
            for s, cc, cr, kr, qc in zip(scores, cum_c, cum_r, key_r, query_c)
        ]
        carried = [
            above(*halves(b * (k * jnp.exp(c[C - 1 : C] - c))))
            for b, k, c in zip(base, key_c, cum_c)
        ]
        turned = [k.T for k in keys]
        update = [dot(beside(t, t), c) for t, c in zip(turned, carried)]
        both = [beside(b.astype(BF16), weight_ref[n]) for n, b in zip(ns, base)]
        seen = [dot(beside(*halves(s)), above(b, b)) for s, b in zip(scores, both)]
        for n, u, s, q, qc, c in zip(ns, update, seen, q32, query_c, cum_c):
            b_ref[n] = u
            su_ref[n] = s[:, :C]
            qe_ref[n] = beside(*halves(q * (qc * jnp.exp(c)) - s[:, C:]))

    def advance(g, state):
        for k in range(GROUP):
            n = g * GROUP + k
            high, low = halves(state)
            queries = qe_ref[n]
            out = dot(queries, above(high, high)) + su_ref[n]
            scale = lax.rsqrt(jnp.mean(out * out, axis=1, keepdims=True) + 1e-05)
            out_ref[n] = (out * scale).astype(BF16)
            a_high, a_low = a_ref[n, :, :C], a_ref[n, :, C:]
            state = dot(beside(a_high, a_high), above(high, low)) + dot(a_low, high) + b_ref[n]
        return state

    prepare(0)

    def step(g, state):
        state = advance(g - 1, state)
        prepare(g)
        return state

    state = lax.fori_loop(1, chunks // GROUP, step, jnp.zeros((C, C), F32))
    advance(chunks // GROUP - 1, state)


def delta(keys, blocks, parts):
    chunks = blocks.shape[0]
    return pl.pallas_call(
        delta_kernel,
        out_shape=jax.ShapeDtypeStruct((chunks, C, C), BF16),
        in_specs=[VMEM] * 9,
        out_specs=VMEM,
        scratch_shapes=[
            pltpu.VMEM((chunks, C, C), F32),
            pltpu.VMEM((chunks, C, 2 * C), BF16),
            pltpu.VMEM((chunks, C, C), F32),
        ],
        cost_estimate=pl.CostEstimate(flops=4 * 10**9, bytes_accessed=2**21, transcendentals=0),
        name="delta",
    )(keys, blocks, *parts)


def slots_kernel(index_ref, dest_ref, source_ref, count_ref):
    experts = count_ref.shape[0]
    capacity = source_ref.shape[0] // experts

    def clear(e, carry):
        count_ref[e] = 0
        for k in range(capacity):
            source_ref[e * capacity + k] = 0
        return carry

    lax.fori_loop(0, experts, clear, 0)

    tokens = index_ref.shape[0] // 4

    def place(t, carry):
        for k in range(4):
            at = k * tokens + t
            e = index_ref[at]
            used = count_ref[e]
            count_ref[e] = used + 1
            slot = e * capacity + used
            dest_ref[at] = slot
            source_ref[slot] = t
        return carry

    lax.fori_loop(0, tokens, place, 0)


def slots(index, experts, capacity):
    return pl.pallas_call(
        slots_kernel,
        out_shape=(
            jax.ShapeDtypeStruct(index.shape, jnp.int32),
            jax.ShapeDtypeStruct((experts * capacity,), jnp.int32),
        ),
        in_specs=[SMEM],
        out_specs=(SMEM, SMEM),
        scratch_shapes=[pltpu.SMEM((experts,), jnp.int32)],
        name="slots",
    )(index)


def project_kernel(
    rec_ref, gate_ref, head_gain_ref, residual_ref, gain_ref, source_ref, place_ref,
    *rest,
):
    weight_refs = rest[:8]
    normed_ref, out_ref, gated_ref, mixed_ref, w_ref, sems = rest[8:]
    copies = [
        pltpu.make_async_copy(weight_refs[k], w_ref.at[k], sems.at[k]) for k in range(8)
    ]
    for copy in copies:
        copy.start()
    heads = rec_ref.shape[0]
    head_gain = head_gain_ref[...]
    for h in range(heads):
        columns = slice(h * C, (h + 1) * C)
        gate = gate_ref[0, :, columns].astype(F32)
        gate = gate / (1.0 + jnp.exp(-gate))
        gated_ref[:, columns] = (rec_ref[h].astype(F32) * head_gain * gate).astype(BF16)
    for k in range(8):
        copies[k].wait()
        mixed_ref[place_ref[k]] = dot(gated_ref[...], w_ref[k])
    total = jnp.concatenate([mixed_ref[k] for k in range(8)], axis=1)
    total = total + residual_ref[0].astype(F32)
    centred = total - jnp.mean(total, axis=1, keepdims=True)
    variance = jnp.mean(centred * centred, axis=1, keepdims=True)
    normed = (centred * lax.rsqrt(variance + 1e-05) * gain_ref[...]).astype(BF16)
    swap = swap_matrix()
    tiles = normed.shape[1] // C
    for g in range(normed.shape[0] // 16):
        rows = normed[g * 16 : (g + 1) * 16]
        stacked = jnp.concatenate([rows[:, j * C : (j + 1) * C] for j in range(tiles)], axis=0)
        turned = dot(swap, stacked).astype(BF16)
        normed_ref[g * 16 : (g + 1) * 16] = turned.reshape(16, tiles, C)

    def send(i, carry):
        for k in range(16):
            slot = i * 16 + k
            out_ref[slot] = normed_ref[source_ref[slot]]
        return carry

    lax.fori_loop(0, out_ref.shape[0] // 16, send, 0)


def project(recurrent, gate, head_gain, residual, gain, source, place, weights):
    tokens = residual.shape[1]
    features = residual.shape[2]
    tiles = features // C
    return pl.pallas_call(
        project_kernel,
        out_shape=(
            jax.ShapeDtypeStruct((tokens, tiles, C), BF16),
            jax.ShapeDtypeStruct((source.shape[0], tiles, C), BF16),
        ),
        in_specs=[VMEM] * 5 + [SMEM] * 2 + [HBM] * 8,
        out_specs=(VMEM, VMEM),
        scratch_shapes=[
            pltpu.VMEM((tokens, features), BF16),
            pltpu.VMEM((8, tokens, features // 8), F32),
            pltpu.VMEM((8, features, features // 8), BF16),
            pltpu.SemaphoreType.DMA((8,)),
        ],
        cost_estimate=pl.CostEstimate(flops=10**9, bytes_accessed=2**24, transcendentals=0),
        name="project",
    )(recurrent, gate, head_gain, residual, gain, source, place, *weights)


FF_BLOCK = 256


def expert_kernel(x_ref, gate_ref, up_ref, down_ref, out_ref, rows_ref, hidden_ref, made_ref):
    step = pl.program_id(0)
    slots_ = x_ref.shape[0]
    tiles = x_ref.shape[1]
    groups = slots_ // 16
    ff_steps = hidden_ref.shape[0]

    @pl.when(step == 0)
    def _():
        swap = swap_matrix()

        def turn(i, carry):
            for k in range(2):
                start = pl.multiple_of((i * 4 + k * 2) * 16, 16)
                other = pl.multiple_of(start + 16, 16)
                turned = dot(
                    swap,
                    beside(
                        x_ref[pl.ds(start, 16)].reshape(16 * tiles, C),
                        x_ref[pl.ds(other, 16)].reshape(16 * tiles, C),
                    ),
                ).astype(BF16)
                for j in range(tiles):
                    part = turned[j * 16 : (j + 1) * 16]
                    rows_ref[pl.ds(start, 16), j * C : (j + 1) * C] = part[:, :C]
                    rows_ref[pl.ds(other, 16), j * C : (j + 1) * C] = part[:, C:]
            return carry

        lax.fori_loop(0, groups // 4, turn, 0)

    @pl.when(step < ff_steps)
    def _():
        rows = rows_ref[...]
        gate = jnp.minimum(dot(rows, gate_ref[...]), CLAMP_LIMIT)
        up = jnp.clip(dot(rows, up_ref[...]), -CLAMP_LIMIT, CLAMP_LIMIT)
        hidden = gate / (1.0 + jnp.exp(-SWISH_SLOPE * gate)) * (up + 1.0)
        hidden_ref[step] = hidden.astype(BF16)

    @pl.when(step >= ff_steps)
    def _():
        total = dot(hidden_ref[0], down_ref[0:FF_BLOCK])
        for k in range(1, ff_steps):
            total = total + dot(hidden_ref[k], down_ref[k * FF_BLOCK : (k + 1) * FF_BLOCK])
        made_ref[step - ff_steps] = total.astype(BF16)

    @pl.when(step == pl.num_programs(0) - 1)
    def _():
        swap = swap_matrix()
        down_steps, _rows, width = made_ref.shape

        def stacked(start):
            pieces = []
            for d in range(down_steps):
                piece = made_ref[d, pl.ds(start, 16), :]
                pieces += [piece[:, j * C : (j + 1) * C] for j in range(width // C)]
            return jnp.concatenate(pieces, axis=0)

        def turn(i, carry):
            for k in range(2):
                start = pl.multiple_of((i * 4 + k * 2) * 16, 16)
                other = pl.multiple_of(start + 16, 16)
                turned = dot(swap, beside(stacked(start), stacked(other))).astype(BF16)
                out_ref[pl.ds(start, 16)] = turned[:, :C].reshape(16, tiles, C)
                out_ref[pl.ds(other, 16)] = turned[:, C:].reshape(16, tiles, C)
            return carry

        lax.fori_loop(0, groups // 4, turn, 0)


def expert(rows, gate_weight, up_weight, down_weight):
    slots_, tiles, _lanes = rows.shape
    features, hidden = gate_weight.shape
    ff_steps = hidden // FF_BLOCK
    width = 512
    down_steps = features // width
    return pl.pallas_call(
        expert_kernel,
        grid=(ff_steps + down_steps,),
        out_shape=jax.ShapeDtypeStruct(rows.shape, BF16),
        in_specs=[
            pl.BlockSpec(rows.shape, lambda i: (0, 0, 0), pipeline_mode=pl.Buffered(1)),
            pl.BlockSpec((features, FF_BLOCK), lambda i: (0, jnp.minimum(i, ff_steps - 1))),
            pl.BlockSpec((features, FF_BLOCK), lambda i: (0, jnp.minimum(i, ff_steps - 1))),
            pl.BlockSpec((hidden, width), lambda i: (0, jnp.maximum(i - ff_steps, 0))),
        ],
        out_specs=pl.BlockSpec(rows.shape, lambda i: (0, 0, 0), pipeline_mode=pl.Buffered(1)),
        scratch_shapes=[
            pltpu.VMEM((slots_, features), BF16),
            pltpu.VMEM((ff_steps, slots_, FF_BLOCK), BF16),
            pltpu.VMEM((down_steps, slots_, width), BF16),
        ],
        compiler_params=pltpu.CompilerParams(dimension_semantics=("arbitrary",)),
        cost_estimate=pl.CostEstimate(flops=10**10, bytes_accessed=2**24, transcendentals=0),
        name="expert",
    )(rows, gate_weight, up_weight, down_weight)


def combine_kernel(back_ref, normed_ref, gain_ref, dest_ref, weight_ref, out_ref, z_ref):
    tokens, tiles, _lanes = normed_ref.shape
    swap = swap_matrix()
    gain = gain_ref[...]

    def some(i, carry):
        for k in range(16):
            t = i * 16 + k
            total = normed_ref[t].astype(F32)
            for pick in range(4):
                at = pick * tokens + t
                total = total + weight_ref[at] * back_ref[dest_ref[at]].astype(F32)
            z_ref[t] = total
        return carry

    lax.fori_loop(0, tokens // 16, some, 0)

    def finish(i, carry):
        start = pl.multiple_of(i * 16, 16)
        z = z_ref[pl.ds(start, 16)].reshape(16 * tiles, C)
        high = z.astype(BF16)
        rest = z - high.astype(F32)
        middle = rest.astype(BF16)
        low = (rest - middle.astype(F32)).astype(BF16)
        turned = dot(swap, beside(high, middle))
        turned = turned[:, :C] + turned[:, C:] + dot(swap, low)
        total = jnp.concatenate([turned[j * 16 : (j + 1) * 16] for j in range(tiles)], axis=1)
        centred = total - jnp.mean(total, axis=1, keepdims=True)
        variance = jnp.mean(centred * centred, axis=1, keepdims=True)
        out_ref[0, pl.ds(start, 16), :] = centred * lax.rsqrt(variance + 1e-05) * gain
        return carry

    lax.fori_loop(0, tokens // 16, finish, 0, unroll=2)


def combine(back, normed, gain, dest, weight):
    tokens, tiles, _lanes = normed.shape
    return pl.pallas_call(
        combine_kernel,
        out_shape=jax.ShapeDtypeStruct((1, tokens, tiles * C), F32),
        in_specs=[VMEM] * 3 + [SMEM] * 2,
        out_specs=VMEM,
        scratch_shapes=[pltpu.VMEM((tokens, tiles, C), F32)],
        name="combine",
    )(back, normed, gain, dest, weight)


def gathered(block):
    y_size, core_size = lax.axis_size("dp_0"), lax.axis_size("dp_1")
    y, core = lax.axis_index("dp_0"), lax.axis_index("dp_1")
    found = [block]
    for shift in range(1, y_size):
        pairs = [(i, (i + shift) % y_size) for i in range(y_size)]
        found.append(lax.ppermute(block, "dp_0", pairs))
    places = [((y - shift) % y_size) * core_size + core for shift in range(y_size)]
    others = [((y - shift) % y_size) * core_size + 1 - core for shift in range(y_size)]
    return found, jnp.stack(places + others).astype(jnp.int32)


def per_device(
    residual,
    query,
    key,
    value,
    output_gate_input,
    write_strength_logit,
    decay_head_input,
    added_log_decay,
    head_decay_rate,
    head_norm_gain,
    output_projection,
    mixer_norm_gain,
    token_expert_index,
    token_expert_weight,
    expert_gate_weight,
    expert_up_weight,
    expert_down_weight,
    feedforward_norm_gain,
):
    experts = lax.axis_size(SP_DP)
    tokens, features = residual.shape[1:]
    picks = token_expert_index.shape[2]
    capacity = tokens * picks * 3 // (2 * experts)
    tiles = features // C
    found, places = gathered(output_projection)
    dest, source = slots(token_expert_index[0].T.reshape(-1), experts, capacity)
    keys, blocks = pack(
        query,
        key,
        value,
        write_strength_logit.transpose(0, 2, 1),
        decay_head_input.transpose(0, 2, 1),
    )
    keys = lax.all_to_all(keys, "sp", split_axis=0, concat_axis=0, tiled=True)
    blocks = lax.all_to_all(blocks, "sp", split_axis=0, concat_axis=0, tiled=True)
    parts = chunk_inverse(keys, added_log_decay.reshape(-1, C), head_decay_rate)
    recurrent = delta(keys, blocks, parts)
    recurrent, found = lax.optimization_barrier((recurrent, found))
    returned = lax.all_to_all(recurrent, "sp", split_axis=0, concat_axis=0, tiled=True)
    weights = found + [lax.ppermute(b, "dp_1", [(0, 1), (1, 0)]) for b in found]
    normed, rows = project(
        returned,
        output_gate_input,
        head_norm_gain.reshape(1, C),
        residual,
        mixer_norm_gain.reshape(1, features),
        source,
        places,
        weights,
    )
    rows = rows.reshape(experts, capacity * tiles, C)
    rows = lax.all_to_all(rows, SP_DP, split_axis=0, concat_axis=0, tiled=True)
    made = expert(
        rows.reshape(experts * capacity, tiles, C),
        expert_gate_weight[0],
        expert_up_weight[0],
        expert_down_weight[0],
    )
    made = made.reshape(experts, capacity * tiles, C)
    back = lax.all_to_all(made, SP_DP, split_axis=0, concat_axis=0, tiled=True)
    return combine(
        back.reshape(experts * capacity, tiles, C),
        normed,
        feedforward_norm_gain.reshape(1, features),
        dest,
        token_expert_weight[0].T.reshape(-1),
    )


def solution(mesh):
    torus = Mesh(mesh.devices.reshape(mesh.shape["sp"], 4, 2), ("sp", "dp_0", "dp_1"))
    return jax.shard_map(
        per_device,
        mesh=torus,
        in_specs=(
            P(DP, "sp", None),
            P(DP, "sp", None),
            P(DP, "sp", None),
            P(DP, "sp", None),
            P(DP, "sp", None),
            P(DP, "sp", None),
            P(DP, "sp", None),
            P(DP, "sp", None),
            P("sp"),
            P(),
            P(None, DP),
            P(),
            P(DP, "sp", None),
            P(DP, "sp", None),
            P(SP_DP, None, None),
            P(SP_DP, None, None),
            P(SP_DP, None, None),
            P(),
        ),
        out_specs=P(DP, "sp", None),
        check_vma=False,
    )
```

```python
import jax
import jax.numpy as jnp
from jax import lax
from jax.experimental import pallas as pl
from jax.experimental.pallas import tpu as pltpu
from jax.sharding import Mesh
from jax.sharding import PartitionSpec as P


DP = ("dp_0", "dp_1")
SP_DP = ("sp", "dp_0", "dp_1")
CLAMP_LIMIT = 7.0
SWISH_SLOPE = 1.702
F32 = jnp.float32
BF16 = jnp.bfloat16
HIGHEST = lax.Precision.HIGHEST
C = 128
EXTRA = 16
VMEM = pl.BlockSpec(memory_space=pltpu.VMEM)
SMEM = pl.BlockSpec(memory_space=pltpu.SMEM)
HBM = pl.BlockSpec(memory_space=pltpu.HBM)


def near(x):
    return pltpu.with_memory_space_constraint(x, pltpu.VMEM)


def far(x):
    return pltpu.with_memory_space_constraint(x, pltpu.HBM)


def dot(a, b):
    return jnp.dot(a, b, preferred_element_type=F32)


def dot_nt(a, b, precision=None):
    return lax.dot_general(
        a, b, (((1,), (1,)), ((), ())), precision=precision, preferred_element_type=F32
    )


def halves(x):
    high = x.astype(BF16)
    return high, (x - high.astype(F32)).astype(BF16)


def iotas(rows, columns):
    shape = (rows, columns)
    return lax.broadcasted_iota(jnp.int32, shape, 0), lax.broadcasted_iota(jnp.int32, shape, 1)


def swap_matrix():
    row, column = iotas(256, 256)
    return jnp.where((row % 16) * 16 + row // 16 == column, 1.0, 0.0).astype(BF16)


def pack_kernel(q_ref, k_ref, v_ref, logit_ref, decay_ref, key_out_ref, out_ref, sems):
    heads = out_ref.shape[0]
    copies = []
    for h in range(heads):
        columns = slice(h * C, (h + 1) * C)
        for source, target in (
            (k_ref, key_out_ref.at[h, 0:C]),
            (q_ref, out_ref.at[h, 0:C]),
            (v_ref, out_ref.at[h, C : 2 * C]),
        ):
            copy = pltpu.make_async_copy(source.at[0, :, columns], target, sems.at[len(copies)])
            copy.start()
            copies.append(copy)
    logits = logit_ref[0].astype(F32)
    decays = decay_ref[0].astype(F32)
    extra_row, _ = iotas(EXTRA, C)
    for h in range(heads):
        extra = jnp.where(extra_row == 0, logits[h : h + 1], decays[h : h + 1])
        key_out_ref[h, C : C + EXTRA] = extra.astype(BF16)
    for copy in copies:
        copy.wait()


def pack(query, key, value, logit, decay_input):
    heads = logit.shape[1]
    return pl.pallas_call(
        pack_kernel,
        out_shape=(
            jax.ShapeDtypeStruct((heads, C + EXTRA, C), BF16),
            jax.ShapeDtypeStruct((heads, 2 * C, C), BF16),
        ),
        in_specs=[HBM] * 3 + [VMEM] * 2,
        out_specs=(VMEM, VMEM),
        scratch_shapes=[pltpu.SemaphoreType.DMA((3 * heads,))],
        compiler_params=pltpu.CompilerParams(vmem_limit_bytes=12 * 2**20),
        name="pack",
    )(far(query), far(key), far(value), far(logit), far(decay_input))


GROUP = 4


def column_of(ref, n):
    lane = lax.broadcasted_iota(jnp.int32, ref.shape, 1)
    return jnp.sum(jnp.where(lane == n, ref[...], 0.0), axis=1, keepdims=True)


def beside(a, b):
    return jnp.concatenate([a, b], axis=1)


def above(a, b):
    return jnp.concatenate([a, b], axis=0)


def group_copies(pairs, sems, g):
    part = pl.ds(g * GROUP, GROUP)
    return [
        pltpu.make_async_copy(source.at[part], target.at[part], sems.at[k, g])
        for k, (source, target) in enumerate(pairs)
    ]


def inverse_kernel(
    x_ref, added_ref, rate_ref,
    base_hbm, weight_hbm, a_hbm, cum_col_ref, cum_row_ref, key_col_ref, key_row_ref,
    base_ref, weight_ref, a_ref, write_col_ref, write_row_ref, sems,
):
    pairs = ((base_ref, base_hbm), (weight_ref, weight_hbm), (a_ref, a_hbm))
    chunks = x_ref.shape[0]
    row, column = iotas(C, C)
    inclusive = row >= column
    strict = row > column
    diagonal = row == column

    chunk_row, _ = iotas(chunks, C)
    logits = jnp.zeros((chunks, C), F32)
    decays = jnp.zeros((chunks, C), F32)
    for n in range(chunks):
        extra = x_ref[n, C : C + EXTRA].astype(F32)
        logits = jnp.where(chunk_row == n, extra[0:1], logits)
        decays = jnp.where(chunk_row == n, extra[1:2], decays)
    softplus = jnp.maximum(decays, 0.0) + jnp.log(1.0 + jnp.exp(-jnp.abs(decays)))
    log_decay = added_ref[...] - rate_ref[0] * softplus
    upper = jnp.where(row <= column, 1.0, 0.0)
    lower = jnp.where(inclusive, 1.0, 0.0)
    eye = jnp.where(diagonal, 1.0, 0.0)
    cum_row_ref[...] = jnp.dot(log_decay, upper, precision=HIGHEST, preferred_element_type=F32)
    cum_col_ref[...] = dot_nt(lower, log_decay, precision=HIGHEST)
    write = 1.0 / (1.0 + jnp.exp(-logits))
    write_row_ref[...] = write
    write_col_ref[...] = dot_nt(eye, write, precision=HIGHEST)
    lane = lax.broadcasted_iota(jnp.int32, (C, chunks), 1)

    def group(g, key_columns):
        ns = [g * GROUP + k for k in range(GROUP)]
        keys = [x_ref[n, 0:C] for n in ns]
        products = [dot_nt(k, k) for k in keys]
        cum_c = [column_of(cum_col_ref, n) for n in ns]
        write_c = [column_of(write_col_ref, n) for n in ns]
        cum_r = [cum_row_ref[pl.ds(n, 1), :] for n in ns]
        write_r = [write_row_ref[pl.ds(n, 1), :] for n in ns]
        squares = [jnp.where(diagonal, p, 0.0) for p in products]
        key_c = [lax.rsqrt(jnp.sum(s, axis=1, keepdims=True) + 1e-06) for s in squares]
        key_r = [lax.rsqrt(jnp.sum(s, axis=0, keepdims=True) + 1e-06) for s in squares]
        for n, c, r in zip(ns, key_c, key_r):
            key_columns = jnp.where(lane == n, c, key_columns)
            key_row_ref[pl.ds(n, 1), :] = r
        lower_part = [
            jnp.where(
                strict,
                p * jnp.exp(jnp.where(inclusive, cc - cr, -jnp.inf)) * (wc * kc) * kr,
                0.0,
            )
            for p, cc, cr, wc, kc, kr in zip(products, cum_c, cum_r, write_c, key_c, key_r)
        ]

        left = [beside(*halves(part)) for part in lower_part]
        pair = (row // 2 == column // 2) & strict
        inverse = [jnp.where(pair, -part, eye) for part in lower_part]
        size = 2
        while size < C:
            highs = [i.astype(BF16) for i in inverse]
            first = [dot(f, above(h, h)) for f, h in zip(left, highs)]
            first = [above(*halves(f)) for f in first]
            second = [dot(beside(h, h), f) for h, f in zip(highs, first)]
            joined = (row // (2 * size) == column // (2 * size)) & (row // size > column // size)
            inverse = [jnp.where(joined, -s, i) for s, i in zip(second, inverse)]
            size *= 2

        for n, i, w in zip(ns, inverse, write_r):
            base_ref[n] = beside(*halves(i * w))
        weight = [
            beside(*halves(i * (w * jnp.exp(c) * k)))
            for i, w, c, k in zip(inverse, write_r, cum_r, key_r)
        ]
        weight = [dot(w, above(k, k)) for w, k in zip(weight, keys)]
        for n, w in zip(ns, weight):
            weight_ref[n] = w.astype(BF16)
        last = [c[C - 1 : C] for c in cum_c]
        carried = [
            above(*halves(w * (k * jnp.exp(end - c))))
            for w, k, end, c in zip(weight, key_c, last, cum_c)
        ]
        turned = [k.T for k in keys]
        update = [dot(beside(t, t), c) for t, c in zip(turned, carried)]
        for n, u, end in zip(ns, update, last):
            a_ref[n] = beside(*halves(jnp.where(diagonal, jnp.exp(end), 0.0) - u))
        for copy in group_copies(pairs, sems, g):
            copy.start()
        return key_columns

    key_col_ref[...] = lax.fori_loop(
        0, chunks // GROUP, group, jnp.zeros((C, chunks), F32)
    )
    for g in range(chunks // GROUP):
        for copy in group_copies(pairs, sems, g):
            copy.wait()


def chunk_inverse(blocks, added, decay_rate):
    chunks = blocks.shape[0]
    wide = pltpu.HBM((chunks, C, 2 * C), BF16)
    columns = jax.ShapeDtypeStruct((C, chunks), F32)
    rows = jax.ShapeDtypeStruct((chunks, C), F32)
    return pl.pallas_call(
        inverse_kernel,
        out_shape=(
            wide, pltpu.HBM((chunks, C, C), BF16), wide, columns, rows, columns, rows,
        ),
        in_specs=[VMEM, VMEM, SMEM],
        out_specs=(HBM,) * 3 + (VMEM,) * 4,
        scratch_shapes=[
            pltpu.VMEM((chunks, C, 2 * C), BF16),
            pltpu.VMEM((chunks, C, C), BF16),
            pltpu.VMEM((chunks, C, 2 * C), BF16),
            pltpu.VMEM((C, chunks), F32),
            pltpu.VMEM((chunks, C), F32),
            pltpu.SemaphoreType.DMA((3, chunks // GROUP)),
        ],
        compiler_params=pltpu.CompilerParams(vmem_limit_bytes=16 * 2**20),
        cost_estimate=pl.CostEstimate(flops=4 * 10**9, bytes_accessed=2**21, transcendentals=0),
        name="inverse",
    )(near(blocks), added, decay_rate)


def delta_kernel(
    key_hbm, x_ref, base_hbm, weight_hbm, a_hbm, cum_col_ref, cum_row_ref, key_col_ref,
    key_row_ref, out_ref, key_ref, base_ref, weight_ref, a_ref, b_ref, qe_ref, su_ref, sems,
):
    chunks = x_ref.shape[0]
    pairs = (
        (key_hbm, key_ref), (base_hbm, base_ref), (weight_hbm, weight_ref), (a_hbm, a_ref),
    )
    for g in range(chunks // GROUP):
        for copy in group_copies(pairs, sems, g):
            copy.start()
    row, column = iotas(C, C)
    inclusive = row >= column

    def prepare(g):
        for copy in group_copies(pairs, sems, g):
            copy.wait()
        ns = [g * GROUP + k for k in range(GROUP)]
        keys = [key_ref[n, 0:C] for n in ns]
        queries = [x_ref[n, 0:C] for n in ns]
        values = [x_ref[n, C : 2 * C] for n in ns]
        scores = [dot_nt(q, k) for q, k in zip(queries, keys)]
        base = [dot(base_ref[n], above(v, v)) for n, v in zip(ns, values)]
        cum_c = [column_of(cum_col_ref, n) for n in ns]
        key_c = [column_of(key_col_ref, n) for n in ns]
        cum_r = [cum_row_ref[pl.ds(n, 1), :] for n in ns]
        key_r = [key_row_ref[pl.ds(n, 1), :] for n in ns]
        q32 = [q.astype(F32) for q in queries]
        query_c = [
            lax.rsqrt(jnp.sum(q * q, axis=1, keepdims=True) + 1e-06) * C ** (-0.5) for q in q32
        ]
        scores = [
            s * jnp.exp(jnp.where(inclusive, cc - cr, -jnp.inf)) * kr * qc
            for s, cc, cr, kr, qc in zip(scores, cum_c, cum_r, key_r, query_c)
        ]
        carried = [
            above(*halves(b * (k * jnp.exp(c[C - 1 : C] - c))))
            for b, k, c in zip(base, key_c, cum_c)
        ]
        turned = [k.T for k in keys]
        update = [dot(beside(t, t), c) for t, c in zip(turned, carried)]
        both = [beside(b.astype(BF16), weight_ref[n]) for n, b in zip(ns, base)]
        seen = [dot(beside(*halves(s)), above(b, b)) for s, b in zip(scores, both)]
        for n, u, s, q, qc, c in zip(ns, update, seen, q32, query_c, cum_c):
            b_ref[n] = u
            su_ref[n] = s[:, :C]
            qe_ref[n] = beside(*halves(q * (qc * jnp.exp(c)) - s[:, C:]))

    def advance(g, state):
        for k in range(GROUP):
            n = g * GROUP + k
            high, low = halves(state)
            queries = qe_ref[n]
            out = dot(queries, above(high, high)) + su_ref[n]
            scale = lax.rsqrt(jnp.mean(out * out, axis=1, keepdims=True) + 1e-05)
            out_ref[n] = (out * scale).astype(BF16)
            a_high, a_low = a_ref[n, :, :C], a_ref[n, :, C:]
            state = dot(beside(a_high, a_high), above(high, low)) + dot(a_low, high) + b_ref[n]
        return state

    prepare(0)

    def step(g, state):
        state = advance(g - 1, state)
        prepare(g)
        return state

    state = lax.fori_loop(1, chunks // GROUP, step, jnp.zeros((C, C), F32))
    advance(chunks // GROUP - 1, state)


def delta(keys, blocks, parts):
    chunks = blocks.shape[0]
    return pl.pallas_call(
        delta_kernel,
        out_shape=jax.ShapeDtypeStruct((chunks, C, C), BF16),
        in_specs=[HBM, VMEM, HBM, HBM, HBM] + [VMEM] * 4,
        out_specs=VMEM,
        scratch_shapes=[
            pltpu.VMEM(keys.shape, BF16),
            pltpu.VMEM((chunks, C, 2 * C), BF16),
            pltpu.VMEM((chunks, C, C), BF16),
            pltpu.VMEM((chunks, C, 2 * C), BF16),
            pltpu.VMEM((chunks, C, C), F32),
            pltpu.VMEM((chunks, C, 2 * C), BF16),
            pltpu.VMEM((chunks, C, C), F32),
            pltpu.SemaphoreType.DMA((4, chunks // GROUP)),
        ],
        compiler_params=pltpu.CompilerParams(vmem_limit_bytes=16 * 2**20),
        cost_estimate=pl.CostEstimate(flops=4 * 10**9, bytes_accessed=2**21, transcendentals=0),
        name="delta",
    )(far(keys), near(blocks), *[far(p) for p in parts[:3]], *parts[3:])


def slots_kernel(index_ref, dest_ref, source_ref, count_ref):
    experts = count_ref.shape[0]
    capacity = source_ref.shape[0] // experts

    def clear(e, carry):
        count_ref[e] = 0
        for k in range(capacity):
            source_ref[e * capacity + k] = 0
        return carry

    lax.fori_loop(0, experts, clear, 0)

    tokens = index_ref.shape[0] // 4

    def place(t, carry):
        for k in range(4):
            at = k * tokens + t
            e = index_ref[at]
            used = count_ref[e]
            count_ref[e] = used + 1
            slot = e * capacity + used
            dest_ref[at] = slot
            source_ref[slot] = t
        return carry

    lax.fori_loop(0, tokens, place, 0)


def slots(index, experts, capacity):
    return pl.pallas_call(
        slots_kernel,
        out_shape=(
            jax.ShapeDtypeStruct(index.shape, jnp.int32),
            jax.ShapeDtypeStruct((experts * capacity,), jnp.int32),
        ),
        in_specs=[SMEM],
        out_specs=(SMEM, SMEM),
        scratch_shapes=[pltpu.SMEM((experts,), jnp.int32)],
        compiler_params=pltpu.CompilerParams(vmem_limit_bytes=2**20),
        name="slots",
    )(index)


def project_kernel(
    rec_ref, gate_hbm, head_gain_ref, residual_hbm, gain_ref, source_ref, place_ref,
    *rest,
):
    weight_refs = rest[:8]
    normed_ref, out_ref, gate_ref, residual_ref, gated_ref, mixed_ref, w_ref, sems = rest[8:]
    gate_copy = pltpu.make_async_copy(gate_hbm, gate_ref, sems.at[8])
    gate_copy.start()
    copies = [
        pltpu.make_async_copy(weight_refs[k], w_ref.at[k], sems.at[k]) for k in range(8)
    ]
    for copy in copies:
        copy.start()
    residual_copy = pltpu.make_async_copy(residual_hbm, residual_ref, sems.at[9])
    residual_copy.start()
    gate_copy.wait()
    heads = rec_ref.shape[0]
    head_gain = head_gain_ref[...]
    for h in range(heads):
        columns = slice(h * C, (h + 1) * C)
        gate = gate_ref[0, :, columns].astype(F32)
        gate = gate / (1.0 + jnp.exp(-gate))
        gated_ref[:, columns] = (rec_ref[h].astype(F32) * head_gain * gate).astype(BF16)
    for k in range(8):
        copies[k].wait()
        mixed_ref[place_ref[k]] = dot(gated_ref[...], w_ref[k])
    total = jnp.concatenate([mixed_ref[k] for k in range(8)], axis=1)
    residual_copy.wait()
    total = total + residual_ref[0].astype(F32)
    centred = total - jnp.mean(total, axis=1, keepdims=True)
    variance = jnp.mean(centred * centred, axis=1, keepdims=True)
    normed = (centred * lax.rsqrt(variance + 1e-05) * gain_ref[...]).astype(BF16)
    swap = swap_matrix()
    tiles = normed.shape[1] // C
    for g in range(normed.shape[0] // 16):
        rows = normed[g * 16 : (g + 1) * 16]
        stacked = jnp.concatenate([rows[:, j * C : (j + 1) * C] for j in range(tiles)], axis=0)
        turned = dot(swap, stacked).astype(BF16)
        normed_ref[g * 16 : (g + 1) * 16] = turned.reshape(16, tiles, C)

    def send(i, carry):
        for k in range(16):
            slot = i * 16 + k
            out_ref[slot] = normed_ref[source_ref[slot]]
        return carry

    lax.fori_loop(0, out_ref.shape[0] // 16, send, 0)


def project(recurrent, gate, head_gain, residual, gain, source, place, weights):
    tokens = residual.shape[1]
    features = residual.shape[2]
    tiles = features // C
    return pl.pallas_call(
        project_kernel,
        out_shape=(
            jax.ShapeDtypeStruct((tokens, tiles, C), BF16),
            jax.ShapeDtypeStruct((source.shape[0], tiles, C), BF16),
        ),
        in_specs=[VMEM, HBM, VMEM, HBM, VMEM] + [SMEM] * 2 + [HBM] * 8,
        out_specs=(VMEM, VMEM),
        scratch_shapes=[
            pltpu.VMEM((1, tokens, features), BF16),
            pltpu.VMEM((1, tokens, features), BF16),
            pltpu.VMEM((tokens, features), BF16),
            pltpu.VMEM((8, tokens, features // 8), F32),
            pltpu.VMEM((8, features, features // 8), BF16),
            pltpu.SemaphoreType.DMA((10,)),
        ],
        compiler_params=pltpu.CompilerParams(vmem_limit_bytes=24 * 2**20),
        cost_estimate=pl.CostEstimate(flops=10**9, bytes_accessed=2**24, transcendentals=0),
        name="project",
    )(
        near(recurrent), far(gate), head_gain, far(residual), gain, source, place,
        *[far(w) for w in weights],
    )


FF_BLOCK = 512
DOWN_ROWS = 384
TURN_UNROLL = 6


def expert_kernel(
    x_ref, gate_hbm, up_hbm, down_hbm, out_ref, gate_ref, up_ref, down_ref, rows_ref, hidden_ref,
    sems,
):
    slots_, tiles, _ = x_ref.shape
    copies = [
        pltpu.make_async_copy(source, target, sems.at[k])
        for k, (source, target) in enumerate(
            ((gate_hbm, gate_ref), (up_hbm, up_ref), (down_hbm, down_ref))
        )
    ]
    for copy in copies:
        copy.start()
    swap = swap_matrix()

    def turn(i, carry):
        for k in range(TURN_UNROLL):
            start = pl.multiple_of((i * TURN_UNROLL + k) * 32, 32)
            pieces = [x_ref[pl.ds(start + o, 16)].reshape(16 * tiles, C) for o in (0, 16)]
            turned = dot(swap, beside(*pieces)).astype(BF16)
            for j in range(tiles):
                part = turned[j * 16 : (j + 1) * 16]
                rows_ref[pl.ds(start, 16), j * C : (j + 1) * C] = part[:, :C]
                rows_ref[pl.ds(start + 16, 16), j * C : (j + 1) * C] = part[:, C:]
        return carry

    lax.fori_loop(0, slots_ // (32 * TURN_UNROLL), turn, 0)
    copies[0].wait()
    copies[1].wait()

    def widen(f, carry):
        columns = pl.ds(pl.multiple_of(f * FF_BLOCK, FF_BLOCK), FF_BLOCK)
        rows = rows_ref[...]
        gate = jnp.minimum(dot(rows, gate_ref[:, columns]), CLAMP_LIMIT)
        up = jnp.clip(dot(rows, up_ref[:, columns]), -CLAMP_LIMIT, CLAMP_LIMIT)
        hidden = gate / (1.0 + jnp.exp(-SWISH_SLOPE * gate)) * (up + 1.0)
        hidden_ref[:, columns] = hidden.astype(BF16)
        return carry

    lax.fori_loop(0, hidden_ref.shape[1] // FF_BLOCK, widen, 0)
    copies[2].wait()

    def narrow(i, carry):
        start = pl.multiple_of(i * DOWN_ROWS, DOWN_ROWS)
        made = dot(hidden_ref[pl.ds(start, DOWN_ROWS)], down_ref[...]).astype(BF16)
        for g in range(0, DOWN_ROWS, 32):
            stacked = [
                jnp.concatenate(
                    [made[k : k + 16, j * C : (j + 1) * C] for j in range(tiles)], axis=0
                )
                for k in (g, g + 16)
            ]
            turned = dot(swap, beside(*stacked)).astype(BF16)
            out_ref[pl.ds(start + g, 16)] = turned[:, :C].reshape(16, tiles, C)
            out_ref[pl.ds(start + g + 16, 16)] = turned[:, C:].reshape(16, tiles, C)
        return carry

    lax.fori_loop(0, slots_ // DOWN_ROWS, narrow, 0)


def expert(rows, gate_weight, up_weight, down_weight):
    slots_, _, _ = rows.shape
    features, hidden = gate_weight.shape
    return pl.pallas_call(
        expert_kernel,
        out_shape=jax.ShapeDtypeStruct(rows.shape, BF16),
        in_specs=[VMEM, HBM, HBM, HBM],
        out_specs=VMEM,
        scratch_shapes=[
            pltpu.VMEM(gate_weight.shape, BF16),
            pltpu.VMEM(up_weight.shape, BF16),
            pltpu.VMEM(down_weight.shape, BF16),
            pltpu.VMEM((slots_, features), BF16),
            pltpu.VMEM((slots_, hidden), BF16),
            pltpu.SemaphoreType.DMA((3,)),
        ],
        compiler_params=pltpu.CompilerParams(vmem_limit_bytes=36 * 2**20),
        cost_estimate=pl.CostEstimate(flops=10**10, bytes_accessed=2**24, transcendentals=0),
        name="expert",
    )(near(rows), far(gate_weight), far(up_weight), far(down_weight))


def combine_kernel(back_ref, normed_ref, gain_ref, dest_ref, weight_ref, out_ref, z_ref):
    tokens, tiles, _ = normed_ref.shape
    swap = swap_matrix()
    gain = gain_ref[...]

    def some(i, carry):
        for k in range(16):
            t = i * 16 + k
            total = normed_ref[t].astype(F32)
            for pick in range(4):
                at = pick * tokens + t
                total = total + weight_ref[at] * back_ref[dest_ref[at]].astype(F32)
            z_ref[t] = total
        return carry

    lax.fori_loop(0, tokens // 16, some, 0)

    def finish(i, carry):
        start = pl.multiple_of(i * 16, 16)
        z = z_ref[pl.ds(start, 16)].reshape(16 * tiles, C)
        high = z.astype(BF16)
        rest = z - high.astype(F32)
        middle = rest.astype(BF16)
        low = (rest - middle.astype(F32)).astype(BF16)
        turned = dot(swap, beside(high, middle))
        turned = turned[:, :C] + turned[:, C:] + dot(swap, low)
        total = jnp.concatenate([turned[j * 16 : (j + 1) * 16] for j in range(tiles)], axis=1)
        centred = total - jnp.mean(total, axis=1, keepdims=True)
        variance = jnp.mean(centred * centred, axis=1, keepdims=True)
        out_ref[0, pl.ds(start, 16), :] = centred * lax.rsqrt(variance + 1e-05) * gain
        return carry

    lax.fori_loop(0, tokens // 16, finish, 0, unroll=2)


def combine(back, normed, gain, dest, weight):
    tokens, tiles, _ = normed.shape
    return pl.pallas_call(
        combine_kernel,
        out_shape=jax.ShapeDtypeStruct((1, tokens, tiles * C), F32),
        in_specs=[VMEM] * 3 + [SMEM] * 2,
        out_specs=VMEM,
        scratch_shapes=[pltpu.VMEM((tokens, tiles, C), F32)],
        compiler_params=pltpu.CompilerParams(vmem_limit_bytes=12 * 2**20),
        name="combine",
    )(near(back), near(normed), gain, dest, weight)


def gathered(block):
    y_size, core_size = lax.axis_size("dp_0"), lax.axis_size("dp_1")
    y, core = lax.axis_index("dp_0"), lax.axis_index("dp_1")
    found = [block]
    for shift in range(1, y_size):
        pairs = [(i, (i + shift) % y_size) for i in range(y_size)]
        found.append(lax.ppermute(block, "dp_0", pairs))
    places = [((y - shift) % y_size) * core_size + core for shift in range(y_size)]
    others = [((y - shift) % y_size) * core_size + 1 - core for shift in range(y_size)]
    return found, jnp.stack(places + others).astype(jnp.int32)


def layer(
    residual,
    query,
    key,
    value,
    output_gate_input,
    write_strength_logit,
    decay_head_input,
    added_log_decay,
    head_decay_rate,
    head_norm_gain,
    output_projection,
    mixer_norm_gain,
    token_expert_index,
    token_expert_weight,
    expert_gate_weight,
    expert_up_weight,
    expert_down_weight,
    feedforward_norm_gain,
):
    experts = lax.axis_size(SP_DP)
    tokens, features = residual.shape[1:]
    picks = token_expert_index.shape[2]
    capacity = tokens * picks * 3 // (2 * experts)
    tiles = features // C
    found, places = gathered(output_projection)
    dest, source = slots(token_expert_index[0].T.reshape(-1), experts, capacity)
    keys, blocks = pack(
        query,
        key,
        value,
        write_strength_logit.transpose(0, 2, 1),
        decay_head_input.transpose(0, 2, 1),
    )
    keys = lax.all_to_all(keys, "sp", split_axis=0, concat_axis=0, tiled=True)
    blocks = lax.all_to_all(blocks, "sp", split_axis=0, concat_axis=0, tiled=True)
    parts = chunk_inverse(keys, added_log_decay.reshape(-1, C), head_decay_rate)
    recurrent = delta(keys, blocks, parts)
    recurrent, found = lax.optimization_barrier((recurrent, found))
    returned = lax.all_to_all(recurrent, "sp", split_axis=0, concat_axis=0, tiled=True)
    weights = list(found)
    for b in found:
        weights.append(lax.ppermute(b, "dp_1", [(0, 1), (1, 0)]))
    normed, rows = project(
        returned,
        output_gate_input,
        head_norm_gain.reshape(1, C),
        residual,
        mixer_norm_gain.reshape(1, features),
        source,
        places,
        weights,
    )
    rows = rows.reshape(experts, capacity * tiles, C)
    rows = lax.all_to_all(rows, SP_DP, split_axis=0, concat_axis=0, tiled=True)
    made = expert(
        rows.reshape(experts * capacity, tiles, C),
        expert_gate_weight[0],
        expert_up_weight[0],
        expert_down_weight[0],
    )
    made = made.reshape(experts, capacity * tiles, C)
    back = lax.all_to_all(made, SP_DP, split_axis=0, concat_axis=0, tiled=True)
    return combine(
        back.reshape(experts * capacity, tiles, C),
        normed,
        feedforward_norm_gain.reshape(1, features),
        dest,
        token_expert_weight[0].T.reshape(-1),
    )


def solution(mesh):
    torus = Mesh(mesh.devices.reshape(mesh.shape["sp"], 4, 2), ("sp", "dp_0", "dp_1"))
    return jax.shard_map(
        layer,
        mesh=torus,
        in_specs=(
            P(DP, "sp", None),
            P(DP, "sp", None),
            P(DP, "sp", None),
            P(DP, "sp", None),
            P(DP, "sp", None),
            P(DP, "sp", None),
            P(DP, "sp", None),
            P(DP, "sp", None),
            P("sp"),
            P(),
            P(None, DP),
            P(),
            P(DP, "sp", None),
            P(DP, "sp", None),
            P(SP_DP, None, None),
            P(SP_DP, None, None),
            P(SP_DP, None, None),
            P(),
        ),
        out_specs=P(DP, "sp", None),
        check_vma=False,
    )
```

```python
import jax
import jax.numpy as jnp
from jax import lax
from jax.experimental import pallas as pl
from jax.experimental.pallas import tpu as pltpu
from jax.sharding import Mesh
from jax.sharding import PartitionSpec as P


DP = ("dp_0", "dp_1")
SP_DP = ("sp", "dp_0", "dp_1")
CLAMP_LIMIT = 7.0
SWISH_SLOPE = 1.702
F32 = jnp.float32
BF16 = jnp.bfloat16
HIGHEST = lax.Precision.HIGHEST
C = 128
EXTRA = 16
VMEM = pl.BlockSpec(memory_space=pltpu.VMEM)
SMEM = pl.BlockSpec(memory_space=pltpu.SMEM)
HBM = pl.BlockSpec(memory_space=pltpu.HBM)


def near(x):
    return pltpu.with_memory_space_constraint(x, pltpu.VMEM)


def far(x):
    return pltpu.with_memory_space_constraint(x, pltpu.HBM)


def dot(a, b):
    return jnp.dot(a, b, preferred_element_type=F32)


def dot_nt(a, b, precision=None):
    return lax.dot_general(
        a, b, (((1,), (1,)), ((), ())), precision=precision, preferred_element_type=F32
    )


def halves(x):
    high = x.astype(BF16)
    return high, (x - high.astype(F32)).astype(BF16)


def iotas(rows, columns):
    shape = (rows, columns)
    return lax.broadcasted_iota(jnp.int32, shape, 0), lax.broadcasted_iota(jnp.int32, shape, 1)


def swap_matrix():
    row, column = iotas(256, 256)
    return jnp.where((row % 16) * 16 + row // 16 == column, 1.0, 0.0).astype(BF16)


def pack_kernel(q_ref, k_ref, v_ref, logit_ref, decay_ref, out_ref, sems):
    heads = out_ref.shape[0]
    copies = []
    for h in range(heads):
        columns = slice(h * C, (h + 1) * C)
        for k, source in enumerate((k_ref, q_ref, v_ref)):
            copy = pltpu.make_async_copy(
                source.at[0, :, columns],
                out_ref.at[h, k * C : (k + 1) * C],
                sems.at[len(copies)],
            )
            copy.start()
            copies.append(copy)
    logits = logit_ref[0].astype(F32)
    decays = decay_ref[0].astype(F32)
    extra_row, _ = iotas(EXTRA, C)
    for h in range(heads):
        extra = jnp.where(extra_row == 0, logits[h : h + 1], decays[h : h + 1])
        out_ref[h, 3 * C : 3 * C + EXTRA] = extra.astype(BF16)
    for copy in copies:
        copy.wait()


def pack(query, key, value, logit, decay_input):
    heads = logit.shape[1]
    return pl.pallas_call(
        pack_kernel,
        out_shape=jax.ShapeDtypeStruct((heads, 3 * C + EXTRA, C), BF16),
        in_specs=[HBM] * 3 + [VMEM] * 2,
        out_specs=VMEM,
        scratch_shapes=[pltpu.SemaphoreType.DMA((3 * heads,))],
        compiler_params=pltpu.CompilerParams(vmem_limit_bytes=12 * 2**20),
        name="pack",
    )(far(query), far(key), far(value), far(logit), far(decay_input))


GROUP = 8


def column_of(ref, n):
    lane = lax.broadcasted_iota(jnp.int32, ref.shape, 1)
    return jnp.sum(jnp.where(lane == n, ref[...], 0.0), axis=1, keepdims=True)


def beside(a, b):
    return jnp.concatenate([a, b], axis=1)


def above(a, b):
    return jnp.concatenate([a, b], axis=0)


def recurrence_kernel(
    x_ref, added_ref, rate_ref, out_ref, base_ref, weight_ref, a_ref, b_ref, qe_ref, su_ref,
    cum_col_ref, cum_row_ref, key_col_ref, key_row_ref, write_col_ref, write_row_ref,
):
    inverse_part(
        x_ref, added_ref, rate_ref, base_ref, weight_ref, a_ref,
        cum_col_ref, cum_row_ref, key_col_ref, key_row_ref, write_col_ref, write_row_ref,
    )
    delta_part(
        x_ref, base_ref, weight_ref, a_ref, cum_col_ref, cum_row_ref, key_col_ref, key_row_ref,
        out_ref, b_ref, qe_ref, su_ref,
    )


def inverse_part(
    x_ref, added_ref, rate_ref, base_ref, weight_ref, a_ref,
    cum_col_ref, cum_row_ref, key_col_ref, key_row_ref, write_col_ref, write_row_ref,
):
    chunks = x_ref.shape[0]
    row, column = iotas(C, C)
    inclusive = row >= column
    strict = row > column
    diagonal = row == column

    chunk_row, _ = iotas(chunks, C)
    logits = jnp.zeros((chunks, C), F32)
    decays = jnp.zeros((chunks, C), F32)
    for n in range(chunks):
        extra = x_ref[n, 3 * C : 3 * C + EXTRA].astype(F32)
        logits = jnp.where(chunk_row == n, extra[0:1], logits)
        decays = jnp.where(chunk_row == n, extra[1:2], decays)
    softplus = jnp.maximum(decays, 0.0) + jnp.log(1.0 + jnp.exp(-jnp.abs(decays)))
    log_decay = added_ref[...] - rate_ref[0] * softplus
    upper = jnp.where(row <= column, 1.0, 0.0)
    lower = jnp.where(inclusive, 1.0, 0.0)
    eye = jnp.where(diagonal, 1.0, 0.0)
    cum_row_ref[...] = jnp.dot(log_decay, upper, precision=HIGHEST, preferred_element_type=F32)
    cum_col_ref[...] = dot_nt(lower, log_decay, precision=HIGHEST)
    write = 1.0 / (1.0 + jnp.exp(-logits))
    write_row_ref[...] = write
    write_col_ref[...] = dot_nt(eye, write, precision=HIGHEST)
    lane = lax.broadcasted_iota(jnp.int32, (C, chunks), 1)

    def group(g, key_columns):
        ns = [g * GROUP + k for k in range(GROUP)]
        keys = [x_ref[n, 0:C] for n in ns]
        products = [dot_nt(k, k) for k in keys]
        cum_c = [column_of(cum_col_ref, n) for n in ns]
        write_c = [column_of(write_col_ref, n) for n in ns]
        cum_r = [cum_row_ref[pl.ds(n, 1), :] for n in ns]
        write_r = [write_row_ref[pl.ds(n, 1), :] for n in ns]
        squares = [jnp.where(diagonal, p, 0.0) for p in products]
        key_c = [lax.rsqrt(jnp.sum(s, axis=1, keepdims=True) + 1e-06) for s in squares]
        key_r = [lax.rsqrt(jnp.sum(s, axis=0, keepdims=True) + 1e-06) for s in squares]
        for n, c, r in zip(ns, key_c, key_r):
            key_columns = jnp.where(lane == n, c, key_columns)
            key_row_ref[pl.ds(n, 1), :] = r
        lower_part = [
            jnp.where(
                strict,
                p * jnp.exp(jnp.where(inclusive, cc - cr, -jnp.inf)) * (wc * kc) * kr,
                0.0,
            )
            for p, cc, cr, wc, kc, kr in zip(products, cum_c, cum_r, write_c, key_c, key_r)
        ]

        left = [beside(*halves(part)) for part in lower_part]
        pair = (row // 2 == column // 2) & strict
        inverse = [jnp.where(pair, -part, eye) for part in lower_part]
        size = 2
        while size < C:
            highs = [i.astype(BF16) for i in inverse]
            first = [dot(f, above(h, h)) for f, h in zip(left, highs)]
            first = [above(*halves(f)) for f in first]
            second = [dot(beside(h, h), f) for h, f in zip(highs, first)]
            joined = (row // (2 * size) == column // (2 * size)) & (row // size > column // size)
            inverse = [jnp.where(joined, -s, i) for s, i in zip(second, inverse)]
            size *= 2

        for n, i, w in zip(ns, inverse, write_r):
            base_ref[n] = beside(*halves(i * w))
        weight = [
            beside(*halves(i * (w * jnp.exp(c) * k)))
            for i, w, c, k in zip(inverse, write_r, cum_r, key_r)
        ]
        weight = [dot(w, above(k, k)) for w, k in zip(weight, keys)]
        for n, w in zip(ns, weight):
            weight_ref[n] = w.astype(BF16)
        last = [c[C - 1 : C] for c in cum_c]
        carried = [
            above(*halves(w * (k * jnp.exp(end - c))))
            for w, k, end, c in zip(weight, key_c, last, cum_c)
        ]
        turned = [k.T for k in keys]
        update = [dot(beside(t, t), c) for t, c in zip(turned, carried)]
        for n, u, end in zip(ns, update, last):
            a_ref[n] = beside(*halves(jnp.where(diagonal, jnp.exp(end), 0.0) - u))
        return key_columns

    key_col_ref[...] = lax.fori_loop(
        0, chunks // GROUP, group, jnp.zeros((C, chunks), F32)
    )


def delta_part(
    x_ref, base_ref, weight_ref, a_ref, cum_col_ref, cum_row_ref, key_col_ref, key_row_ref,
    out_ref, b_ref, qe_ref, su_ref,
):
    chunks = x_ref.shape[0]
    row, column = iotas(C, C)
    inclusive = row >= column

    def prepare(g):
        ns = [g * GROUP + k for k in range(GROUP)]
        keys = [x_ref[n, 0:C] for n in ns]
        queries = [x_ref[n, C : 2 * C] for n in ns]
        values = [x_ref[n, 2 * C : 3 * C] for n in ns]
        scores = [dot_nt(q, k) for q, k in zip(queries, keys)]
        base = [dot(base_ref[n], above(v, v)) for n, v in zip(ns, values)]
        cum_c = [column_of(cum_col_ref, n) for n in ns]
        key_c = [column_of(key_col_ref, n) for n in ns]
        cum_r = [cum_row_ref[pl.ds(n, 1), :] for n in ns]
        key_r = [key_row_ref[pl.ds(n, 1), :] for n in ns]
        q32 = [q.astype(F32) for q in queries]
        query_c = [
            lax.rsqrt(jnp.sum(q * q, axis=1, keepdims=True) + 1e-06) * C ** (-0.5) for q in q32
        ]
        scores = [
            s * jnp.exp(jnp.where(inclusive, cc - cr, -jnp.inf)) * kr * qc
            for s, cc, cr, kr, qc in zip(scores, cum_c, cum_r, key_r, query_c)
        ]
        carried = [
            above(*halves(b * (k * jnp.exp(c[C - 1 : C] - c))))
            for b, k, c in zip(base, key_c, cum_c)
        ]
        turned = [k.T for k in keys]
        update = [dot(beside(t, t), c) for t, c in zip(turned, carried)]
        both = [beside(b.astype(BF16), weight_ref[n]) for n, b in zip(ns, base)]
        seen = [dot(beside(*halves(s)), above(b, b)) for s, b in zip(scores, both)]
        for n, u, s, q, qc, c in zip(ns, update, seen, q32, query_c, cum_c):
            b_ref[n] = u
            su_ref[n] = s[:, :C]
            qe_ref[n] = beside(*halves(q * (qc * jnp.exp(c)) - s[:, C:]))

    def advance(g, state):
        for k in range(GROUP):
            n = g * GROUP + k
            high, low = halves(state)
            queries = qe_ref[n]
            out = dot(queries, above(high, high)) + su_ref[n]
            scale = lax.rsqrt(jnp.mean(out * out, axis=1, keepdims=True) + 1e-05)
            out_ref[n] = (out * scale).astype(BF16)
            a_high, a_low = a_ref[n, :, :C], a_ref[n, :, C:]
            state = dot(beside(a_high, a_high), above(high, low)) + dot(a_low, high) + b_ref[n]
        return state

    prepare(0)

    def step(g, state):
        state = advance(g - 1, state)
        prepare(g)
        return state

    state = lax.fori_loop(1, chunks // GROUP, step, jnp.zeros((C, C), F32))
    advance(chunks // GROUP - 1, state)


def recurrence(blocks, added, decay_rate):
    chunks = blocks.shape[0]
    square = pltpu.VMEM((chunks, C, C), F32)
    wide = pltpu.VMEM((chunks, C, 2 * C), BF16)
    columns = pltpu.VMEM((C, chunks), F32)
    rows = pltpu.VMEM((chunks, C), F32)
    return pl.pallas_call(
        recurrence_kernel,
        out_shape=jax.ShapeDtypeStruct((chunks, C, C), BF16),
        in_specs=[VMEM, VMEM, SMEM],
        out_specs=VMEM,
        scratch_shapes=[
            wide, pltpu.VMEM((chunks, C, C), BF16), wide, square, wide, square,
            columns, rows, columns, rows, columns, rows,
        ],
        compiler_params=pltpu.CompilerParams(vmem_limit_bytes=24 * 2**20),
        cost_estimate=pl.CostEstimate(flops=8 * 10**9, bytes_accessed=2**21, transcendentals=0),
        name="recurrence",
    )(near(blocks), added, decay_rate)


def slots_kernel(index_ref, dest_ref, source_ref, count_ref):
    experts = count_ref.shape[0]
    capacity = source_ref.shape[0] // experts

    def clear(e, carry):
        count_ref[e] = 0
        for k in range(capacity):
            source_ref[e * capacity + k] = 0
        return carry

    lax.fori_loop(0, experts, clear, 0)

    tokens = index_ref.shape[0] // 4

    def place(t, carry):
        for k in range(4):
            at = k * tokens + t
            e = index_ref[at]
            used = count_ref[e]
            count_ref[e] = used + 1
            slot = e * capacity + used
            dest_ref[at] = slot
            source_ref[slot] = t
        return carry

    lax.fori_loop(0, tokens, place, 0)


def slots(index, experts, capacity):
    return pl.pallas_call(
        slots_kernel,
        out_shape=(
            jax.ShapeDtypeStruct(index.shape, jnp.int32),
            jax.ShapeDtypeStruct((experts * capacity,), jnp.int32),
        ),
        in_specs=[SMEM],
        out_specs=(SMEM, SMEM),
        scratch_shapes=[pltpu.SMEM((experts,), jnp.int32)],
        compiler_params=pltpu.CompilerParams(vmem_limit_bytes=2**20),
        name="slots",
    )(index)


def project_kernel(
    rec_ref, gate_hbm, head_gain_ref, residual_hbm, gain_ref, source_ref, place_ref,
    *rest,
):
    weight_refs = rest[:8]
    normed_ref, out_ref, gate_ref, residual_ref, gated_ref, mixed_ref, w_ref, sems = rest[8:]
    gate_copy = pltpu.make_async_copy(gate_hbm, gate_ref, sems.at[8])
    gate_copy.start()
    copies = [
        pltpu.make_async_copy(weight_refs[k], w_ref.at[k], sems.at[k]) for k in range(8)
    ]
    for copy in copies:
        copy.start()
    residual_copy = pltpu.make_async_copy(residual_hbm, residual_ref, sems.at[9])
    residual_copy.start()
    gate_copy.wait()
    heads = rec_ref.shape[0]
    head_gain = head_gain_ref[...]
    for h in range(heads):
        columns = slice(h * C, (h + 1) * C)
        gate = gate_ref[0, :, columns].astype(F32)
        gate = gate / (1.0 + jnp.exp(-gate))
        gated_ref[:, columns] = (rec_ref[h].astype(F32) * head_gain * gate).astype(BF16)
    for k in range(8):
        copies[k].wait()
        mixed_ref[place_ref[k]] = dot(gated_ref[...], w_ref[k])
    total = jnp.concatenate([mixed_ref[k] for k in range(8)], axis=1)
    residual_copy.wait()
    total = total + residual_ref[0].astype(F32)
    centred = total - jnp.mean(total, axis=1, keepdims=True)
    variance = jnp.mean(centred * centred, axis=1, keepdims=True)
    normed = (centred * lax.rsqrt(variance + 1e-05) * gain_ref[...]).astype(BF16)
    swap = swap_matrix()
    tiles = normed.shape[1] // C
    for g in range(normed.shape[0] // 16):
        rows = normed[g * 16 : (g + 1) * 16]
        stacked = jnp.concatenate([rows[:, j * C : (j + 1) * C] for j in range(tiles)], axis=0)
        turned = dot(swap, stacked).astype(BF16)
        normed_ref[g * 16 : (g + 1) * 16] = turned.reshape(16, tiles, C)

    def send(i, carry):
        for k in range(16):
            slot = i * 16 + k
            out_ref[slot] = normed_ref[source_ref[slot]]
        return carry

    lax.fori_loop(0, out_ref.shape[0] // 16, send, 0)


def project(recurrent, gate, head_gain, residual, gain, source, place, weights):
    tokens = residual.shape[1]
    features = residual.shape[2]
    tiles = features // C
    return pl.pallas_call(
        project_kernel,
        out_shape=(
            jax.ShapeDtypeStruct((tokens, tiles, C), BF16),
            jax.ShapeDtypeStruct((source.shape[0], tiles, C), BF16),
        ),
        in_specs=[VMEM, HBM, VMEM, HBM, VMEM] + [SMEM] * 2 + [HBM] * 8,
        out_specs=(VMEM, VMEM),
        scratch_shapes=[
            pltpu.VMEM((1, tokens, features), BF16),
            pltpu.VMEM((1, tokens, features), BF16),
            pltpu.VMEM((tokens, features), BF16),
            pltpu.VMEM((8, tokens, features // 8), F32),
            pltpu.VMEM((8, features, features // 8), BF16),
            pltpu.SemaphoreType.DMA((10,)),
        ],
        compiler_params=pltpu.CompilerParams(vmem_limit_bytes=24 * 2**20),
        cost_estimate=pl.CostEstimate(flops=10**9, bytes_accessed=2**24, transcendentals=0),
        name="project",
    )(
        near(recurrent), far(gate), head_gain, far(residual), gain, source, place,
        *[far(w) for w in weights],
    )


FF_BLOCK = 512
DOWN_ROWS = 384
TURN_UNROLL = 6


def expert_kernel(
    x_ref, gate_hbm, up_hbm, down_hbm, out_ref, gate_ref, up_ref, down_ref, rows_ref, hidden_ref,
    sems,
):
    slots_, tiles, _ = x_ref.shape
    copies = [
        pltpu.make_async_copy(source, target, sems.at[k])
        for k, (source, target) in enumerate(
            ((gate_hbm, gate_ref), (up_hbm, up_ref), (down_hbm, down_ref))
        )
    ]
    for copy in copies:
        copy.start()
    swap = swap_matrix()

    def turn(i, carry):
        for k in range(TURN_UNROLL):
            start = pl.multiple_of((i * TURN_UNROLL + k) * 32, 32)
            pieces = [x_ref[pl.ds(start + o, 16)].reshape(16 * tiles, C) for o in (0, 16)]
            turned = dot(swap, beside(*pieces)).astype(BF16)
            for j in range(tiles):
                part = turned[j * 16 : (j + 1) * 16]
                rows_ref[pl.ds(start, 16), j * C : (j + 1) * C] = part[:, :C]
                rows_ref[pl.ds(start + 16, 16), j * C : (j + 1) * C] = part[:, C:]
        return carry

    lax.fori_loop(0, slots_ // (32 * TURN_UNROLL), turn, 0)
    copies[0].wait()
    copies[1].wait()

    def widen(f, carry):
        columns = pl.ds(pl.multiple_of(f * FF_BLOCK, FF_BLOCK), FF_BLOCK)
        rows = rows_ref[...]
        gate = jnp.minimum(dot(rows, gate_ref[:, columns]), CLAMP_LIMIT)
        up = jnp.clip(dot(rows, up_ref[:, columns]), -CLAMP_LIMIT, CLAMP_LIMIT)
        hidden = gate / (1.0 + jnp.exp(-SWISH_SLOPE * gate)) * (up + 1.0)
        hidden_ref[:, columns] = hidden.astype(BF16)
        return carry

    lax.fori_loop(0, hidden_ref.shape[1] // FF_BLOCK, widen, 0)
    copies[2].wait()

    def narrow(i, carry):
        start = pl.multiple_of(i * DOWN_ROWS, DOWN_ROWS)
        made = dot(hidden_ref[pl.ds(start, DOWN_ROWS)], down_ref[...]).astype(BF16)
        for g in range(0, DOWN_ROWS, 32):
            stacked = [
                jnp.concatenate(
                    [made[k : k + 16, j * C : (j + 1) * C] for j in range(tiles)], axis=0
                )
                for k in (g, g + 16)
            ]
            turned = dot(swap, beside(*stacked)).astype(BF16)
            out_ref[pl.ds(start + g, 16)] = turned[:, :C].reshape(16, tiles, C)
            out_ref[pl.ds(start + g + 16, 16)] = turned[:, C:].reshape(16, tiles, C)
        return carry

    lax.fori_loop(0, slots_ // DOWN_ROWS, narrow, 0)


def expert(rows, gate_weight, up_weight, down_weight):
    slots_, _, _ = rows.shape
    features, hidden = gate_weight.shape
    return pl.pallas_call(
        expert_kernel,
        out_shape=jax.ShapeDtypeStruct(rows.shape, BF16),
        in_specs=[VMEM, HBM, HBM, HBM],
        out_specs=VMEM,
        scratch_shapes=[
            pltpu.VMEM(gate_weight.shape, BF16),
            pltpu.VMEM(up_weight.shape, BF16),
            pltpu.VMEM(down_weight.shape, BF16),
            pltpu.VMEM((slots_, features), BF16),
            pltpu.VMEM((slots_, hidden), BF16),
            pltpu.SemaphoreType.DMA((3,)),
        ],
        compiler_params=pltpu.CompilerParams(vmem_limit_bytes=36 * 2**20),
        cost_estimate=pl.CostEstimate(flops=10**10, bytes_accessed=2**24, transcendentals=0),
        name="expert",
    )(near(rows), far(gate_weight), far(up_weight), far(down_weight))


def combine_kernel(back_ref, normed_ref, gain_ref, dest_ref, weight_ref, out_ref, z_ref):
    tokens, tiles, _ = normed_ref.shape
    swap = swap_matrix()
    gain = gain_ref[...]

    def some(i, carry):
        for k in range(16):
            t = i * 16 + k
            total = normed_ref[t].astype(F32)
            for pick in range(4):
                at = pick * tokens + t
                total = total + weight_ref[at] * back_ref[dest_ref[at]].astype(F32)
            z_ref[t] = total
        return carry

    lax.fori_loop(0, tokens // 16, some, 0)

    def finish(i, carry):
        start = pl.multiple_of(i * 16, 16)
        z = z_ref[pl.ds(start, 16)].reshape(16 * tiles, C)
        high = z.astype(BF16)
        rest = z - high.astype(F32)
        middle = rest.astype(BF16)
        low = (rest - middle.astype(F32)).astype(BF16)
        turned = dot(swap, beside(high, middle))
        turned = turned[:, :C] + turned[:, C:] + dot(swap, low)
        total = jnp.concatenate([turned[j * 16 : (j + 1) * 16] for j in range(tiles)], axis=1)
        centred = total - jnp.mean(total, axis=1, keepdims=True)
        variance = jnp.mean(centred * centred, axis=1, keepdims=True)
        out_ref[0, pl.ds(start, 16), :] = centred * lax.rsqrt(variance + 1e-05) * gain
        return carry

    lax.fori_loop(0, tokens // 16, finish, 0, unroll=2)


def combine(back, normed, gain, dest, weight):
    tokens, tiles, _ = normed.shape
    return pl.pallas_call(
        combine_kernel,
        out_shape=jax.ShapeDtypeStruct((1, tokens, tiles * C), F32),
        in_specs=[VMEM] * 3 + [SMEM] * 2,
        out_specs=VMEM,
        scratch_shapes=[pltpu.VMEM((tokens, tiles, C), F32)],
        compiler_params=pltpu.CompilerParams(vmem_limit_bytes=12 * 2**20),
        name="combine",
    )(near(back), near(normed), gain, dest, weight)


def gathered(block):
    y_size, core_size = lax.axis_size("dp_0"), lax.axis_size("dp_1")
    y, core = lax.axis_index("dp_0"), lax.axis_index("dp_1")
    found = [block]
    for shift in range(1, y_size):
        pairs = [(i, (i + shift) % y_size) for i in range(y_size)]
        found.append(lax.ppermute(block, "dp_0", pairs))
    places = [((y - shift) % y_size) * core_size + core for shift in range(y_size)]
    others = [((y - shift) % y_size) * core_size + 1 - core for shift in range(y_size)]
    return found, jnp.stack(places + others).astype(jnp.int32)


def layer(
    residual,
    query,
    key,
    value,
    output_gate_input,
    write_strength_logit,
    decay_head_input,
    added_log_decay,
    head_decay_rate,
    head_norm_gain,
    output_projection,
    mixer_norm_gain,
    token_expert_index,
    token_expert_weight,
    expert_gate_weight,
    expert_up_weight,
    expert_down_weight,
    feedforward_norm_gain,
):
    experts = lax.axis_size(SP_DP)
    tokens, features = residual.shape[1:]
    picks = token_expert_index.shape[2]
    capacity = tokens * picks * 3 // (2 * experts)
    tiles = features // C
    found, places = gathered(output_projection)
    dest, source = slots(token_expert_index[0].T.reshape(-1), experts, capacity)
    blocks = pack(
        query,
        key,
        value,
        write_strength_logit.transpose(0, 2, 1),
        decay_head_input.transpose(0, 2, 1),
    )
    blocks = lax.all_to_all(blocks, "sp", split_axis=0, concat_axis=0, tiled=True)
    recurrent = recurrence(blocks, added_log_decay.reshape(-1, C), head_decay_rate)
    recurrent, found = lax.optimization_barrier((recurrent, found))
    returned = lax.all_to_all(recurrent, "sp", split_axis=0, concat_axis=0, tiled=True)
    weights = list(found)
    for b in found:
        weights.append(lax.ppermute(b, "dp_1", [(0, 1), (1, 0)]))
    normed, rows = project(
        returned,
        output_gate_input,
        head_norm_gain.reshape(1, C),
        residual,
        mixer_norm_gain.reshape(1, features),
        source,
        places,
        weights,
    )
    rows = rows.reshape(experts, capacity * tiles, C)
    rows = lax.all_to_all(rows, SP_DP, split_axis=0, concat_axis=0, tiled=True)
    made = expert(
        rows.reshape(experts * capacity, tiles, C),
        expert_gate_weight[0],
        expert_up_weight[0],
        expert_down_weight[0],
    )
    made = made.reshape(experts, capacity * tiles, C)
    back = lax.all_to_all(made, SP_DP, split_axis=0, concat_axis=0, tiled=True)
    return combine(
        back.reshape(experts * capacity, tiles, C),
        normed,
        feedforward_norm_gain.reshape(1, features),
        dest,
        token_expert_weight[0].T.reshape(-1),
    )


def solution(mesh):
    torus = Mesh(mesh.devices.reshape(mesh.shape["sp"], 4, 2), ("sp", "dp_0", "dp_1"))
    return jax.shard_map(
        layer,
        mesh=torus,
        in_specs=(
            P(DP, "sp", None),
            P(DP, "sp", None),
            P(DP, "sp", None),
            P(DP, "sp", None),
            P(DP, "sp", None),
            P(DP, "sp", None),
            P(DP, "sp", None),
            P(DP, "sp", None),
            P("sp"),
            P(),
            P(None, DP),
            P(),
            P(DP, "sp", None),
            P(DP, "sp", None),
            P(SP_DP, None, None),
            P(SP_DP, None, None),
            P(SP_DP, None, None),
            P(),
        ),
        out_specs=P(DP, "sp", None),
        check_vma=False,
    )
```

```python
import jax
import jax.numpy as jnp
from jax import lax
from jax.experimental import pallas as pl
from jax.experimental.pallas import tpu as pltpu
from jax.sharding import Mesh
from jax.sharding import PartitionSpec as P


DP = ("dp_0", "dp_1")
SP_DP = ("sp", "dp_0", "dp_1")
CLAMP_LIMIT = 7.0
SWISH_SLOPE = 1.702
F32 = jnp.float32
BF16 = jnp.bfloat16
HIGHEST = lax.Precision.HIGHEST
C = 128
EXTRA = 16
VMEM = pl.BlockSpec(memory_space=pltpu.VMEM)
SMEM = pl.BlockSpec(memory_space=pltpu.SMEM)
HBM = pl.BlockSpec(memory_space=pltpu.HBM)


def near(x):
    return pltpu.with_memory_space_constraint(x, pltpu.VMEM)


def far(x):
    return pltpu.with_memory_space_constraint(x, pltpu.HBM)


def dot(a, b):
    return jnp.dot(a, b, preferred_element_type=F32)


def dot_nt(a, b, precision=None):
    return lax.dot_general(
        a, b, (((1,), (1,)), ((), ())), precision=precision, preferred_element_type=F32
    )


def halves(x):
    high = x.astype(BF16)
    return high, (x - high.astype(F32)).astype(BF16)


def iotas(rows, columns):
    shape = (rows, columns)
    return lax.broadcasted_iota(jnp.int32, shape, 0), lax.broadcasted_iota(jnp.int32, shape, 1)


def swap_matrix():
    row, column = iotas(256, 256)
    return jnp.where((row % 16) * 16 + row // 16 == column, 1.0, 0.0).astype(BF16)


def pack_kernel(q_ref, k_ref, v_ref, logit_ref, decay_ref, out_hbm, out_ref, sems, out_sems):
    heads = out_ref.shape[0]
    copies = []
    for h in range(heads):
        columns = slice(h * C, (h + 1) * C)
        for k, source in enumerate((k_ref, q_ref, v_ref)):
            copy = pltpu.make_async_copy(
                source.at[0, :, columns],
                out_ref.at[h, k * C : (k + 1) * C],
                sems.at[len(copies)],
            )
            copy.start()
            copies.append(copy)
    logits = logit_ref[0].astype(F32)
    decays = decay_ref[0].astype(F32)
    extra_row, _ = iotas(EXTRA, C)
    for h in range(heads):
        extra = jnp.where(extra_row == 0, logits[h : h + 1], decays[h : h + 1])
        out_ref[h, 3 * C : 3 * C + EXTRA] = extra.astype(BF16)
    sent = []
    for h in range(heads):
        for copy in copies[3 * h : 3 * h + 3]:
            copy.wait()
        sent.append(pltpu.make_async_copy(out_ref.at[h], out_hbm.at[h], out_sems.at[h]))
        sent[h].start()
    for copy in sent:
        copy.wait()


def pack(query, key, value, logit, decay_input):
    heads = logit.shape[1]
    return pl.pallas_call(
        pack_kernel,
        out_shape=pltpu.HBM((heads, 3 * C + EXTRA, C), BF16),
        in_specs=[HBM] * 3 + [VMEM] * 2,
        out_specs=HBM,
        scratch_shapes=[
            pltpu.VMEM((heads, 3 * C + EXTRA, C), BF16),
            pltpu.SemaphoreType.DMA((3 * heads,)),
            pltpu.SemaphoreType.DMA((heads,)),
        ],
        compiler_params=pltpu.CompilerParams(vmem_limit_bytes=12 * 2**20),
        name="pack",
    )(far(query), far(key), far(value), far(logit), far(decay_input))


GROUP = 8
WIDE_GROUP = 16


def column_of(ref, n):
    lane = lax.broadcasted_iota(jnp.int32, ref.shape, 1)
    return jnp.sum(jnp.where(lane == n, ref[...], 0.0), axis=1, keepdims=True)


def beside(a, b):
    return jnp.concatenate([a, b], axis=1)


def above(a, b):
    return jnp.concatenate([a, b], axis=0)


def recurrence_kernel(
    x_ref, added_ref, rate_ref, out_ref, base_ref, weight_ref, a_ref, b_ref, qe_ref, su_ref,
    cum_col_ref, cum_row_ref, key_col_ref, key_row_ref, write_col_ref, write_row_ref,
):
    inverse_part(
        x_ref, added_ref, rate_ref, base_ref, weight_ref, a_ref,
        cum_col_ref, cum_row_ref, key_col_ref, key_row_ref, write_col_ref, write_row_ref,
    )
    delta_part(
        x_ref, base_ref, weight_ref, a_ref, cum_col_ref, cum_row_ref, key_col_ref, key_row_ref,
        out_ref, b_ref, qe_ref, su_ref,
    )


def inverse_part(
    x_ref, added_ref, rate_ref, base_ref, weight_ref, a_ref,
    cum_col_ref, cum_row_ref, key_col_ref, key_row_ref, write_col_ref, write_row_ref,
):
    chunks = x_ref.shape[0]
    row, column = iotas(C, C)
    inclusive = row >= column
    strict = row > column
    diagonal = row == column

    chunk_row, _ = iotas(chunks, C)
    logits = jnp.zeros((chunks, C), F32)
    decays = jnp.zeros((chunks, C), F32)
    for n in range(chunks):
        extra = x_ref[n, 3 * C : 3 * C + EXTRA].astype(F32)
        logits = jnp.where(chunk_row == n, extra[0:1], logits)
        decays = jnp.where(chunk_row == n, extra[1:2], decays)
    softplus = jnp.maximum(decays, 0.0) + jnp.log(1.0 + jnp.exp(-jnp.abs(decays)))
    log_decay = added_ref[...] - rate_ref[0] * softplus
    upper = jnp.where(row <= column, 1.0, 0.0)
    lower = jnp.where(inclusive, 1.0, 0.0)
    eye = jnp.where(diagonal, 1.0, 0.0)
    cum_row_ref[...] = jnp.dot(log_decay, upper, precision=HIGHEST, preferred_element_type=F32)
    cum_col_ref[...] = dot_nt(lower, log_decay, precision=HIGHEST)
    write = 1.0 / (1.0 + jnp.exp(-logits))
    write_row_ref[...] = write
    write_col_ref[...] = dot_nt(eye, write, precision=HIGHEST)
    lane = lax.broadcasted_iota(jnp.int32, (C, chunks), 1)

    def group(g, key_columns):
        ns = [g * WIDE_GROUP + k for k in range(WIDE_GROUP)]
        keys = [x_ref[n, 0:C] for n in ns]
        products = [dot_nt(k, k) for k in keys]
        cum_c = [column_of(cum_col_ref, n) for n in ns]
        write_c = [column_of(write_col_ref, n) for n in ns]
        cum_r = [cum_row_ref[pl.ds(n, 1), :] for n in ns]
        write_r = [write_row_ref[pl.ds(n, 1), :] for n in ns]
        squares = [jnp.where(diagonal, p, 0.0) for p in products]
        key_c = [lax.rsqrt(jnp.sum(s, axis=1, keepdims=True) + 1e-06) for s in squares]
        key_r = [lax.rsqrt(jnp.sum(s, axis=0, keepdims=True) + 1e-06) for s in squares]
        for n, c, r in zip(ns, key_c, key_r):
            key_columns = jnp.where(lane == n, c, key_columns)
            key_row_ref[pl.ds(n, 1), :] = r
        lower_part = [
            jnp.where(
                strict,
                p * jnp.exp(jnp.where(inclusive, cc - cr, -jnp.inf)) * (wc * kc) * kr,
                0.0,
            )
            for p, cc, cr, wc, kc, kr in zip(products, cum_c, cum_r, write_c, key_c, key_r)
        ]

        left = [beside(*halves(part)) for part in lower_part]
        pair = (row // 2 == column // 2) & strict
        inverse = [jnp.where(pair, -part, eye) for part in lower_part]
        size = 2
        while size < C:
            highs = [i.astype(BF16) for i in inverse]
            first = [dot(f, above(h, h)) for f, h in zip(left, highs)]
            first = [above(*halves(f)) for f in first]
            second = [dot(beside(h, h), f) for h, f in zip(highs, first)]
            joined = (row // (2 * size) == column // (2 * size)) & (row // size > column // size)
            inverse = [jnp.where(joined, -s, i) for s, i in zip(second, inverse)]
            size *= 2

        for n, i, w in zip(ns, inverse, write_r):
            base_ref[n] = beside(*halves(i * w))
        weight = [
            beside(*halves(i * (w * jnp.exp(c) * k)))
            for i, w, c, k in zip(inverse, write_r, cum_r, key_r)
        ]
        weight = [dot(w, above(k, k)) for w, k in zip(weight, keys)]
        for n, w in zip(ns, weight):
            weight_ref[n] = w.astype(BF16)
        last = [c[C - 1 : C] for c in cum_c]
        carried = [
            above(*halves(w * (k * jnp.exp(end - c))))
            for w, k, end, c in zip(weight, key_c, last, cum_c)
        ]
        turned = [k.T for k in keys]
        update = [dot(beside(t, t), c) for t, c in zip(turned, carried)]
        for n, u, end in zip(ns, update, last):
            a_ref[n] = beside(*halves(jnp.where(diagonal, jnp.exp(end), 0.0) - u))
        return key_columns

    key_col_ref[...] = lax.fori_loop(
        0, chunks // WIDE_GROUP, group, jnp.zeros((C, chunks), F32)
    )


def delta_part(
    x_ref, base_ref, weight_ref, a_ref, cum_col_ref, cum_row_ref, key_col_ref, key_row_ref,
    out_ref, b_ref, qe_ref, su_ref,
):
    chunks = x_ref.shape[0]
    row, column = iotas(C, C)
    inclusive = row >= column

    def prepare(g):
        ns = [g * GROUP + k for k in range(GROUP)]
        keys = [x_ref[n, 0:C] for n in ns]
        queries = [x_ref[n, C : 2 * C] for n in ns]
        values = [x_ref[n, 2 * C : 3 * C] for n in ns]
        scores = [dot_nt(q, k) for q, k in zip(queries, keys)]
        base = [dot(base_ref[n], above(v, v)) for n, v in zip(ns, values)]
        cum_c = [column_of(cum_col_ref, n) for n in ns]
        key_c = [column_of(key_col_ref, n) for n in ns]
        cum_r = [cum_row_ref[pl.ds(n, 1), :] for n in ns]
        key_r = [key_row_ref[pl.ds(n, 1), :] for n in ns]
        q32 = [q.astype(F32) for q in queries]
        query_c = [
            lax.rsqrt(jnp.sum(q * q, axis=1, keepdims=True) + 1e-06) * C ** (-0.5) for q in q32
        ]
        scores = [
            s * jnp.exp(jnp.where(inclusive, cc - cr, -jnp.inf)) * kr * qc
            for s, cc, cr, kr, qc in zip(scores, cum_c, cum_r, key_r, query_c)
        ]
        carried = [
            above(*halves(b * (k * jnp.exp(c[C - 1 : C] - c))))
            for b, k, c in zip(base, key_c, cum_c)
        ]
        turned = [k.T for k in keys]
        update = [dot(beside(t, t), c) for t, c in zip(turned, carried)]
        both = [beside(b.astype(BF16), weight_ref[n]) for n, b in zip(ns, base)]
        seen = [dot(beside(*halves(s)), above(b, b)) for s, b in zip(scores, both)]
        for n, u, s, q, qc, c in zip(ns, update, seen, q32, query_c, cum_c):
            b_ref[n] = u
            su_ref[n] = s[:, :C]
            qe_ref[n] = beside(*halves(q * (qc * jnp.exp(c)) - s[:, C:]))

    def advance(g, state):
        for k in range(GROUP):
            n = g * GROUP + k
            high, low = halves(state)
            queries = qe_ref[n]
            out = dot(queries, above(high, high)) + su_ref[n]
            scale = lax.rsqrt(jnp.mean(out * out, axis=1, keepdims=True) + 1e-05)
            out_ref[n] = (out * scale).astype(BF16)
            a_high, a_low = a_ref[n, :, :C], a_ref[n, :, C:]
            state = dot(beside(a_high, a_high), above(high, low)) + dot(a_low, high) + b_ref[n]
        return state

    prepare(0)

    def step(g, state):
        state = advance(g - 1, state)
        prepare(g)
        return state

    state = lax.fori_loop(1, chunks // GROUP, step, jnp.zeros((C, C), F32))
    advance(chunks // GROUP - 1, state)


def recurrence(blocks, added, decay_rate):
    chunks = blocks.shape[0]
    square = pltpu.VMEM((chunks, C, C), F32)
    wide = pltpu.VMEM((chunks, C, 2 * C), BF16)
    columns = pltpu.VMEM((C, chunks), F32)
    rows = pltpu.VMEM((chunks, C), F32)
    return pl.pallas_call(
        recurrence_kernel,
        out_shape=jax.ShapeDtypeStruct((chunks, C, C), BF16),
        in_specs=[VMEM, VMEM, SMEM],
        out_specs=VMEM,
        scratch_shapes=[
            wide, pltpu.VMEM((chunks, C, C), BF16), wide, square, wide, square,
            columns, rows, columns, rows, columns, rows,
        ],
        compiler_params=pltpu.CompilerParams(vmem_limit_bytes=24 * 2**20),
        cost_estimate=pl.CostEstimate(flops=8 * 10**9, bytes_accessed=2**21, transcendentals=0),
        name="recurrence",
    )(near(blocks), added, decay_rate)


def slots_kernel(index_ref, dest_ref, source_ref, count_ref):
    experts = count_ref.shape[0]
    capacity = source_ref.shape[0] // experts

    def clear(e, carry):
        count_ref[e] = 0
        for k in range(capacity):
            source_ref[e * capacity + k] = 0
        return carry

    lax.fori_loop(0, experts, clear, 0)

    tokens = index_ref.shape[0] // 4

    def place(t, carry):
        for k in range(4):
            at = k * tokens + t
            e = index_ref[at]
            used = count_ref[e]
            count_ref[e] = used + 1
            slot = e * capacity + used
            dest_ref[at] = slot
            source_ref[slot] = t
        return carry

    lax.fori_loop(0, tokens, place, 0)


def slots(index, experts, capacity):
    return pl.pallas_call(
        slots_kernel,
        out_shape=(
            jax.ShapeDtypeStruct(index.shape, jnp.int32),
            jax.ShapeDtypeStruct((experts * capacity,), jnp.int32),
        ),
        in_specs=[SMEM],
        out_specs=(SMEM, SMEM),
        scratch_shapes=[pltpu.SMEM((experts,), jnp.int32)],
        compiler_params=pltpu.CompilerParams(vmem_limit_bytes=2**20),
        name="slots",
    )(index)


def project_kernel(
    rec_ref, gate_hbm, head_gain_ref, residual_hbm, gain_ref, source_ref, place_ref,
    *rest,
):
    weight_refs = rest[:8]
    normed_ref, out_ref, gate_ref, residual_ref, gated_ref, mixed_ref, w_ref, sems = rest[8:]
    gate_copy = pltpu.make_async_copy(gate_hbm, gate_ref, sems.at[8])
    gate_copy.start()
    copies = [
        pltpu.make_async_copy(weight_refs[k], w_ref.at[k], sems.at[k]) for k in range(8)
    ]
    for copy in copies:
        copy.start()
    residual_copy = pltpu.make_async_copy(residual_hbm, residual_ref, sems.at[9])
    residual_copy.start()
    gate_copy.wait()
    heads = rec_ref.shape[0]
    head_gain = head_gain_ref[...]
    for h in range(heads):
        columns = slice(h * C, (h + 1) * C)
        gate = gate_ref[0, :, columns].astype(F32)
        gate = gate / (1.0 + jnp.exp(-gate))
        gated_ref[:, columns] = (rec_ref[h].astype(F32) * head_gain * gate).astype(BF16)
    for k in range(8):
        copies[k].wait()
        mixed_ref[place_ref[k]] = dot(gated_ref[...], w_ref[k])
    total = jnp.concatenate([mixed_ref[k] for k in range(8)], axis=1)
    residual_copy.wait()
    total = total + residual_ref[0].astype(F32)
    centred = total - jnp.mean(total, axis=1, keepdims=True)
    variance = jnp.mean(centred * centred, axis=1, keepdims=True)
    normed = (centred * lax.rsqrt(variance + 1e-05) * gain_ref[...]).astype(BF16)
    swap = swap_matrix()
    tiles = normed.shape[1] // C
    for g in range(normed.shape[0] // 16):
        rows = normed[g * 16 : (g + 1) * 16]
        stacked = jnp.concatenate([rows[:, j * C : (j + 1) * C] for j in range(tiles)], axis=0)
        turned = dot(swap, stacked).astype(BF16)
        normed_ref[g * 16 : (g + 1) * 16] = turned.reshape(16, tiles, C)

    def send(i, carry):
        for k in range(16):
            slot = i * 16 + k
            out_ref[slot] = normed_ref[source_ref[slot]]
        return carry

    lax.fori_loop(0, out_ref.shape[0] // 16, send, 0)


def project(recurrent, gate, head_gain, residual, gain, source, place, weights):
    tokens = residual.shape[1]
    features = residual.shape[2]
    tiles = features // C
    return pl.pallas_call(
        project_kernel,
        out_shape=(
            jax.ShapeDtypeStruct((tokens, tiles, C), BF16),
            jax.ShapeDtypeStruct((source.shape[0], tiles, C), BF16),
        ),
        in_specs=[VMEM, HBM, VMEM, HBM, VMEM] + [SMEM] * 2 + [HBM] * 8,
        out_specs=(VMEM, VMEM),
        scratch_shapes=[
            pltpu.VMEM((1, tokens, features), BF16),
            pltpu.VMEM((1, tokens, features), BF16),
            pltpu.VMEM((tokens, features), BF16),
            pltpu.VMEM((8, tokens, features // 8), F32),
            pltpu.VMEM((8, features, features // 8), BF16),
            pltpu.SemaphoreType.DMA((10,)),
        ],
        compiler_params=pltpu.CompilerParams(vmem_limit_bytes=24 * 2**20),
        cost_estimate=pl.CostEstimate(flops=10**9, bytes_accessed=2**24, transcendentals=0),
        name="project",
    )(
        near(recurrent), far(gate), head_gain, far(residual), gain, source, place,
        *[far(w) for w in weights],
    )


FF_BLOCK = 512
DOWN_ROWS = 384
TURN_UNROLL = 6


def expert_kernel(
    x_ref, gate_hbm, up_hbm, down_hbm, out_ref, gate_ref, up_ref, down_ref, rows_ref, hidden_ref,
    sems,
):
    slots_, tiles, _ = x_ref.shape
    copies = [
        pltpu.make_async_copy(source, target, sems.at[k])
        for k, (source, target) in enumerate(
            ((gate_hbm, gate_ref), (up_hbm, up_ref), (down_hbm, down_ref))
        )
    ]
    for copy in copies:
        copy.start()
    swap = swap_matrix()

    def turn(i, carry):
        for k in range(TURN_UNROLL):
            start = pl.multiple_of((i * TURN_UNROLL + k) * 32, 32)
            pieces = [x_ref[pl.ds(start + o, 16)].reshape(16 * tiles, C) for o in (0, 16)]
            turned = dot(swap, beside(*pieces)).astype(BF16)
            for j in range(tiles):
                part = turned[j * 16 : (j + 1) * 16]
                rows_ref[pl.ds(start, 16), j * C : (j + 1) * C] = part[:, :C]
                rows_ref[pl.ds(start + 16, 16), j * C : (j + 1) * C] = part[:, C:]
        return carry

    lax.fori_loop(0, slots_ // (32 * TURN_UNROLL), turn, 0)
    copies[0].wait()
    copies[1].wait()

    def widen(f, carry):
        columns = pl.ds(pl.multiple_of(f * FF_BLOCK, FF_BLOCK), FF_BLOCK)
        rows = rows_ref[...]
        gate = jnp.minimum(dot(rows, gate_ref[:, columns]), CLAMP_LIMIT)
        up = jnp.clip(dot(rows, up_ref[:, columns]), -CLAMP_LIMIT, CLAMP_LIMIT)
        hidden = gate / (1.0 + jnp.exp(-SWISH_SLOPE * gate)) * (up + 1.0)
        hidden_ref[:, columns] = hidden.astype(BF16)
        return carry

    lax.fori_loop(0, hidden_ref.shape[1] // FF_BLOCK, widen, 0)
    copies[2].wait()

    def narrow(i, carry):
        start = pl.multiple_of(i * DOWN_ROWS, DOWN_ROWS)
        made = dot(hidden_ref[pl.ds(start, DOWN_ROWS)], down_ref[...]).astype(BF16)
        for g in range(0, DOWN_ROWS, 32):
            stacked = [
                jnp.concatenate(
                    [made[k : k + 16, j * C : (j + 1) * C] for j in range(tiles)], axis=0
                )
                for k in (g, g + 16)
            ]
            turned = dot(swap, beside(*stacked)).astype(BF16)
            out_ref[pl.ds(start + g, 16)] = turned[:, :C].reshape(16, tiles, C)
            out_ref[pl.ds(start + g + 16, 16)] = turned[:, C:].reshape(16, tiles, C)
        return carry

    lax.fori_loop(0, slots_ // DOWN_ROWS, narrow, 0)


def expert(rows, gate_weight, up_weight, down_weight):
    slots_, _, _ = rows.shape
    features, hidden = gate_weight.shape
    return pl.pallas_call(
        expert_kernel,
        out_shape=jax.ShapeDtypeStruct(rows.shape, BF16),
        in_specs=[VMEM, HBM, HBM, HBM],
        out_specs=VMEM,
        scratch_shapes=[
            pltpu.VMEM(gate_weight.shape, BF16),
            pltpu.VMEM(up_weight.shape, BF16),
            pltpu.VMEM(down_weight.shape, BF16),
            pltpu.VMEM((slots_, features), BF16),
            pltpu.VMEM((slots_, hidden), BF16),
            pltpu.SemaphoreType.DMA((3,)),
        ],
        compiler_params=pltpu.CompilerParams(vmem_limit_bytes=36 * 2**20),
        cost_estimate=pl.CostEstimate(flops=10**10, bytes_accessed=2**24, transcendentals=0),
        name="expert",
    )(near(rows), far(gate_weight), far(up_weight), far(down_weight))


def combine_kernel(
    back_ref, normed_ref, gain_ref, dest_ref, weight_ref, out_hbm, z_ref, out_ref, sems
):
    tokens, tiles, _ = normed_ref.shape
    swap = swap_matrix()
    gain = gain_ref[...]

    def copy_of(i):
        part = pl.ds(pl.multiple_of(i * 16, 16), 16)
        return pltpu.make_async_copy(out_ref.at[part], out_hbm.at[0, part], sems.at[i])

    def add(i):
        for k in range(16):
            t = i * 16 + k
            total = normed_ref[t].astype(F32)
            for pick in range(4):
                at = pick * tokens + t
                total = total + weight_ref[at] * back_ref[dest_ref[at]].astype(F32)
            z_ref[t] = total

    def finish(i):
        start = pl.multiple_of(i * 16, 16)
        z = z_ref[pl.ds(start, 16)].reshape(16 * tiles, C)
        high = z.astype(BF16)
        rest = z - high.astype(F32)
        middle = rest.astype(BF16)
        low = (rest - middle.astype(F32)).astype(BF16)
        turned = dot(swap, beside(high, middle))
        turned = turned[:, :C] + turned[:, C:] + dot(swap, low)
        total = jnp.concatenate([turned[j * 16 : (j + 1) * 16] for j in range(tiles)], axis=1)
        centred = total - jnp.mean(total, axis=1, keepdims=True)
        variance = jnp.mean(centred * centred, axis=1, keepdims=True)
        out_ref[pl.ds(start, 16), :] = centred * lax.rsqrt(variance + 1e-05) * gain
        copy_of(i).start()

    add(0)

    def step(i, carry):
        finish(i - 1)
        add(i)
        return carry

    groups = tokens // 16
    lax.fori_loop(1, groups, step, 0)
    finish(groups - 1)
    for i in range(groups):
        copy_of(i).wait()


def combine(back, normed, gain, dest, weight):
    tokens, tiles, _ = normed.shape
    return pl.pallas_call(
        combine_kernel,
        out_shape=pltpu.HBM((1, tokens, tiles * C), F32),
        in_specs=[VMEM] * 3 + [SMEM] * 2,
        out_specs=HBM,
        scratch_shapes=[
            pltpu.VMEM((tokens, tiles, C), F32),
            pltpu.VMEM((tokens, tiles * C), F32),
            pltpu.SemaphoreType.DMA((tokens // 16,)),
        ],
        compiler_params=pltpu.CompilerParams(vmem_limit_bytes=12 * 2**20),
        name="combine",
    )(near(back), near(normed), gain, dest, weight)


def gathered(block):
    y_size, core_size = lax.axis_size("dp_0"), lax.axis_size("dp_1")
    y, core = lax.axis_index("dp_0"), lax.axis_index("dp_1")
    found = [block]
    for shift in range(1, y_size):
        pairs = [(i, (i + shift) % y_size) for i in range(y_size)]
        found.append(lax.ppermute(block, "dp_0", pairs))
    places = [((y - shift) % y_size) * core_size + core for shift in range(y_size)]
    others = [((y - shift) % y_size) * core_size + 1 - core for shift in range(y_size)]
    return found, jnp.stack(places + others).astype(jnp.int32)


def layer(
    residual,
    query,
    key,
    value,
    output_gate_input,
    write_strength_logit,
    decay_head_input,
    added_log_decay,
    head_decay_rate,
    head_norm_gain,
    output_projection,
    mixer_norm_gain,
    token_expert_index,
    token_expert_weight,
    expert_gate_weight,
    expert_up_weight,
    expert_down_weight,
    feedforward_norm_gain,
):
    experts = lax.axis_size(SP_DP)
    tokens, features = residual.shape[1:]
    picks = token_expert_index.shape[2]
    capacity = tokens * picks * 3 // (2 * experts)
    tiles = features // C
    found, places = gathered(output_projection)
    dest, source = slots(token_expert_index[0].T.reshape(-1), experts, capacity)
    blocks = pack(
        query,
        key,
        value,
        write_strength_logit.transpose(0, 2, 1),
        decay_head_input.transpose(0, 2, 1),
    )
    blocks = lax.all_to_all(blocks, "sp", split_axis=0, concat_axis=0, tiled=True)
    recurrent = recurrence(blocks, added_log_decay.reshape(-1, C), head_decay_rate)
    returned = lax.all_to_all(recurrent, "sp", split_axis=0, concat_axis=0, tiled=True)
    weights = list(found)
    for b in found:
        weights.append(lax.ppermute(b, "dp_1", [(0, 1), (1, 0)]))
    normed, rows = project(
        returned,
        output_gate_input,
        head_norm_gain.reshape(1, C),
        residual,
        mixer_norm_gain.reshape(1, features),
        source,
        places,
        weights,
    )
    rows = rows.reshape(experts, capacity * tiles, C)
    rows = lax.all_to_all(rows, SP_DP, split_axis=0, concat_axis=0, tiled=True)
    made = expert(
        rows.reshape(experts * capacity, tiles, C),
        expert_gate_weight[0],
        expert_up_weight[0],
        expert_down_weight[0],
    )
    made = made.reshape(experts, capacity * tiles, C)
    back = lax.all_to_all(made, SP_DP, split_axis=0, concat_axis=0, tiled=True)
    return combine(
        back.reshape(experts * capacity, tiles, C),
        normed,
        feedforward_norm_gain.reshape(1, features),
        dest,
        token_expert_weight[0].T.reshape(-1),
    )


def solution(mesh):
    torus = Mesh(mesh.devices.reshape(mesh.shape["sp"], 4, 2), ("sp", "dp_0", "dp_1"))
    return jax.shard_map(
        layer,
        mesh=torus,
        in_specs=(
            P(DP, "sp", None),
            P(DP, "sp", None),
            P(DP, "sp", None),
            P(DP, "sp", None),
            P(DP, "sp", None),
            P(DP, "sp", None),
            P(DP, "sp", None),
            P(DP, "sp", None),
            P("sp"),
            P(),
            P(None, DP),
            P(),
            P(DP, "sp", None),
            P(DP, "sp", None),
            P(SP_DP, None, None),
            P(SP_DP, None, None),
            P(SP_DP, None, None),
            P(),
        ),
        out_specs=P(DP, "sp", None),
        check_vma=False,
    )
```

```python
import jax
import jax.numpy as jnp
from jax import lax
from jax.experimental import pallas as pl
from jax.experimental.pallas import tpu as pltpu
from jax.sharding import Mesh
from jax.sharding import PartitionSpec as P


DP = ("dp_0", "dp_1")
SP_DP = ("sp", "dp_0", "dp_1")
CLAMP_LIMIT = 7.0
SWISH_SLOPE = 1.702
F32 = jnp.float32
BF16 = jnp.bfloat16
HIGHEST = lax.Precision.HIGHEST
C = 128
EXTRA = 16
VMEM = pl.BlockSpec(memory_space=pltpu.VMEM)
SMEM = pl.BlockSpec(memory_space=pltpu.SMEM)
HBM = pl.BlockSpec(memory_space=pltpu.HBM)


def near(x):
    return pltpu.with_memory_space_constraint(x, pltpu.VMEM)


def far(x):
    return pltpu.with_memory_space_constraint(x, pltpu.HBM)


def dot(a, b):
    return jnp.dot(a, b, preferred_element_type=F32)


def dot_nt(a, b, precision=None):
    return lax.dot_general(
        a, b, (((1,), (1,)), ((), ())), precision=precision, preferred_element_type=F32
    )


def halves(x):
    high = x.astype(BF16)
    return high, (x - high.astype(F32)).astype(BF16)


def iotas(rows, columns):
    shape = (rows, columns)
    return lax.broadcasted_iota(jnp.int32, shape, 0), lax.broadcasted_iota(jnp.int32, shape, 1)


def swap_matrix():
    row, column = iotas(256, 256)
    return jnp.where((row % 16) * 16 + row // 16 == column, 1.0, 0.0).astype(BF16)


def pack_kernel(q_ref, k_ref, v_ref, logit_ref, decay_ref, out_hbm, out_ref, sems, out_sems):
    heads = out_ref.shape[0]
    copies = []
    for h in range(heads):
        columns = slice(h * C, (h + 1) * C)
        for k, source in enumerate((k_ref, q_ref, v_ref)):
            copy = pltpu.make_async_copy(
                source.at[0, :, columns],
                out_ref.at[h, k * C : (k + 1) * C],
                sems.at[len(copies)],
            )
            copy.start()
            copies.append(copy)
    logits = logit_ref[0].astype(F32)
    decays = decay_ref[0].astype(F32)
    extra_row, _ = iotas(EXTRA, C)
    for h in range(heads):
        extra = jnp.where(extra_row == 0, logits[h : h + 1], decays[h : h + 1])
        out_ref[h, 3 * C : 3 * C + EXTRA] = extra.astype(BF16)
    sent = []
    for h in range(heads):
        for copy in copies[3 * h : 3 * h + 3]:
            copy.wait()
        sent.append(pltpu.make_async_copy(out_ref.at[h], out_hbm.at[h], out_sems.at[h]))
        sent[h].start()
    for copy in sent:
        copy.wait()


def pack(query, key, value, logit, decay_input):
    heads = logit.shape[1]
    return pl.pallas_call(
        pack_kernel,
        out_shape=pltpu.HBM((heads, 3 * C + EXTRA, C), BF16),
        in_specs=[HBM] * 3 + [VMEM] * 2,
        out_specs=HBM,
        scratch_shapes=[
            pltpu.VMEM((heads, 3 * C + EXTRA, C), BF16),
            pltpu.SemaphoreType.DMA((3 * heads,)),
            pltpu.SemaphoreType.DMA((heads,)),
        ],
        compiler_params=pltpu.CompilerParams(vmem_limit_bytes=12 * 2**20),
        name="pack",
    )(far(query), far(key), far(value), far(logit), far(decay_input))


GROUP = 8
WIDE_GROUP = 16


def column_of(ref, n):
    lane = lax.broadcasted_iota(jnp.int32, ref.shape, 1)
    return jnp.sum(jnp.where(lane == n, ref[...], 0.0), axis=1, keepdims=True)


def beside(a, b):
    return jnp.concatenate([a, b], axis=1)


def above(a, b):
    return jnp.concatenate([a, b], axis=0)


def recurrence_kernel(
    x_ref, added_ref, rate_ref, out_ref, base_ref, weight_ref, a_ref, b_ref, qe_ref, su_ref,
    cum_col_ref, cum_row_ref, key_col_ref, key_row_ref, write_col_ref, write_row_ref,
):
    inverse_part(
        x_ref, added_ref, rate_ref, base_ref, weight_ref, a_ref,
        cum_col_ref, cum_row_ref, key_col_ref, key_row_ref, write_col_ref, write_row_ref,
    )
    delta_part(
        x_ref, base_ref, weight_ref, a_ref, cum_col_ref, cum_row_ref, key_col_ref, key_row_ref,
        out_ref, b_ref, qe_ref, su_ref,
    )


def inverse_part(
    x_ref, added_ref, rate_ref, base_ref, weight_ref, a_ref,
    cum_col_ref, cum_row_ref, key_col_ref, key_row_ref, write_col_ref, write_row_ref,
):
    chunks = x_ref.shape[0]
    row, column = iotas(C, C)
    inclusive = row >= column
    strict = row > column
    diagonal = row == column

    chunk_row, _ = iotas(chunks, C)
    logits = jnp.zeros((chunks, C), F32)
    decays = jnp.zeros((chunks, C), F32)
    for n in range(chunks):
        extra = x_ref[n, 3 * C : 3 * C + EXTRA].astype(F32)
        logits = jnp.where(chunk_row == n, extra[0:1], logits)
        decays = jnp.where(chunk_row == n, extra[1:2], decays)
    softplus = jnp.maximum(decays, 0.0) + jnp.log(1.0 + jnp.exp(-jnp.abs(decays)))
    log_decay = added_ref[...] - rate_ref[0] * softplus
    upper = jnp.where(row <= column, 1.0, 0.0)
    lower = jnp.where(inclusive, 1.0, 0.0)
    eye = jnp.where(diagonal, 1.0, 0.0)
    cum_row_ref[...] = jnp.dot(log_decay, upper, precision=HIGHEST, preferred_element_type=F32)
    cum_col_ref[...] = dot_nt(lower, log_decay, precision=HIGHEST)
    write = 1.0 / (1.0 + jnp.exp(-logits))
    write_row_ref[...] = write
    write_col_ref[...] = dot_nt(eye, write, precision=HIGHEST)
    lane = lax.broadcasted_iota(jnp.int32, (C, chunks), 1)

    def group(g, key_columns):
        ns = [g * WIDE_GROUP + k for k in range(WIDE_GROUP)]
        keys = [x_ref[n, 0:C] for n in ns]
        products = [dot_nt(k, k) for k in keys]
        cum_c = [column_of(cum_col_ref, n) for n in ns]
        write_c = [column_of(write_col_ref, n) for n in ns]
        cum_r = [cum_row_ref[pl.ds(n, 1), :] for n in ns]
        write_r = [write_row_ref[pl.ds(n, 1), :] for n in ns]
        squares = [jnp.where(diagonal, p, 0.0) for p in products]
        key_c = [lax.rsqrt(jnp.sum(s, axis=1, keepdims=True) + 1e-06) for s in squares]
        key_r = [lax.rsqrt(jnp.sum(s, axis=0, keepdims=True) + 1e-06) for s in squares]
        for n, c, r in zip(ns, key_c, key_r):
            key_columns = jnp.where(lane == n, c, key_columns)
            key_row_ref[pl.ds(n, 1), :] = r
        lower_part = [
            jnp.where(
                strict,
                p * jnp.exp(jnp.where(inclusive, cc - cr, -jnp.inf)) * (wc * kc) * kr,
                0.0,
            )
            for p, cc, cr, wc, kc, kr in zip(products, cum_c, cum_r, write_c, key_c, key_r)
        ]

        left = [beside(*halves(part)) for part in lower_part]
        pair = (row // 2 == column // 2) & strict
        inverse = [jnp.where(pair, -part, eye) for part in lower_part]
        size = 2
        while size < C:
            highs = [i.astype(BF16) for i in inverse]
            first = [dot(f, above(h, h)) for f, h in zip(left, highs)]
            first = [above(*halves(f)) for f in first]
            second = [dot(beside(h, h), f) for h, f in zip(highs, first)]
            joined = (row // (2 * size) == column // (2 * size)) & (row // size > column // size)
            inverse = [jnp.where(joined, -s, i) for s, i in zip(second, inverse)]
            size *= 2

        for n, i, w in zip(ns, inverse, write_r):
            base_ref[n] = beside(*halves(i * w))
        weight = [
            beside(*halves(i * (w * jnp.exp(c) * k)))
            for i, w, c, k in zip(inverse, write_r, cum_r, key_r)
        ]
        weight = [dot(w, above(k, k)) for w, k in zip(weight, keys)]
        for n, w in zip(ns, weight):
            weight_ref[n] = w.astype(BF16)
        last = [c[C - 1 : C] for c in cum_c]
        carried = [
            above(*halves(w * (k * jnp.exp(end - c))))
            for w, k, end, c in zip(weight, key_c, last, cum_c)
        ]
        turned = [k.T for k in keys]
        update = [dot(beside(t, t), c) for t, c in zip(turned, carried)]
        for n, u, end in zip(ns, update, last):
            a_ref[n] = beside(*halves(jnp.where(diagonal, jnp.exp(end), 0.0) - u))
        return key_columns

    key_col_ref[...] = lax.fori_loop(
        0, chunks // WIDE_GROUP, group, jnp.zeros((C, chunks), F32)
    )


def delta_part(
    x_ref, base_ref, weight_ref, a_ref, cum_col_ref, cum_row_ref, key_col_ref, key_row_ref,
    out_ref, b_ref, qe_ref, su_ref,
):
    chunks = x_ref.shape[0]
    row, column = iotas(C, C)
    inclusive = row >= column

    def prepare(g):
        ns = [g * GROUP + k for k in range(GROUP)]
        keys = [x_ref[n, 0:C] for n in ns]
        queries = [x_ref[n, C : 2 * C] for n in ns]
        values = [x_ref[n, 2 * C : 3 * C] for n in ns]
        scores = [dot_nt(q, k) for q, k in zip(queries, keys)]
        base = [dot(base_ref[n], above(v, v)) for n, v in zip(ns, values)]
        cum_c = [column_of(cum_col_ref, n) for n in ns]
        key_c = [column_of(key_col_ref, n) for n in ns]
        cum_r = [cum_row_ref[pl.ds(n, 1), :] for n in ns]
        key_r = [key_row_ref[pl.ds(n, 1), :] for n in ns]
        q32 = [q.astype(F32) for q in queries]
        query_c = [
            lax.rsqrt(jnp.sum(q * q, axis=1, keepdims=True) + 1e-06) * C ** (-0.5) for q in q32
        ]
        scores = [
            s * jnp.exp(jnp.where(inclusive, cc - cr, -jnp.inf)) * kr * qc
            for s, cc, cr, kr, qc in zip(scores, cum_c, cum_r, key_r, query_c)
        ]
        carried = [
            above(*halves(b * (k * jnp.exp(c[C - 1 : C] - c))))
            for b, k, c in zip(base, key_c, cum_c)
        ]
        turned = [k.T for k in keys]
        update = [dot(beside(t, t), c) for t, c in zip(turned, carried)]
        both = [beside(b.astype(BF16), weight_ref[n]) for n, b in zip(ns, base)]
        seen = [dot(beside(*halves(s)), above(b, b)) for s, b in zip(scores, both)]
        for n, u, s, q, qc, c in zip(ns, update, seen, q32, query_c, cum_c):
            b_ref[n] = u
            su_ref[n] = s[:, :C]
            qe_ref[n] = beside(*halves(q * (qc * jnp.exp(c)) - s[:, C:]))

    def advance(g, state):
        for k in range(GROUP):
            n = g * GROUP + k
            high, low = halves(state)
            queries = qe_ref[n]
            out = dot(queries, above(high, high)) + su_ref[n]
            scale = lax.rsqrt(jnp.mean(out * out, axis=1, keepdims=True) + 1e-05)
            out_ref[n] = (out * scale).astype(BF16)
            a_high, a_low = a_ref[n, :, :C], a_ref[n, :, C:]
            state = dot(beside(a_high, a_high), above(high, low)) + dot(a_low, high) + b_ref[n]
        return state

    prepare(0)

    def step(g, state):
        state = advance(g - 1, state)
        prepare(g)
        return state

    state = lax.fori_loop(1, chunks // GROUP, step, jnp.zeros((C, C), F32))
    advance(chunks // GROUP - 1, state)


def recurrence(blocks, added, decay_rate):
    chunks = blocks.shape[0]
    square = pltpu.VMEM((chunks, C, C), F32)
    wide = pltpu.VMEM((chunks, C, 2 * C), BF16)
    columns = pltpu.VMEM((C, chunks), F32)
    rows = pltpu.VMEM((chunks, C), F32)
    return pl.pallas_call(
        recurrence_kernel,
        out_shape=jax.ShapeDtypeStruct((chunks, C, C), BF16),
        in_specs=[VMEM, VMEM, SMEM],
        out_specs=VMEM,
        scratch_shapes=[
            wide, pltpu.VMEM((chunks, C, C), BF16), wide, square, wide, square,
            columns, rows, columns, rows, columns, rows,
        ],
        compiler_params=pltpu.CompilerParams(vmem_limit_bytes=24 * 2**20),
        cost_estimate=pl.CostEstimate(flops=8 * 10**9, bytes_accessed=2**21, transcendentals=0),
        name="recurrence",
    )(near(blocks), added, decay_rate)


def slots_kernel(index_ref, dest_ref, source_ref, count_ref):
    experts = count_ref.shape[0]
    capacity = source_ref.shape[0] // experts

    def clear(e, carry):
        count_ref[e] = 0
        for k in range(capacity):
            source_ref[e * capacity + k] = 0
        return carry

    lax.fori_loop(0, experts, clear, 0)

    tokens = index_ref.shape[0] // 4

    def place(t, carry):
        for k in range(4):
            at = k * tokens + t
            e = index_ref[at]
            used = count_ref[e]
            count_ref[e] = used + 1
            slot = e * capacity + used
            dest_ref[at] = slot
            source_ref[slot] = t
        return carry

    lax.fori_loop(0, tokens, place, 0)


def slots(index, experts, capacity):
    return pl.pallas_call(
        slots_kernel,
        out_shape=(
            jax.ShapeDtypeStruct(index.shape, jnp.int32),
            jax.ShapeDtypeStruct((experts * capacity,), jnp.int32),
        ),
        in_specs=[SMEM],
        out_specs=(SMEM, SMEM),
        scratch_shapes=[pltpu.SMEM((experts,), jnp.int32)],
        compiler_params=pltpu.CompilerParams(vmem_limit_bytes=2**20),
        name="slots",
    )(index)


def project_kernel(
    rec_ref, gate_hbm, head_gain_ref, residual_hbm, gain_ref, source_ref, place_ref,
    *rest,
):
    weight_refs = rest[:8]
    normed_ref, out_ref, gate_ref, residual_ref, gated_ref, mixed_ref, w_ref, sems = rest[8:]
    gate_copy = pltpu.make_async_copy(gate_hbm, gate_ref, sems.at[8])
    gate_copy.start()
    copies = [
        pltpu.make_async_copy(weight_refs[k], w_ref.at[k], sems.at[k]) for k in range(8)
    ]
    for copy in copies:
        copy.start()
    residual_copy = pltpu.make_async_copy(residual_hbm, residual_ref, sems.at[9])
    residual_copy.start()
    gate_copy.wait()
    heads = rec_ref.shape[0]
    head_gain = head_gain_ref[...]
    for h in range(heads):
        columns = slice(h * C, (h + 1) * C)
        gate = gate_ref[0, :, columns].astype(F32)
        gate = gate / (1.0 + jnp.exp(-gate))
        gated_ref[:, columns] = (rec_ref[h].astype(F32) * head_gain * gate).astype(BF16)
    for k in range(8):
        copies[k].wait()
        mixed_ref[place_ref[k]] = dot(gated_ref[...], w_ref[k])
    total = jnp.concatenate([mixed_ref[k] for k in range(8)], axis=1)
    residual_copy.wait()
    total = total + residual_ref[0].astype(F32)
    centred = total - jnp.mean(total, axis=1, keepdims=True)
    variance = jnp.mean(centred * centred, axis=1, keepdims=True)
    normed = (centred * lax.rsqrt(variance + 1e-05) * gain_ref[...]).astype(BF16)
    swap = swap_matrix()
    tiles = normed.shape[1] // C
    for g in range(normed.shape[0] // 16):
        rows = normed[g * 16 : (g + 1) * 16]
        stacked = jnp.concatenate([rows[:, j * C : (j + 1) * C] for j in range(tiles)], axis=0)
        turned = dot(swap, stacked).astype(BF16)
        normed_ref[g * 16 : (g + 1) * 16] = turned.reshape(16, tiles, C)

    def send(i, carry):
        for k in range(16):
            slot = i * 16 + k
            out_ref[slot] = normed_ref[source_ref[slot]]
        return carry

    lax.fori_loop(0, out_ref.shape[0] // 16, send, 0)


def project(recurrent, gate, head_gain, residual, gain, source, place, weights):
    tokens = residual.shape[1]
    features = residual.shape[2]
    tiles = features // C
    return pl.pallas_call(
        project_kernel,
        out_shape=(
            jax.ShapeDtypeStruct((tokens, tiles, C), BF16),
            jax.ShapeDtypeStruct((source.shape[0], tiles, C), BF16),
        ),
        in_specs=[VMEM, HBM, VMEM, HBM, VMEM] + [SMEM] * 2 + [HBM] * 8,
        out_specs=(VMEM, VMEM),
        scratch_shapes=[
            pltpu.VMEM((1, tokens, features), BF16),
            pltpu.VMEM((1, tokens, features), BF16),
            pltpu.VMEM((tokens, features), BF16),
            pltpu.VMEM((8, tokens, features // 8), F32),
            pltpu.VMEM((8, features, features // 8), BF16),
            pltpu.SemaphoreType.DMA((10,)),
        ],
        compiler_params=pltpu.CompilerParams(vmem_limit_bytes=24 * 2**20),
        cost_estimate=pl.CostEstimate(flops=10**9, bytes_accessed=2**24, transcendentals=0),
        name="project",
    )(
        near(recurrent), far(gate), head_gain, far(residual), gain, source, place,
        *[far(w) for w in weights],
    )


FF_BLOCK = 512
DOWN_ROWS = 384
TURN_UNROLL = 6


def expert_kernel(
    x_ref, gate_hbm, up_hbm, down_hbm, out_ref, gate_ref, up_ref, down_ref, rows_ref, hidden_ref,
    sems,
):
    slots_, tiles, _ = x_ref.shape
    copies = [
        pltpu.make_async_copy(source, target, sems.at[k])
        for k, (source, target) in enumerate(
            ((gate_hbm, gate_ref), (up_hbm, up_ref), (down_hbm, down_ref))
        )
    ]
    for copy in copies:
        copy.start()
    swap = swap_matrix()

    def turn(i, carry):
        for k in range(TURN_UNROLL):
            start = pl.multiple_of((i * TURN_UNROLL + k) * 32, 32)
            pieces = [x_ref[pl.ds(start + o, 16)].reshape(16 * tiles, C) for o in (0, 16)]
            turned = dot(swap, beside(*pieces)).astype(BF16)
            for j in range(tiles):
                part = turned[j * 16 : (j + 1) * 16]
                rows_ref[pl.ds(start, 16), j * C : (j + 1) * C] = part[:, :C]
                rows_ref[pl.ds(start + 16, 16), j * C : (j + 1) * C] = part[:, C:]
        return carry

    lax.fori_loop(0, slots_ // (32 * TURN_UNROLL), turn, 0)
    copies[0].wait()
    copies[1].wait()

    def widen(f, carry):
        columns = pl.ds(pl.multiple_of(f * FF_BLOCK, FF_BLOCK), FF_BLOCK)
        rows = rows_ref[...]
        gate = jnp.minimum(dot(rows, gate_ref[:, columns]), CLAMP_LIMIT)
        up = jnp.clip(dot(rows, up_ref[:, columns]), -CLAMP_LIMIT, CLAMP_LIMIT)
        hidden = gate / (1.0 + jnp.exp(-SWISH_SLOPE * gate)) * (up + 1.0)
        hidden_ref[:, columns] = hidden.astype(BF16)
        return carry

    lax.fori_loop(0, hidden_ref.shape[1] // FF_BLOCK, widen, 0)
    copies[2].wait()

    def narrow(i, carry):
        start = pl.multiple_of(i * DOWN_ROWS, DOWN_ROWS)
        made = dot(hidden_ref[pl.ds(start, DOWN_ROWS)], down_ref[...]).astype(BF16)
        for g in range(0, DOWN_ROWS, 32):
            stacked = [
                jnp.concatenate(
                    [made[k : k + 16, j * C : (j + 1) * C] for j in range(tiles)], axis=0
                )
                for k in (g, g + 16)
            ]
            turned = dot(swap, beside(*stacked)).astype(BF16)
            out_ref[pl.ds(start + g, 16)] = turned[:, :C].reshape(16, tiles, C)
            out_ref[pl.ds(start + g + 16, 16)] = turned[:, C:].reshape(16, tiles, C)
        return carry

    lax.fori_loop(0, slots_ // DOWN_ROWS, narrow, 0)


def expert(rows, gate_weight, up_weight, down_weight):
    slots_, _, _ = rows.shape
    features, hidden = gate_weight.shape
    return pl.pallas_call(
        expert_kernel,
        out_shape=jax.ShapeDtypeStruct(rows.shape, BF16),
        in_specs=[VMEM, HBM, HBM, HBM],
        out_specs=VMEM,
        scratch_shapes=[
            pltpu.VMEM(gate_weight.shape, BF16),
            pltpu.VMEM(up_weight.shape, BF16),
            pltpu.VMEM(down_weight.shape, BF16),
            pltpu.VMEM((slots_, features), BF16),
            pltpu.VMEM((slots_, hidden), BF16),
            pltpu.SemaphoreType.DMA((3,)),
        ],
        compiler_params=pltpu.CompilerParams(vmem_limit_bytes=36 * 2**20),
        cost_estimate=pl.CostEstimate(flops=10**10, bytes_accessed=2**24, transcendentals=0),
        name="expert",
    )(near(rows), far(gate_weight), far(up_weight), far(down_weight))


def combine_kernel(back_ref, normed_ref, gain_ref, dest_ref, weight_ref, out_ref, z_ref):
    tokens, tiles, _ = normed_ref.shape
    swap = swap_matrix()
    gain = gain_ref[...]

    def some(i, carry):
        for k in range(16):
            t = i * 16 + k
            total = normed_ref[t].astype(F32)
            for pick in range(4):
                at = pick * tokens + t
                total = total + weight_ref[at] * back_ref[dest_ref[at]].astype(F32)
            z_ref[t] = total
        return carry

    lax.fori_loop(0, tokens // 16, some, 0)

    def finish(i, carry):
        start = pl.multiple_of(i * 16, 16)
        z = z_ref[pl.ds(start, 16)].reshape(16 * tiles, C)
        high = z.astype(BF16)
        rest = z - high.astype(F32)
        middle = rest.astype(BF16)
        low = (rest - middle.astype(F32)).astype(BF16)
        turned = dot(swap, beside(high, middle))
        turned = turned[:, :C] + turned[:, C:] + dot(swap, low)
        total = jnp.concatenate([turned[j * 16 : (j + 1) * 16] for j in range(tiles)], axis=1)
        centred = total - jnp.mean(total, axis=1, keepdims=True)
        variance = jnp.mean(centred * centred, axis=1, keepdims=True)
        out_ref[0, pl.ds(start, 16), :] = centred * lax.rsqrt(variance + 1e-05) * gain
        return carry

    lax.fori_loop(0, tokens // 16, finish, 0, unroll=2)


def combine(back, normed, gain, dest, weight):
    tokens, tiles, _ = normed.shape
    return pl.pallas_call(
        combine_kernel,
        out_shape=jax.ShapeDtypeStruct((1, tokens, tiles * C), F32),
        in_specs=[VMEM] * 3 + [SMEM] * 2,
        out_specs=VMEM,
        scratch_shapes=[pltpu.VMEM((tokens, tiles, C), F32)],
        compiler_params=pltpu.CompilerParams(vmem_limit_bytes=12 * 2**20),
        name="combine",
    )(near(back), near(normed), gain, dest, weight)


def gathered(block):
    y_size, core_size = lax.axis_size("dp_0"), lax.axis_size("dp_1")
    y, core = lax.axis_index("dp_0"), lax.axis_index("dp_1")
    found = [block]
    for shift in range(1, y_size):
        pairs = [(i, (i + shift) % y_size) for i in range(y_size)]
        found.append(lax.ppermute(block, "dp_0", pairs))
    places = [((y - shift) % y_size) * core_size + core for shift in range(y_size)]
    others = [((y - shift) % y_size) * core_size + 1 - core for shift in range(y_size)]
    return found, jnp.stack(places + others).astype(jnp.int32)


def layer(
    residual,
    query,
    key,
    value,
    output_gate_input,
    write_strength_logit,
    decay_head_input,
    added_log_decay,
    head_decay_rate,
    head_norm_gain,
    output_projection,
    mixer_norm_gain,
    token_expert_index,
    token_expert_weight,
    expert_gate_weight,
    expert_up_weight,
    expert_down_weight,
    feedforward_norm_gain,
):
    experts = lax.axis_size(SP_DP)
    tokens, features = residual.shape[1:]
    picks = token_expert_index.shape[2]
    capacity = tokens * picks * 3 // (2 * experts)
    tiles = features // C
    found, places = gathered(output_projection)
    dest, source = slots(token_expert_index[0].T.reshape(-1), experts, capacity)
    blocks = pack(
        query,
        key,
        value,
        write_strength_logit.transpose(0, 2, 1),
        decay_head_input.transpose(0, 2, 1),
    )
    blocks = lax.all_to_all(blocks, "sp", split_axis=0, concat_axis=0, tiled=True)
    recurrent = recurrence(blocks, added_log_decay.reshape(-1, C), head_decay_rate)
    returned = lax.all_to_all(recurrent, "sp", split_axis=0, concat_axis=0, tiled=True)
    weights = list(found)
    for b in found:
        weights.append(lax.ppermute(b, "dp_1", [(0, 1), (1, 0)]))
    normed, rows = project(
        returned,
        output_gate_input,
        head_norm_gain.reshape(1, C),
        residual,
        mixer_norm_gain.reshape(1, features),
        source,
        places,
        weights,
    )
    rows = rows.reshape(experts, capacity * tiles, C)
    rows = lax.all_to_all(rows, SP_DP, split_axis=0, concat_axis=0, tiled=True)
    made = expert(
        rows.reshape(experts * capacity, tiles, C),
        expert_gate_weight[0],
        expert_up_weight[0],
        expert_down_weight[0],
    )
    made = made.reshape(experts, capacity * tiles, C)
    back = lax.all_to_all(made, SP_DP, split_axis=0, concat_axis=0, tiled=True)
    return combine(
        back.reshape(experts * capacity, tiles, C),
        normed,
        feedforward_norm_gain.reshape(1, features),
        dest,
        token_expert_weight[0].T.reshape(-1),
    )


def solution(mesh):
    torus = Mesh(mesh.devices.reshape(mesh.shape["sp"], 4, 2), ("sp", "dp_0", "dp_1"))
    return jax.shard_map(
        layer,
        mesh=torus,
        in_specs=(
            P(DP, "sp", None),
            P(DP, "sp", None),
            P(DP, "sp", None),
            P(DP, "sp", None),
            P(DP, "sp", None),
            P(DP, "sp", None),
            P(DP, "sp", None),
            P(DP, "sp", None),
            P("sp"),
            P(),
            P(None, DP),
            P(),
            P(DP, "sp", None),
            P(DP, "sp", None),
            P(SP_DP, None, None),
            P(SP_DP, None, None),
            P(SP_DP, None, None),
            P(),
        ),
        out_specs=P(DP, "sp", None),
        check_vma=False,
    )
```

```python
import jax
import jax.numpy as jnp
from jax import lax
from jax.experimental import pallas as pl
from jax.experimental.pallas import tpu as pltpu
from jax.sharding import Mesh
from jax.sharding import PartitionSpec as P


DP = ("dp_0", "dp_1")
SP_DP = ("sp", "dp_0", "dp_1")
CLAMP_LIMIT = 7.0
SWISH_SLOPE = 1.702
F32 = jnp.float32
BF16 = jnp.bfloat16
HIGHEST = lax.Precision.HIGHEST
C = 128
EXTRA = 16
VMEM = pl.BlockSpec(memory_space=pltpu.VMEM)
SMEM = pl.BlockSpec(memory_space=pltpu.SMEM)
HBM = pl.BlockSpec(memory_space=pltpu.HBM)


def near(x):
    return pltpu.with_memory_space_constraint(x, pltpu.VMEM)


def far(x):
    return pltpu.with_memory_space_constraint(x, pltpu.HBM)


def dot(a, b):
    return jnp.dot(a, b, preferred_element_type=F32)


def dot_nt(a, b, precision=None):
    return lax.dot_general(
        a, b, (((1,), (1,)), ((), ())), precision=precision, preferred_element_type=F32
    )


def halves(x):
    high = x.astype(BF16)
    return high, (x - high.astype(F32)).astype(BF16)


def iotas(rows, columns):
    shape = (rows, columns)
    return lax.broadcasted_iota(jnp.int32, shape, 0), lax.broadcasted_iota(jnp.int32, shape, 1)


def swap_matrix():
    row, column = iotas(256, 256)
    return jnp.where((row % 16) * 16 + row // 16 == column, 1.0, 0.0).astype(BF16)


def pack_kernel(q_ref, k_ref, v_ref, logit_ref, decay_ref, out_hbm, out_ref, sems, out_sems):
    heads = out_ref.shape[0]
    copies = []
    for h in range(heads):
        columns = slice(h * C, (h + 1) * C)
        for k, source in enumerate((k_ref, q_ref, v_ref)):
            copy = pltpu.make_async_copy(
                source.at[0, :, columns],
                out_ref.at[h, k * C : (k + 1) * C],
                sems.at[len(copies)],
            )
            copy.start()
            copies.append(copy)
    logits = logit_ref[0].astype(F32)
    decays = decay_ref[0].astype(F32)
    extra_row, _ = iotas(EXTRA, C)
    for h in range(heads):
        extra = jnp.where(extra_row == 0, logits[h : h + 1], decays[h : h + 1])
        out_ref[h, 3 * C : 3 * C + EXTRA] = extra.astype(BF16)
    sent = []
    for h in range(heads):
        for copy in copies[3 * h : 3 * h + 3]:
            copy.wait()
        sent.append(pltpu.make_async_copy(out_ref.at[h], out_hbm.at[h], out_sems.at[h]))
        sent[h].start()
    for copy in sent:
        copy.wait()


def pack(query, key, value, logit, decay_input):
    heads = logit.shape[1]
    return pl.pallas_call(
        pack_kernel,
        out_shape=pltpu.HBM((heads, 3 * C + EXTRA, C), BF16),
        in_specs=[HBM] * 3 + [VMEM] * 2,
        out_specs=HBM,
        scratch_shapes=[
            pltpu.VMEM((heads, 3 * C + EXTRA, C), BF16),
            pltpu.SemaphoreType.DMA((3 * heads,)),
            pltpu.SemaphoreType.DMA((heads,)),
        ],
        compiler_params=pltpu.CompilerParams(vmem_limit_bytes=12 * 2**20),
        name="pack",
    )(far(query), far(key), far(value), far(logit), far(decay_input))


GROUP = 8
WIDE_GROUP = 16


def column_of(ref, n):
    lane = lax.broadcasted_iota(jnp.int32, ref.shape, 1)
    return jnp.sum(jnp.where(lane == n, ref[...], 0.0), axis=1, keepdims=True)


def beside(a, b):
    return jnp.concatenate([a, b], axis=1)


def above(a, b):
    return jnp.concatenate([a, b], axis=0)


def recurrence_kernel(
    x_ref, added_ref, rate_ref, out_hbm, base_ref, weight_ref, a_ref, b_ref, qe_ref, su_ref,
    cum_col_ref, cum_row_ref, key_col_ref, key_row_ref, write_col_ref, write_row_ref, out_ref,
    sems,
):
    def send(g):
        part = pl.ds(g * GROUP, GROUP)
        return pltpu.make_async_copy(out_ref.at[part], out_hbm.at[part], sems.at[g])

    inverse_part(
        x_ref, added_ref, rate_ref, base_ref, weight_ref, a_ref,
        cum_col_ref, cum_row_ref, key_col_ref, key_row_ref, write_col_ref, write_row_ref,
    )
    delta_part(
        x_ref, base_ref, weight_ref, a_ref, cum_col_ref, cum_row_ref, key_col_ref, key_row_ref,
        out_ref, b_ref, qe_ref, su_ref, send,
    )
    for g in range(x_ref.shape[0] // GROUP):
        send(g).wait()


def inverse_part(
    x_ref, added_ref, rate_ref, base_ref, weight_ref, a_ref,
    cum_col_ref, cum_row_ref, key_col_ref, key_row_ref, write_col_ref, write_row_ref,
):
    chunks = x_ref.shape[0]
    row, column = iotas(C, C)
    inclusive = row >= column
    strict = row > column
    diagonal = row == column

    chunk_row, _ = iotas(chunks, C)
    logits = jnp.zeros((chunks, C), F32)
    decays = jnp.zeros((chunks, C), F32)
    for n in range(chunks):
        extra = x_ref[n, 3 * C : 3 * C + EXTRA].astype(F32)
        logits = jnp.where(chunk_row == n, extra[0:1], logits)
        decays = jnp.where(chunk_row == n, extra[1:2], decays)
    softplus = jnp.maximum(decays, 0.0) + jnp.log(1.0 + jnp.exp(-jnp.abs(decays)))
    log_decay = added_ref[...] - rate_ref[0] * softplus
    upper = jnp.where(row <= column, 1.0, 0.0)
    lower = jnp.where(inclusive, 1.0, 0.0)
    eye = jnp.where(diagonal, 1.0, 0.0)
    cum_row_ref[...] = jnp.dot(log_decay, upper, precision=HIGHEST, preferred_element_type=F32)
    cum_col_ref[...] = dot_nt(lower, log_decay, precision=HIGHEST)
    write = 1.0 / (1.0 + jnp.exp(-logits))
    write_row_ref[...] = write
    write_col_ref[...] = dot_nt(eye, write, precision=HIGHEST)
    lane = lax.broadcasted_iota(jnp.int32, (C, chunks), 1)

    def group(g, key_columns):
        ns = [g * WIDE_GROUP + k for k in range(WIDE_GROUP)]
        keys = [x_ref[n, 0:C] for n in ns]
        products = [dot_nt(k, k) for k in keys]
        cum_c = [column_of(cum_col_ref, n) for n in ns]
        write_c = [column_of(write_col_ref, n) for n in ns]
        cum_r = [cum_row_ref[pl.ds(n, 1), :] for n in ns]
        write_r = [write_row_ref[pl.ds(n, 1), :] for n in ns]
        squares = [jnp.where(diagonal, p, 0.0) for p in products]
        key_c = [lax.rsqrt(jnp.sum(s, axis=1, keepdims=True) + 1e-06) for s in squares]
        key_r = [lax.rsqrt(jnp.sum(s, axis=0, keepdims=True) + 1e-06) for s in squares]
        for n, c, r in zip(ns, key_c, key_r):
            key_columns = jnp.where(lane == n, c, key_columns)
            key_row_ref[pl.ds(n, 1), :] = r
        lower_part = [
            jnp.where(
                strict,
                p * jnp.exp(jnp.where(inclusive, cc - cr, -jnp.inf)) * (wc * kc) * kr,
                0.0,
            )
            for p, cc, cr, wc, kc, kr in zip(products, cum_c, cum_r, write_c, key_c, key_r)
        ]

        left = [beside(*halves(part)) for part in lower_part]
        pair = (row // 2 == column // 2) & strict
        inverse = [jnp.where(pair, -part, eye) for part in lower_part]
        size = 2
        while size < C:
            highs = [i.astype(BF16) for i in inverse]
            first = [dot(f, above(h, h)) for f, h in zip(left, highs)]
            first = [above(*halves(f)) for f in first]
            second = [dot(beside(h, h), f) for h, f in zip(highs, first)]
            joined = (row // (2 * size) == column // (2 * size)) & (row // size > column // size)
            inverse = [jnp.where(joined, -s, i) for s, i in zip(second, inverse)]
            size *= 2

        for n, i, w in zip(ns, inverse, write_r):
            base_ref[n] = beside(*halves(i * w))
        weight = [
            beside(*halves(i * (w * jnp.exp(c) * k)))
            for i, w, c, k in zip(inverse, write_r, cum_r, key_r)
        ]
        weight = [dot(w, above(k, k)) for w, k in zip(weight, keys)]
        for n, w in zip(ns, weight):
            weight_ref[n] = w.astype(BF16)
        last = [c[C - 1 : C] for c in cum_c]
        carried = [
            above(*halves(w * (k * jnp.exp(end - c))))
            for w, k, end, c in zip(weight, key_c, last, cum_c)
        ]
        turned = [k.T for k in keys]
        update = [dot(beside(t, t), c) for t, c in zip(turned, carried)]
        for n, u, end in zip(ns, update, last):
            a_ref[n] = beside(*halves(jnp.where(diagonal, jnp.exp(end), 0.0) - u))
        return key_columns

    key_col_ref[...] = lax.fori_loop(
        0, chunks // WIDE_GROUP, group, jnp.zeros((C, chunks), F32)
    )


def delta_part(
    x_ref, base_ref, weight_ref, a_ref, cum_col_ref, cum_row_ref, key_col_ref, key_row_ref,
    out_ref, b_ref, qe_ref, su_ref, send,
):
    chunks = x_ref.shape[0]
    row, column = iotas(C, C)
    inclusive = row >= column

    def prepare(g):
        ns = [g * GROUP + k for k in range(GROUP)]
        keys = [x_ref[n, 0:C] for n in ns]
        queries = [x_ref[n, C : 2 * C] for n in ns]
        values = [x_ref[n, 2 * C : 3 * C] for n in ns]
        scores = [dot_nt(q, k) for q, k in zip(queries, keys)]
        base = [dot(base_ref[n], above(v, v)) for n, v in zip(ns, values)]
        cum_c = [column_of(cum_col_ref, n) for n in ns]
        key_c = [column_of(key_col_ref, n) for n in ns]
        cum_r = [cum_row_ref[pl.ds(n, 1), :] for n in ns]
        key_r = [key_row_ref[pl.ds(n, 1), :] for n in ns]
        q32 = [q.astype(F32) for q in queries]
        query_c = [
            lax.rsqrt(jnp.sum(q * q, axis=1, keepdims=True) + 1e-06) * C ** (-0.5) for q in q32
        ]
        scores = [
            s * jnp.exp(jnp.where(inclusive, cc - cr, -jnp.inf)) * kr * qc
            for s, cc, cr, kr, qc in zip(scores, cum_c, cum_r, key_r, query_c)
        ]
        carried = [
            above(*halves(b * (k * jnp.exp(c[C - 1 : C] - c))))
            for b, k, c in zip(base, key_c, cum_c)
        ]
        turned = [k.T for k in keys]
        update = [dot(beside(t, t), c) for t, c in zip(turned, carried)]
        both = [beside(b.astype(BF16), weight_ref[n]) for n, b in zip(ns, base)]
        seen = [dot(beside(*halves(s)), above(b, b)) for s, b in zip(scores, both)]
        for n, u, s, q, qc, c in zip(ns, update, seen, q32, query_c, cum_c):
            b_ref[n] = u
            su_ref[n] = s[:, :C]
            qe_ref[n] = beside(*halves(q * (qc * jnp.exp(c)) - s[:, C:]))

    def advance(g, state):
        for k in range(GROUP):
            n = g * GROUP + k
            high, low = halves(state)
            queries = qe_ref[n]
            out = dot(queries, above(high, high)) + su_ref[n]
            scale = lax.rsqrt(jnp.mean(out * out, axis=1, keepdims=True) + 1e-05)
            out_ref[n] = (out * scale).astype(BF16)
            a_high, a_low = a_ref[n, :, :C], a_ref[n, :, C:]
            state = dot(beside(a_high, a_high), above(high, low)) + dot(a_low, high) + b_ref[n]
        return state

    prepare(0)

    def step(g, state):
        state = advance(g - 1, state)
        send(g - 1).start()
        prepare(g)
        return state

    state = lax.fori_loop(1, chunks // GROUP, step, jnp.zeros((C, C), F32))
    advance(chunks // GROUP - 1, state)
    send(chunks // GROUP - 1).start()


def recurrence(blocks, added, decay_rate):
    chunks = blocks.shape[0]
    square = pltpu.VMEM((chunks, C, C), F32)
    wide = pltpu.VMEM((chunks, C, 2 * C), BF16)
    columns = pltpu.VMEM((C, chunks), F32)
    rows = pltpu.VMEM((chunks, C), F32)
    return pl.pallas_call(
        recurrence_kernel,
        out_shape=pltpu.HBM((chunks, C, C), BF16),
        in_specs=[VMEM, VMEM, SMEM],
        out_specs=HBM,
        scratch_shapes=[
            wide, pltpu.VMEM((chunks, C, C), BF16), wide, square, wide, square,
            columns, rows, columns, rows, columns, rows,
            pltpu.VMEM((chunks, C, C), BF16), pltpu.SemaphoreType.DMA((chunks // GROUP,)),
        ],
        compiler_params=pltpu.CompilerParams(vmem_limit_bytes=24 * 2**20),
        cost_estimate=pl.CostEstimate(flops=8 * 10**9, bytes_accessed=2**21, transcendentals=0),
        name="recurrence",
    )(near(blocks), added, decay_rate)


def slots_kernel(index_ref, dest_ref, source_ref, count_ref):
    experts = count_ref.shape[0]
    capacity = source_ref.shape[0] // experts

    def clear(e, carry):
        count_ref[e] = 0
        for k in range(capacity):
            source_ref[e * capacity + k] = 0
        return carry

    lax.fori_loop(0, experts, clear, 0)

    tokens = index_ref.shape[0] // 4

    def place(t, carry):
        for k in range(4):
            at = k * tokens + t
            e = index_ref[at]
            used = count_ref[e]
            count_ref[e] = used + 1
            slot = e * capacity + used
            dest_ref[at] = slot
            source_ref[slot] = t
        return carry

    lax.fori_loop(0, tokens, place, 0)


def slots(index, experts, capacity):
    return pl.pallas_call(
        slots_kernel,
        out_shape=(
            jax.ShapeDtypeStruct(index.shape, jnp.int32),
            jax.ShapeDtypeStruct((experts * capacity,), jnp.int32),
        ),
        in_specs=[SMEM],
        out_specs=(SMEM, SMEM),
        scratch_shapes=[pltpu.SMEM((experts,), jnp.int32)],
        compiler_params=pltpu.CompilerParams(vmem_limit_bytes=2**20),
        name="slots",
    )(index)


FETCHED = 6


def project_kernel(
    rec_ref, gate_hbm, head_gain_ref, residual_hbm, gain_ref, source_ref, place_ref,
    *rest,
):
    weight_refs = rest[:8]
    normed_ref, out_ref, gate_ref, residual_ref, gated_ref, mixed_ref, w_ref, sems = rest[8:]
    gate_copy = pltpu.make_async_copy(gate_hbm, gate_ref, sems.at[8])
    gate_copy.start()
    copies = [
        pltpu.make_async_copy(weight_refs[k], w_ref.at[k], sems.at[k]) for k in range(FETCHED)
    ]
    for copy in copies:
        copy.start()
    residual_copy = pltpu.make_async_copy(residual_hbm, residual_ref, sems.at[9])
    residual_copy.start()
    gate_copy.wait()
    heads = rec_ref.shape[0]
    head_gain = head_gain_ref[...]
    for h in range(heads):
        columns = slice(h * C, (h + 1) * C)
        gate = gate_ref[0, :, columns].astype(F32)
        gate = gate / (1.0 + jnp.exp(-gate))
        gated_ref[:, columns] = (rec_ref[h].astype(F32) * head_gain * gate).astype(BF16)
    for k in range(FETCHED, 8):
        mixed_ref[place_ref[k]] = dot(gated_ref[...], weight_refs[k][...])
    for k in range(FETCHED):
        copies[k].wait()
        mixed_ref[place_ref[k]] = dot(gated_ref[...], w_ref[k])
    total = jnp.concatenate([mixed_ref[k] for k in range(8)], axis=1)
    residual_copy.wait()
    total = total + residual_ref[0].astype(F32)
    centred = total - jnp.mean(total, axis=1, keepdims=True)
    variance = jnp.mean(centred * centred, axis=1, keepdims=True)
    normed = (centred * lax.rsqrt(variance + 1e-05) * gain_ref[...]).astype(BF16)
    swap = swap_matrix()
    tiles = normed.shape[1] // C
    for g in range(normed.shape[0] // 16):
        rows = normed[g * 16 : (g + 1) * 16]
        stacked = jnp.concatenate([rows[:, j * C : (j + 1) * C] for j in range(tiles)], axis=0)
        turned = dot(swap, stacked).astype(BF16)
        normed_ref[g * 16 : (g + 1) * 16] = turned.reshape(16, tiles, C)

    def send(i, carry):
        for k in range(16):
            slot = i * 16 + k
            out_ref[slot] = normed_ref[source_ref[slot]]
        return carry

    lax.fori_loop(0, out_ref.shape[0] // 16, send, 0)


def project(recurrent, gate, head_gain, residual, gain, source, place, weights):
    tokens = residual.shape[1]
    features = residual.shape[2]
    tiles = features // C
    return pl.pallas_call(
        project_kernel,
        out_shape=(
            jax.ShapeDtypeStruct((tokens, tiles, C), BF16),
            jax.ShapeDtypeStruct((source.shape[0], tiles, C), BF16),
        ),
        in_specs=[VMEM, HBM, VMEM, HBM, VMEM] + [SMEM] * 2
        + [HBM] * FETCHED + [VMEM] * (8 - FETCHED),
        out_specs=(VMEM, VMEM),
        scratch_shapes=[
            pltpu.VMEM((1, tokens, features), BF16),
            pltpu.VMEM((1, tokens, features), BF16),
            pltpu.VMEM((tokens, features), BF16),
            pltpu.VMEM((8, tokens, features // 8), F32),
            pltpu.VMEM((FETCHED, features, features // 8), BF16),
            pltpu.SemaphoreType.DMA((10,)),
        ],
        compiler_params=pltpu.CompilerParams(vmem_limit_bytes=24 * 2**20),
        cost_estimate=pl.CostEstimate(flops=10**9, bytes_accessed=2**24, transcendentals=0),
        name="project",
    )(
        near(recurrent), far(gate), head_gain, far(residual), gain, source, place,
        *[far(w) for w in weights[:FETCHED]], *[near(w) for w in weights[FETCHED:]],
    )


FF_BLOCK = 512
DOWN_ROWS = 384
TURN_UNROLL = 6


def expert_kernel(
    x_ref, gate_hbm, up_hbm, down_hbm, out_ref, gate_ref, up_ref, down_ref, rows_ref, hidden_ref,
    sems,
):
    slots_, tiles, _ = x_ref.shape
    blocks = hidden_ref.shape[1] // FF_BLOCK
    copies = []
    for f in range(blocks):
        columns = slice(f * FF_BLOCK, (f + 1) * FF_BLOCK)
        for source, target in ((gate_hbm, gate_ref), (up_hbm, up_ref)):
            copies.append(
                pltpu.make_async_copy(
                    source.at[:, columns], target.at[:, columns], sems.at[len(copies)]
                )
            )
    copies.append(pltpu.make_async_copy(down_hbm, down_ref, sems.at[len(copies)]))
    for copy in copies:
        copy.start()
    swap = swap_matrix()

    def turn(i, carry):
        for k in range(TURN_UNROLL):
            start = pl.multiple_of((i * TURN_UNROLL + k) * 32, 32)
            pieces = [x_ref[pl.ds(start + o, 16)].reshape(16 * tiles, C) for o in (0, 16)]
            turned = dot(swap, beside(*pieces)).astype(BF16)
            for j in range(tiles):
                part = turned[j * 16 : (j + 1) * 16]
                rows_ref[pl.ds(start, 16), j * C : (j + 1) * C] = part[:, :C]
                rows_ref[pl.ds(start + 16, 16), j * C : (j + 1) * C] = part[:, C:]
        return carry

    lax.fori_loop(0, slots_ // (32 * TURN_UNROLL), turn, 0)
    for f in range(blocks):
        copies[2 * f].wait()
        copies[2 * f + 1].wait()
        columns = slice(f * FF_BLOCK, (f + 1) * FF_BLOCK)
        rows = rows_ref[...]
        gate = jnp.minimum(dot(rows, gate_ref[:, columns]), CLAMP_LIMIT)
        up = jnp.clip(dot(rows, up_ref[:, columns]), -CLAMP_LIMIT, CLAMP_LIMIT)
        hidden = gate / (1.0 + jnp.exp(-SWISH_SLOPE * gate)) * (up + 1.0)
        hidden_ref[:, columns] = hidden.astype(BF16)
    copies[-1].wait()

    def narrow(i, carry):
        start = pl.multiple_of(i * DOWN_ROWS, DOWN_ROWS)
        made = dot(hidden_ref[pl.ds(start, DOWN_ROWS)], down_ref[...]).astype(BF16)
        for g in range(0, DOWN_ROWS, 32):
            stacked = [
                jnp.concatenate(
                    [made[k : k + 16, j * C : (j + 1) * C] for j in range(tiles)], axis=0
                )
                for k in (g, g + 16)
            ]
            turned = dot(swap, beside(*stacked)).astype(BF16)
            out_ref[pl.ds(start + g, 16)] = turned[:, :C].reshape(16, tiles, C)
            out_ref[pl.ds(start + g + 16, 16)] = turned[:, C:].reshape(16, tiles, C)
        return carry

    lax.fori_loop(0, slots_ // DOWN_ROWS, narrow, 0)


def expert(rows, gate_weight, up_weight, down_weight):
    slots_, _, _ = rows.shape
    features, hidden = gate_weight.shape
    return pl.pallas_call(
        expert_kernel,
        out_shape=jax.ShapeDtypeStruct(rows.shape, BF16),
        in_specs=[VMEM, HBM, HBM, HBM],
        out_specs=VMEM,
        scratch_shapes=[
            pltpu.VMEM(gate_weight.shape, BF16),
            pltpu.VMEM(up_weight.shape, BF16),
            pltpu.VMEM(down_weight.shape, BF16),
            pltpu.VMEM((slots_, features), BF16),
            pltpu.VMEM((slots_, hidden), BF16),
            pltpu.SemaphoreType.DMA((2 * (hidden // FF_BLOCK) + 1,)),
        ],
        compiler_params=pltpu.CompilerParams(vmem_limit_bytes=36 * 2**20),
        cost_estimate=pl.CostEstimate(flops=10**10, bytes_accessed=2**24, transcendentals=0),
        name="expert",
    )(near(rows), far(gate_weight), far(up_weight), far(down_weight))


def combine_kernel(
    back_ref, normed_ref, gain_ref, dest_ref, weight_ref, out_hbm, z_ref, out_ref, sems
):
    tokens, tiles, _ = normed_ref.shape
    swap = swap_matrix()
    gain = gain_ref[...]

    def some(i, carry):
        for k in range(16):
            t = i * 16 + k
            total = normed_ref[t].astype(F32)
            for pick in range(4):
                at = pick * tokens + t
                total = total + weight_ref[at] * back_ref[dest_ref[at]].astype(F32)
            z_ref[t] = total
        return carry

    lax.fori_loop(0, tokens // 16, some, 0)

    def finish(i, carry):
        start = pl.multiple_of(i * 16, 16)
        z = z_ref[pl.ds(start, 16)].reshape(16 * tiles, C)
        high = z.astype(BF16)
        rest = z - high.astype(F32)
        middle = rest.astype(BF16)
        low = (rest - middle.astype(F32)).astype(BF16)
        turned = dot(swap, beside(high, middle))
        turned = turned[:, :C] + turned[:, C:] + dot(swap, low)
        total = jnp.concatenate([turned[j * 16 : (j + 1) * 16] for j in range(tiles)], axis=1)
        centred = total - jnp.mean(total, axis=1, keepdims=True)
        variance = jnp.mean(centred * centred, axis=1, keepdims=True)
        out_ref[pl.ds(start, 16), :] = centred * lax.rsqrt(variance + 1e-05) * gain
        send(i).start()
        return carry

    def send(i):
        part = pl.ds(pl.multiple_of(i * 16, 16), 16)
        return pltpu.make_async_copy(out_ref.at[part], out_hbm.at[0, part], sems.at[i])

    lax.fori_loop(0, tokens // 16, finish, 0, unroll=2)
    for i in range(tokens // 16):
        send(i).wait()


def combine(back, normed, gain, dest, weight):
    tokens, tiles, _ = normed.shape
    return pl.pallas_call(
        combine_kernel,
        out_shape=pltpu.HBM((1, tokens, tiles * C), F32),
        in_specs=[VMEM] * 3 + [SMEM] * 2,
        out_specs=HBM,
        scratch_shapes=[
            pltpu.VMEM((tokens, tiles, C), F32),
            pltpu.VMEM((tokens, tiles * C), F32),
            pltpu.SemaphoreType.DMA((tokens // 16,)),
        ],
        compiler_params=pltpu.CompilerParams(vmem_limit_bytes=12 * 2**20),
        name="combine",
    )(near(back), near(normed), gain, dest, weight)


def gathered(block):
    y_size, core_size = lax.axis_size("dp_0"), lax.axis_size("dp_1")
    y, core = lax.axis_index("dp_0"), lax.axis_index("dp_1")
    found = [block]
    for shift in range(1, y_size):
        pairs = [(i, (i + shift) % y_size) for i in range(y_size)]
        found.append(lax.ppermute(block, "dp_0", pairs))
    places = [((y - shift) % y_size) * core_size + core for shift in range(y_size)]
    others = [((y - shift) % y_size) * core_size + 1 - core for shift in range(y_size)]
    return found, jnp.stack(places + others).astype(jnp.int32)


def layer(
    residual,
    query,
    key,
    value,
    output_gate_input,
    write_strength_logit,
    decay_head_input,
    added_log_decay,
    head_decay_rate,
    head_norm_gain,
    output_projection,
    mixer_norm_gain,
    token_expert_index,
    token_expert_weight,
    expert_gate_weight,
    expert_up_weight,
    expert_down_weight,
    feedforward_norm_gain,
):
    experts = lax.axis_size(SP_DP)
    tokens, features = residual.shape[1:]
    picks = token_expert_index.shape[2]
    capacity = tokens * picks * 3 // (2 * experts)
    tiles = features // C
    found, places = gathered(output_projection)
    dest, source = slots(token_expert_index[0].T.reshape(-1), experts, capacity)
    blocks = pack(
        query,
        key,
        value,
        write_strength_logit.transpose(0, 2, 1),
        decay_head_input.transpose(0, 2, 1),
    )
    blocks = lax.all_to_all(blocks, "sp", split_axis=0, concat_axis=0, tiled=True)
    recurrent = recurrence(blocks, added_log_decay.reshape(-1, C), head_decay_rate)
    returned = lax.all_to_all(recurrent, "sp", split_axis=0, concat_axis=0, tiled=True)
    weights = list(found)
    for b in found:
        weights.append(lax.ppermute(b, "dp_1", [(0, 1), (1, 0)]))
    normed, rows = project(
        returned,
        output_gate_input,
        head_norm_gain.reshape(1, C),
        residual,
        mixer_norm_gain.reshape(1, features),
        source,
        places,
        weights,
    )
    rows = rows.reshape(experts, capacity * tiles, C)
    rows = lax.all_to_all(rows, SP_DP, split_axis=0, concat_axis=0, tiled=True)
    made = expert(
        rows.reshape(experts * capacity, tiles, C),
        expert_gate_weight[0],
        expert_up_weight[0],
        expert_down_weight[0],
    )
    made = made.reshape(experts, capacity * tiles, C)
    back = lax.all_to_all(made, SP_DP, split_axis=0, concat_axis=0, tiled=True)
    return combine(
        back.reshape(experts * capacity, tiles, C),
        normed,
        feedforward_norm_gain.reshape(1, features),
        dest,
        token_expert_weight[0].T.reshape(-1),
    )


def solution(mesh):
    torus = Mesh(mesh.devices.reshape(mesh.shape["sp"], 4, 2), ("sp", "dp_0", "dp_1"))
    return jax.shard_map(
        layer,
        mesh=torus,
        in_specs=(
            P(DP, "sp", None),
            P(DP, "sp", None),
            P(DP, "sp", None),
            P(DP, "sp", None),
            P(DP, "sp", None),
            P(DP, "sp", None),
            P(DP, "sp", None),
            P(DP, "sp", None),
            P("sp"),
            P(),
            P(None, DP),
            P(),
            P(DP, "sp", None),
            P(DP, "sp", None),
            P(SP_DP, None, None),
            P(SP_DP, None, None),
            P(SP_DP, None, None),
            P(),
        ),
        out_specs=P(DP, "sp", None),
        check_vma=False,
    )
```

```python
import jax
import jax.numpy as jnp
from jax import lax
from jax.experimental import pallas as pl
from jax.experimental.pallas import tpu as pltpu
from jax.sharding import Mesh
from jax.sharding import PartitionSpec as P


DP = ("dp_0", "dp_1")
SP_DP = ("sp", "dp_0", "dp_1")
CLAMP_LIMIT = 7.0
SWISH_SLOPE = 1.702
F32 = jnp.float32
BF16 = jnp.bfloat16
HIGHEST = lax.Precision.HIGHEST
C = 128
EXTRA = 16
VMEM = pl.BlockSpec(memory_space=pltpu.VMEM)
SMEM = pl.BlockSpec(memory_space=pltpu.SMEM)
HBM = pl.BlockSpec(memory_space=pltpu.HBM)


def near(x):
    return pltpu.with_memory_space_constraint(x, pltpu.VMEM)


def far(x):
    return pltpu.with_memory_space_constraint(x, pltpu.HBM)


def dot(a, b):
    return jnp.dot(a, b, preferred_element_type=F32)


def dot_nt(a, b, precision=None):
    return lax.dot_general(
        a, b, (((1,), (1,)), ((), ())), precision=precision, preferred_element_type=F32
    )


def halves(x):
    high = x.astype(BF16)
    return high, (x - high.astype(F32)).astype(BF16)


def iotas(rows, columns):
    shape = (rows, columns)
    return lax.broadcasted_iota(jnp.int32, shape, 0), lax.broadcasted_iota(jnp.int32, shape, 1)


def swap_matrix():
    row, column = iotas(256, 256)
    return jnp.where((row % 16) * 16 + row // 16 == column, 1.0, 0.0).astype(BF16)


def pack_kernel(q_ref, k_ref, v_ref, logit_ref, decay_ref, out_hbm, out_ref, sems, out_sems):
    heads = out_ref.shape[0]
    copies = []
    for h in range(heads):
        columns = slice(h * C, (h + 1) * C)
        for k, source in enumerate((k_ref, q_ref, v_ref)):
            copy = pltpu.make_async_copy(
                source.at[0, :, columns],
                out_ref.at[h, k * C : (k + 1) * C],
                sems.at[len(copies)],
            )
            copy.start()
            copies.append(copy)
    logits = logit_ref[0].astype(F32)
    decays = decay_ref[0].astype(F32)
    extra_row, _ = iotas(EXTRA, C)
    for h in range(heads):
        extra = jnp.where(extra_row == 0, logits[h : h + 1], decays[h : h + 1])
        out_ref[h, 3 * C : 3 * C + EXTRA] = extra.astype(BF16)
    sent = []
    for h in range(heads):
        for copy in copies[3 * h : 3 * h + 3]:
            copy.wait()
        sent.append(pltpu.make_async_copy(out_ref.at[h], out_hbm.at[h], out_sems.at[h]))
        sent[h].start()
    for copy in sent:
        copy.wait()


def pack(query, key, value, logit, decay_input):
    heads = logit.shape[1]
    return pl.pallas_call(
        pack_kernel,
        out_shape=pltpu.HBM((heads, 3 * C + EXTRA, C), BF16),
        in_specs=[HBM] * 3 + [VMEM] * 2,
        out_specs=HBM,
        scratch_shapes=[
            pltpu.VMEM((heads, 3 * C + EXTRA, C), BF16),
            pltpu.SemaphoreType.DMA((3 * heads,)),
            pltpu.SemaphoreType.DMA((heads,)),
        ],
        compiler_params=pltpu.CompilerParams(vmem_limit_bytes=12 * 2**20),
        name="pack",
    )(far(query), far(key), far(value), far(logit), far(decay_input))


GROUP = 8
WIDE_GROUP = 16


def column_of(ref, n):
    lane = lax.broadcasted_iota(jnp.int32, ref.shape, 1)
    return jnp.sum(jnp.where(lane == n, ref[...], 0.0), axis=1, keepdims=True)


def beside(a, b):
    return jnp.concatenate([a, b], axis=1)


def above(a, b):
    return jnp.concatenate([a, b], axis=0)


def recurrence_kernel(
    x_ref, added_ref, rate_ref, out_hbm, base_ref, weight_ref, a_ref, b_ref, qe_ref, su_ref,
    cum_col_ref, cum_row_ref, key_col_ref, key_row_ref, write_col_ref, write_row_ref, out_ref,
    sems,
):
    def send(g):
        part = pl.ds(g * GROUP, GROUP)
        return pltpu.make_async_copy(out_ref.at[part], out_hbm.at[part], sems.at[g])

    inverse_part(
        x_ref, added_ref, rate_ref, base_ref, weight_ref, a_ref,
        cum_col_ref, cum_row_ref, key_col_ref, key_row_ref, write_col_ref, write_row_ref,
    )
    delta_part(
        x_ref, base_ref, weight_ref, a_ref, cum_col_ref, cum_row_ref, key_col_ref, key_row_ref,
        out_ref, b_ref, qe_ref, su_ref, send,
    )
    for g in range(x_ref.shape[0] // GROUP):
        send(g).wait()


def inverse_part(
    x_ref, added_ref, rate_ref, base_ref, weight_ref, a_ref,
    cum_col_ref, cum_row_ref, key_col_ref, key_row_ref, write_col_ref, write_row_ref,
):
    chunks = x_ref.shape[0]
    row, column = iotas(C, C)
    inclusive = row >= column
    strict = row > column
    diagonal = row == column

    chunk_row, _ = iotas(chunks, C)
    logits = jnp.zeros((chunks, C), F32)
    decays = jnp.zeros((chunks, C), F32)
    for n in range(chunks):
        extra = x_ref[n, 3 * C : 3 * C + EXTRA].astype(F32)
        logits = jnp.where(chunk_row == n, extra[0:1], logits)
        decays = jnp.where(chunk_row == n, extra[1:2], decays)
    softplus = jnp.maximum(decays, 0.0) + jnp.log(1.0 + jnp.exp(-jnp.abs(decays)))
    log_decay = added_ref[...] - rate_ref[0] * softplus
    upper = jnp.where(row <= column, 1.0, 0.0)
    lower = jnp.where(inclusive, 1.0, 0.0)
    eye = jnp.where(diagonal, 1.0, 0.0)
    cum_row_ref[...] = jnp.dot(log_decay, upper, precision=HIGHEST, preferred_element_type=F32)
    cum_col_ref[...] = dot_nt(lower, log_decay, precision=HIGHEST)
    write = 1.0 / (1.0 + jnp.exp(-logits))
    write_row_ref[...] = write
    write_col_ref[...] = dot_nt(eye, write, precision=HIGHEST)
    lane = lax.broadcasted_iota(jnp.int32, (C, chunks), 1)

    def group(g, key_columns):
        ns = [g * WIDE_GROUP + k for k in range(WIDE_GROUP)]
        keys = [x_ref[n, 0:C] for n in ns]
        products = [dot_nt(k, k) for k in keys]
        cum_c = [column_of(cum_col_ref, n) for n in ns]
        write_c = [column_of(write_col_ref, n) for n in ns]
        cum_r = [cum_row_ref[pl.ds(n, 1), :] for n in ns]
        write_r = [write_row_ref[pl.ds(n, 1), :] for n in ns]
        squares = [jnp.where(diagonal, p, 0.0) for p in products]
        key_c = [lax.rsqrt(jnp.sum(s, axis=1, keepdims=True) + 1e-06) for s in squares]
        key_r = [lax.rsqrt(jnp.sum(s, axis=0, keepdims=True) + 1e-06) for s in squares]
        for n, c, r in zip(ns, key_c, key_r):
            key_columns = jnp.where(lane == n, c, key_columns)
            key_row_ref[pl.ds(n, 1), :] = r
        lower_part = [
            jnp.where(
                strict,
                p * jnp.exp(jnp.where(inclusive, cc - cr, -jnp.inf)) * (wc * kc) * kr,
                0.0,
            )
            for p, cc, cr, wc, kc, kr in zip(products, cum_c, cum_r, write_c, key_c, key_r)
        ]

        left = [beside(*halves(part)) for part in lower_part]
        pair = (row // 2 == column // 2) & strict
        inverse = [jnp.where(pair, -part, eye) for part in lower_part]
        size = 2
        while size < C:
            highs = [i.astype(BF16) for i in inverse]
            first = [dot(f, above(h, h)) for f, h in zip(left, highs)]
            first = [above(*halves(f)) for f in first]
            second = [dot(beside(h, h), f) for h, f in zip(highs, first)]
            joined = (row // (2 * size) == column // (2 * size)) & (row // size > column // size)
            inverse = [jnp.where(joined, -s, i) for s, i in zip(second, inverse)]
            size *= 2

        for n, i, w in zip(ns, inverse, write_r):
            base_ref[n] = beside(*halves(i * w))
        weight = [
            beside(*halves(i * (w * jnp.exp(c) * k)))
            for i, w, c, k in zip(inverse, write_r, cum_r, key_r)
        ]
        weight = [dot(w, above(k, k)) for w, k in zip(weight, keys)]
        for n, w in zip(ns, weight):
            weight_ref[n] = w.astype(BF16)
        last = [c[C - 1 : C] for c in cum_c]
        carried = [
            above(*halves(w * (k * jnp.exp(end - c))))
            for w, k, end, c in zip(weight, key_c, last, cum_c)
        ]
        turned = [k.T for k in keys]
        update = [dot(beside(t, t), c) for t, c in zip(turned, carried)]
        for n, u, end in zip(ns, update, last):
            a_ref[n] = beside(*halves(jnp.where(diagonal, jnp.exp(end), 0.0) - u))
        return key_columns

    key_col_ref[...] = lax.fori_loop(
        0, chunks // WIDE_GROUP, group, jnp.zeros((C, chunks), F32)
    )


def delta_part(
    x_ref, base_ref, weight_ref, a_ref, cum_col_ref, cum_row_ref, key_col_ref, key_row_ref,
    out_ref, b_ref, qe_ref, su_ref, send,
):
    chunks = x_ref.shape[0]
    row, column = iotas(C, C)
    inclusive = row >= column

    def prepare(g):
        ns = [g * GROUP + k for k in range(GROUP)]
        keys = [x_ref[n, 0:C] for n in ns]
        queries = [x_ref[n, C : 2 * C] for n in ns]
        values = [x_ref[n, 2 * C : 3 * C] for n in ns]
        scores = [dot_nt(q, k) for q, k in zip(queries, keys)]
        base = [dot(base_ref[n], above(v, v)) for n, v in zip(ns, values)]
        cum_c = [column_of(cum_col_ref, n) for n in ns]
        key_c = [column_of(key_col_ref, n) for n in ns]
        cum_r = [cum_row_ref[pl.ds(n, 1), :] for n in ns]
        key_r = [key_row_ref[pl.ds(n, 1), :] for n in ns]
        q32 = [q.astype(F32) for q in queries]
        query_c = [
            lax.rsqrt(jnp.sum(q * q, axis=1, keepdims=True) + 1e-06) * C ** (-0.5) for q in q32
        ]
        scores = [
            s * jnp.exp(jnp.where(inclusive, cc - cr, -jnp.inf)) * kr * qc
            for s, cc, cr, kr, qc in zip(scores, cum_c, cum_r, key_r, query_c)
        ]
        carried = [
            above(*halves(b * (k * jnp.exp(c[C - 1 : C] - c))))
            for b, k, c in zip(base, key_c, cum_c)
        ]
        turned = [k.T for k in keys]
        update = [dot(beside(t, t), c) for t, c in zip(turned, carried)]
        both = [beside(b.astype(BF16), weight_ref[n]) for n, b in zip(ns, base)]
        seen = [dot(beside(*halves(s)), above(b, b)) for s, b in zip(scores, both)]
        for n, u, s, q, qc, c in zip(ns, update, seen, q32, query_c, cum_c):
            b_ref[n] = u
            su_ref[n] = s[:, :C]
            qe_ref[n] = beside(*halves(q * (qc * jnp.exp(c)) - s[:, C:]))

    def advance(g, state):
        for k in range(GROUP):
            n = g * GROUP + k
            high, low = halves(state)
            queries = qe_ref[n]
            out = dot(queries, above(high, high)) + su_ref[n]
            scale = lax.rsqrt(jnp.mean(out * out, axis=1, keepdims=True) + 1e-05)
            out_ref[n] = (out * scale).astype(BF16)
            a_high, a_low = a_ref[n, :, :C], a_ref[n, :, C:]
            state = dot(beside(a_high, a_high), above(high, low)) + dot(a_low, high) + b_ref[n]
        return state

    prepare(0)

    def step(g, state):
        state = advance(g - 1, state)
        send(g - 1).start()
        prepare(g)
        return state

    state = lax.fori_loop(1, chunks // GROUP, step, jnp.zeros((C, C), F32))
    advance(chunks // GROUP - 1, state)
    send(chunks // GROUP - 1).start()


def recurrence(blocks, added, decay_rate):
    chunks = blocks.shape[0]
    square = pltpu.VMEM((chunks, C, C), F32)
    wide = pltpu.VMEM((chunks, C, 2 * C), BF16)
    columns = pltpu.VMEM((C, chunks), F32)
    rows = pltpu.VMEM((chunks, C), F32)
    return pl.pallas_call(
        recurrence_kernel,
        out_shape=pltpu.HBM((chunks, C, C), BF16),
        in_specs=[VMEM, VMEM, SMEM],
        out_specs=HBM,
        scratch_shapes=[
            wide, pltpu.VMEM((chunks, C, C), BF16), wide, square, wide, square,
            columns, rows, columns, rows, columns, rows,
            pltpu.VMEM((chunks, C, C), BF16), pltpu.SemaphoreType.DMA((chunks // GROUP,)),
        ],
        compiler_params=pltpu.CompilerParams(vmem_limit_bytes=24 * 2**20),
        cost_estimate=pl.CostEstimate(flops=8 * 10**9, bytes_accessed=2**21, transcendentals=0),
        name="recurrence",
    )(near(blocks), added, decay_rate)


def slots_kernel(index_ref, dest_ref, source_ref, count_ref):
    experts = count_ref.shape[0]
    capacity = source_ref.shape[0] // experts

    def clear(e, carry):
        count_ref[e] = 0
        for k in range(capacity):
            source_ref[e * capacity + k] = 0
        return carry

    lax.fori_loop(0, experts, clear, 0)

    tokens = index_ref.shape[0] // 4

    def place(t, carry):
        for k in range(4):
            at = k * tokens + t
            e = index_ref[at]
            used = count_ref[e]
            count_ref[e] = used + 1
            slot = e * capacity + used
            dest_ref[at] = slot
            source_ref[slot] = t
        return carry

    lax.fori_loop(0, tokens, place, 0)


def slots(index, experts, capacity):
    return pl.pallas_call(
        slots_kernel,
        out_shape=(
            jax.ShapeDtypeStruct(index.shape, jnp.int32),
            jax.ShapeDtypeStruct((experts * capacity,), jnp.int32),
        ),
        in_specs=[SMEM],
        out_specs=(SMEM, SMEM),
        scratch_shapes=[pltpu.SMEM((experts,), jnp.int32)],
        compiler_params=pltpu.CompilerParams(vmem_limit_bytes=2**20),
        name="slots",
    )(index)


FETCHED = 6


def project_kernel(
    rec_ref, gate_ref, head_gain_ref, residual_hbm, gain_ref, source_ref, place_ref,
    *rest,
):
    weight_refs = rest[:8]
    normed_ref, out_ref, residual_ref, gated_ref, mixed_ref, w_ref, sems = rest[8:]
    copies = [
        pltpu.make_async_copy(weight_refs[k], w_ref.at[k], sems.at[k]) for k in range(FETCHED)
    ]
    residual_copy = pltpu.make_async_copy(residual_hbm, residual_ref, sems.at[FETCHED])
    for copy in (*copies, residual_copy):
        copy.start()
    heads = rec_ref.shape[0]
    head_gain = head_gain_ref[...]
    for h in range(heads):
        columns = slice(h * C, (h + 1) * C)
        gate = gate_ref[0, :, columns].astype(F32)
        gate = gate / (1.0 + jnp.exp(-gate))
        gated_ref[:, columns] = (rec_ref[h].astype(F32) * head_gain * gate).astype(BF16)
    for k in range(FETCHED, 8):
        mixed_ref[place_ref[k]] = dot(gated_ref[...], weight_refs[k][...])
    for k in range(FETCHED):
        copies[k].wait()
        mixed_ref[place_ref[k]] = dot(gated_ref[...], w_ref[k])
    total = jnp.concatenate([mixed_ref[k] for k in range(8)], axis=1)
    residual_copy.wait()
    total = total + residual_ref[0].astype(F32)
    centred = total - jnp.mean(total, axis=1, keepdims=True)
    variance = jnp.mean(centred * centred, axis=1, keepdims=True)
    normed = (centred * lax.rsqrt(variance + 1e-05) * gain_ref[...]).astype(BF16)
    swap = swap_matrix()
    tiles = normed.shape[1] // C
    for g in range(normed.shape[0] // 16):
        rows = normed[g * 16 : (g + 1) * 16]
        stacked = jnp.concatenate([rows[:, j * C : (j + 1) * C] for j in range(tiles)], axis=0)
        turned = dot(swap, stacked).astype(BF16)
        normed_ref[g * 16 : (g + 1) * 16] = turned.reshape(16, tiles, C)

    def send(i, carry):
        for k in range(16):
            slot = i * 16 + k
            out_ref[slot] = normed_ref[source_ref[slot]]
        return carry

    lax.fori_loop(0, out_ref.shape[0] // 16, send, 0)


def project(recurrent, gate, head_gain, residual, gain, source, place, weights):
    tokens = residual.shape[1]
    features = residual.shape[2]
    tiles = features // C
    return pl.pallas_call(
        project_kernel,
        out_shape=(
            jax.ShapeDtypeStruct((tokens, tiles, C), BF16),
            jax.ShapeDtypeStruct((source.shape[0], tiles, C), BF16),
        ),
        in_specs=[VMEM, VMEM, VMEM, HBM, VMEM] + [SMEM] * 2
        + [HBM] * FETCHED + [VMEM] * (8 - FETCHED),
        out_specs=(VMEM, VMEM),
        scratch_shapes=[
            pltpu.VMEM((1, tokens, features), BF16),
            pltpu.VMEM((tokens, features), BF16),
            pltpu.VMEM((8, tokens, features // 8), F32),
            pltpu.VMEM((FETCHED, features, features // 8), BF16),
            pltpu.SemaphoreType.DMA((FETCHED + 1,)),
        ],
        compiler_params=pltpu.CompilerParams(vmem_limit_bytes=24 * 2**20),
        cost_estimate=pl.CostEstimate(flops=10**9, bytes_accessed=2**24, transcendentals=0),
        name="project",
    )(
        near(recurrent), near(gate), head_gain, far(residual), gain, source, place,
        *[far(w) for w in weights[:FETCHED]], *[near(w) for w in weights[FETCHED:]],
    )


FF_BLOCK = 512
DOWN_ROWS = 384
TURN_UNROLL = 6


def expert_kernel(
    x_ref, gate_hbm, up_hbm, down_hbm, out_ref, gate_ref, up_ref, down_ref, rows_ref, hidden_ref,
    sems,
):
    slots_, tiles, _ = x_ref.shape
    blocks = hidden_ref.shape[1] // FF_BLOCK
    copies = []
    for f in range(blocks):
        columns = slice(f * FF_BLOCK, (f + 1) * FF_BLOCK)
        for source, target in ((gate_hbm, gate_ref), (up_hbm, up_ref)):
            copies.append(
                pltpu.make_async_copy(
                    source.at[:, columns], target.at[:, columns], sems.at[len(copies)]
                )
            )
    copies.append(pltpu.make_async_copy(down_hbm, down_ref, sems.at[len(copies)]))
    for copy in copies:
        copy.start()
    swap = swap_matrix()

    def turn(i, carry):
        for k in range(TURN_UNROLL):
            start = pl.multiple_of((i * TURN_UNROLL + k) * 32, 32)
            pieces = [x_ref[pl.ds(start + o, 16)].reshape(16 * tiles, C) for o in (0, 16)]
            turned = dot(swap, beside(*pieces)).astype(BF16)
            for j in range(tiles):
                part = turned[j * 16 : (j + 1) * 16]
                rows_ref[pl.ds(start, 16), j * C : (j + 1) * C] = part[:, :C]
                rows_ref[pl.ds(start + 16, 16), j * C : (j + 1) * C] = part[:, C:]
        return carry

    lax.fori_loop(0, slots_ // (32 * TURN_UNROLL), turn, 0)
    for f in range(blocks):
        copies[2 * f].wait()
        copies[2 * f + 1].wait()
        columns = slice(f * FF_BLOCK, (f + 1) * FF_BLOCK)
        rows = rows_ref[...]
        gate = jnp.minimum(dot(rows, gate_ref[:, columns]), CLAMP_LIMIT)
        up = jnp.clip(dot(rows, up_ref[:, columns]), -CLAMP_LIMIT, CLAMP_LIMIT)
        hidden = gate / (1.0 + jnp.exp(-SWISH_SLOPE * gate)) * (up + 1.0)
        hidden_ref[:, columns] = hidden.astype(BF16)
    copies[-1].wait()

    def narrow(i, carry):
        start = pl.multiple_of(i * DOWN_ROWS, DOWN_ROWS)
        made = dot(hidden_ref[pl.ds(start, DOWN_ROWS)], down_ref[...]).astype(BF16)
        for g in range(0, DOWN_ROWS, 32):
            stacked = [
                jnp.concatenate(
                    [made[k : k + 16, j * C : (j + 1) * C] for j in range(tiles)], axis=0
                )
                for k in (g, g + 16)
            ]
            turned = dot(swap, beside(*stacked)).astype(BF16)
            out_ref[pl.ds(start + g, 16)] = turned[:, :C].reshape(16, tiles, C)
            out_ref[pl.ds(start + g + 16, 16)] = turned[:, C:].reshape(16, tiles, C)
        return carry

    lax.fori_loop(0, slots_ // DOWN_ROWS, narrow, 0)


def expert(rows, gate_weight, up_weight, down_weight):
    slots_, _, _ = rows.shape
    features, hidden = gate_weight.shape
    return pl.pallas_call(
        expert_kernel,
        out_shape=jax.ShapeDtypeStruct(rows.shape, BF16),
        in_specs=[VMEM, HBM, HBM, HBM],
        out_specs=VMEM,
        scratch_shapes=[
            pltpu.VMEM(gate_weight.shape, BF16),
            pltpu.VMEM(up_weight.shape, BF16),
            pltpu.VMEM(down_weight.shape, BF16),
            pltpu.VMEM((slots_, features), BF16),
            pltpu.VMEM((slots_, hidden), BF16),
            pltpu.SemaphoreType.DMA((2 * (hidden // FF_BLOCK) + 1,)),
        ],
        compiler_params=pltpu.CompilerParams(vmem_limit_bytes=36 * 2**20),
        cost_estimate=pl.CostEstimate(flops=10**10, bytes_accessed=2**24, transcendentals=0),
        name="expert",
    )(near(rows), far(gate_weight), far(up_weight), far(down_weight))


def combine_kernel(
    back_ref, normed_ref, gain_ref, dest_ref, weight_ref, out_hbm, z_ref, out_ref, sems
):
    tokens, tiles, _ = normed_ref.shape
    swap = swap_matrix()
    gain = gain_ref[...]

    def some(i, carry):
        for k in range(16):
            t = i * 16 + k
            total = normed_ref[t].astype(F32)
            for pick in range(4):
                at = pick * tokens + t
                total = total + weight_ref[at] * back_ref[dest_ref[at]].astype(F32)
            z_ref[t] = total
        return carry

    lax.fori_loop(0, tokens // 16, some, 0)

    def finish(i, carry):
        start = pl.multiple_of(i * 16, 16)
        z = z_ref[pl.ds(start, 16)].reshape(16 * tiles, C)
        high = z.astype(BF16)
        rest = z - high.astype(F32)
        middle = rest.astype(BF16)
        low = (rest - middle.astype(F32)).astype(BF16)
        turned = dot(swap, beside(high, middle))
        turned = turned[:, :C] + turned[:, C:] + dot(swap, low)
        total = jnp.concatenate([turned[j * 16 : (j + 1) * 16] for j in range(tiles)], axis=1)
        centred = total - jnp.mean(total, axis=1, keepdims=True)
        variance = jnp.mean(centred * centred, axis=1, keepdims=True)
        out_ref[pl.ds(start, 16), :] = centred * lax.rsqrt(variance + 1e-05) * gain
        send(i).start()
        return carry

    def send(i):
        part = pl.ds(pl.multiple_of(i * 16, 16), 16)
        return pltpu.make_async_copy(out_ref.at[part], out_hbm.at[0, part], sems.at[i])

    lax.fori_loop(0, tokens // 16, finish, 0, unroll=2)
    for i in range(tokens // 16):
        send(i).wait()


def combine(back, normed, gain, dest, weight):
    tokens, tiles, _ = normed.shape
    return pl.pallas_call(
        combine_kernel,
        out_shape=pltpu.HBM((1, tokens, tiles * C), F32),
        in_specs=[VMEM] * 3 + [SMEM] * 2,
        out_specs=HBM,
        scratch_shapes=[
            pltpu.VMEM((tokens, tiles, C), F32),
            pltpu.VMEM((tokens, tiles * C), F32),
            pltpu.SemaphoreType.DMA((tokens // 16,)),
        ],
        compiler_params=pltpu.CompilerParams(vmem_limit_bytes=12 * 2**20),
        name="combine",
    )(near(back), near(normed), gain, dest, weight)


def gathered(block):
    y_size, core_size = lax.axis_size("dp_0"), lax.axis_size("dp_1")
    y, core = lax.axis_index("dp_0"), lax.axis_index("dp_1")
    found = [block]
    for shift in range(1, y_size):
        pairs = [(i, (i + shift) % y_size) for i in range(y_size)]
        found.append(lax.ppermute(block, "dp_0", pairs))
    places = [((y - shift) % y_size) * core_size + core for shift in range(y_size)]
    others = [((y - shift) % y_size) * core_size + 1 - core for shift in range(y_size)]
    return found, jnp.stack(places + others).astype(jnp.int32)


def layer(
    residual,
    query,
    key,
    value,
    output_gate_input,
    write_strength_logit,
    decay_head_input,
    added_log_decay,
    head_decay_rate,
    head_norm_gain,
    output_projection,
    mixer_norm_gain,
    token_expert_index,
    token_expert_weight,
    expert_gate_weight,
    expert_up_weight,
    expert_down_weight,
    feedforward_norm_gain,
):
    experts = lax.axis_size(SP_DP)
    tokens, features = residual.shape[1:]
    picks = token_expert_index.shape[2]
    capacity = tokens * picks * 3 // (2 * experts)
    tiles = features // C
    found, places = gathered(output_projection)
    dest, source = slots(token_expert_index[0].T.reshape(-1), experts, capacity)
    blocks = pack(
        query,
        key,
        value,
        write_strength_logit.transpose(0, 2, 1),
        decay_head_input.transpose(0, 2, 1),
    )
    blocks = lax.all_to_all(blocks, "sp", split_axis=0, concat_axis=0, tiled=True)
    recurrent = recurrence(blocks, added_log_decay.reshape(-1, C), head_decay_rate)
    returned = lax.all_to_all(recurrent, "sp", split_axis=0, concat_axis=0, tiled=True)
    weights = list(found)
    for b in found:
        weights.append(lax.ppermute(b, "dp_1", [(0, 1), (1, 0)]))
    normed, rows = project(
        returned,
        output_gate_input,
        head_norm_gain.reshape(1, C),
        residual,
        mixer_norm_gain.reshape(1, features),
        source,
        places,
        weights,
    )
    rows = rows.reshape(experts, capacity * tiles, C)
    rows = lax.all_to_all(rows, SP_DP, split_axis=0, concat_axis=0, tiled=True)
    made = expert(
        rows.reshape(experts * capacity, tiles, C),
        expert_gate_weight[0],
        expert_up_weight[0],
        expert_down_weight[0],
    )
    made = made.reshape(experts, capacity * tiles, C)
    back = lax.all_to_all(made, SP_DP, split_axis=0, concat_axis=0, tiled=True)
    return combine(
        back.reshape(experts * capacity, tiles, C),
        normed,
        feedforward_norm_gain.reshape(1, features),
        dest,
        token_expert_weight[0].T.reshape(-1),
    )


def solution(mesh):
    torus = Mesh(mesh.devices.reshape(mesh.shape["sp"], 4, 2), ("sp", "dp_0", "dp_1"))
    return jax.shard_map(
        layer,
        mesh=torus,
        in_specs=(
            P(DP, "sp", None),
            P(DP, "sp", None),
            P(DP, "sp", None),
            P(DP, "sp", None),
            P(DP, "sp", None),
            P(DP, "sp", None),
            P(DP, "sp", None),
            P(DP, "sp", None),
            P("sp"),
            P(),
            P(None, DP),
            P(),
            P(DP, "sp", None),
            P(DP, "sp", None),
            P(SP_DP, None, None),
            P(SP_DP, None, None),
            P(SP_DP, None, None),
            P(),
        ),
        out_specs=P(DP, "sp", None),
        check_vma=False,
    )
```
